256 devices in a mesh: sp: 32 (over z, y), tp: 8 (over x, core).
Axes of the slice: x: 4, y: 4, z: 8, core: 2. Of those that a mesh axis runs over, the one named last changes fastest.
Arguments:
- tokens: bfloat16 [4, 16384, 2048], P(None, ('sp', 'tp')), may hold values from -6 to 6
- in_gain: float32 [2048], replicated, may hold values from 0.1 to 1.9
- query_weight: bfloat16 [2048, 1024], P(None, 'tp'), may hold values from -0.125 to 0.125
- key_weight: bfloat16 [2048, 1024], P(None, 'tp'), may hold values from -0.125 to 0.125
- value_weight: bfloat16 [2048, 1024], P(None, 'tp'), may hold values from -0.125 to 0.125
- gate_weight: bfloat16 [2048, 1024], P(None, 'tp'), may hold values from -0.125 to 0.125
- log_decay: float32 [8], P('tp'), may hold values from -0.034 to 0, as said below
- norm_gain: float32 [1024], P('tp'), may hold values from 0.1 to 1.9
- out_weight: bfloat16 [1024, 2048], replicated, may hold values from -0.1875 to 0.1875
- post_gain: float32 [2048], replicated, may hold values from 0.1 to 1.9
Outputs:
- mixed: bfloat16 [4, 16384, 2048], P(None, ('sp', 'tp'))
The draws below stay inside these ranges and needn't reach their ends.
Inputs may be any that keep to these rules, and one draw needn't show every extreme that they name: `log_decay`: every entry is negative; some heads keep a tenth or more of their memory over 16384 positions, others lose most of it within 30 to 100 positions.
All inputs are finite; a program needn't handle non-finite values.
Results may differ from the reference program's by a relative error of at most 0.015.
Values may be sent and summed in bfloat16 or wider, within the bound.
A program may use at most 64 MiB of HBM per device.

```python
import math
import jax
import jax.numpy as jnp
from jax import lax

D = 2048
HEADS = 8
HEAD_DIM = 128
BLOCK = 128
SEQS = 4
RET_WIDTH = 1024
SEQLEN = 16384


def draw_log_decay(key, part):
    head_order = jax.random.permutation(jax.random.fold_in(key, 11), HEADS)
    slow_heads = head_order < HEADS // 2
    uniform_draw = jax.random.uniform(jax.random.fold_in(key, 12), (HEADS,), jnp.float32)
    slow_rate = math.log(10.0) / SEQLEN * (0.1 + 0.9 * uniform_draw)
    fast_rate = jnp.exp(math.log(1.0 / 100.0) + uniform_draw * (math.log(1.0 / 30.0) - math.log(1.0 / 100.0)))
    return -jnp.where(slow_heads, slow_rate, fast_rate).astype(jnp.float32)


def level_of(stream_key, dims, pieces, smallest, high):
    level = 1.0
    for position, parts in pieces:
        steps = jax.random.uniform(jax.random.fold_in(jax.random.fold_in(stream_key, 6), position), (parts,), jnp.float32, smallest / len(pieces), high / len(pieces))
        level = level * jnp.repeat(jnp.exp(steps), dims[position] // parts).reshape((-1,) + (1,) * (len(dims) - 1 - position))
    return level


def noise(own_key, shape, scale, reach, split=(), kind=jnp.bfloat16):
    level = level_of(own_key, shape, split, -0.22, 0.18) if split else 1.0
    values = jax.random.normal(own_key, shape, jnp.float32) * scale * level
    return jnp.minimum(jnp.maximum(values, -reach), reach).astype(kind)


def setup_inputs(seed: int = 0) -> dict:
    keys = jax.random.split(jax.random.key(seed), 11)
    return {
        "tokens": noise(keys[0], (SEQS, SEQLEN, D), 1.0, 6.0, ((1, 256),)),
        "in_gain": jnp.clip(1.0 + 0.18 * jax.random.normal(keys[1], (D,), jnp.float32), 0.1, 1.9),
        "query_weight": noise(keys[2], (D, RET_WIDTH), D ** -0.5, 0.125, ((1, 8),)),
        "key_weight": noise(keys[3], (D, RET_WIDTH), D ** -0.5, 0.125, ((1, 8),)),
        "value_weight": noise(keys[4], (D, RET_WIDTH), D ** -0.5, 0.125, ((1, 8),)),
        "gate_weight": noise(keys[5], (D, RET_WIDTH), D ** -0.5, 0.125, ((1, 8),)),
        "log_decay": draw_log_decay(jax.random.fold_in(keys[10], 71), 0),
        "norm_gain": jnp.clip(1.0 + 0.18 * jax.random.normal(keys[7], (RET_WIDTH,), jnp.float32), 0.1, 1.9),
        "out_weight": noise(keys[8], (RET_WIDTH, D), RET_WIDTH ** -0.5, 0.1875),
        "post_gain": jnp.clip(1.0 + 0.18 * jax.random.normal(keys[9], (D,), jnp.float32), 0.1, 1.9),
    }


rms_eps = 1e-06
group_eps = 1e-05
rope_base = 10000.0
highest = lax.Precision.HIGHEST

def rotate(values, positions):
    half_dim = values.shape[-1] // 2
    inverse = rope_base ** (-jnp.arange(half_dim, dtype=jnp.float32) / half_dim)
    angles = positions.astype(jnp.float32)[:, None] * inverse[None, :]
    cosine = jnp.cos(angles)
    sine_part = jnp.sin(angles)
    first_half = values[..., :half_dim].astype(jnp.float32)
    second = values[..., half_dim:].astype(jnp.float32)
    return jnp.concatenate([first_half * cosine - second * sine_part, first_half * sine_part + second * cosine], axis=-1)

def retain(queries, key_rows, values, log_decay):
    seq_count, head_count, length, head_width = queries.shape
    block_count = length // BLOCK
    offsets = jnp.arange(BLOCK, dtype=jnp.float32)
    distance = offsets[:, None] - offsets[None, :]
    rate_col = log_decay[:, None, None]
    inside = jnp.where(distance >= 0, jnp.exp(rate_col * jnp.maximum(distance, 0.0)), 0.0)
    query_scale = jnp.exp(log_decay[:, None] * (offsets + 1.0))[..., None]
    key_scale = jnp.exp(log_decay[:, None] * (BLOCK - 1.0 - offsets))[..., None]
    block_decay = jnp.exp(log_decay * BLOCK)[:, None, None]

    def to_blocks(arr):
        return arr.reshape(seq_count, head_count, block_count, BLOCK, arr.shape[-1]).transpose(2, 0, 1, 3, 4)

    def advance(memory, inputs):
        q_block, k_block, v_block = inputs
        qf = q_block.astype(jnp.float32)
        kf = k_block.astype(jnp.float32)
        vf = v_block.astype(jnp.float32)
        scores = jnp.einsum('shqd,shkd->shqk', qf, kf, precision=highest)
        weights = (scores * inside).astype(jnp.bfloat16)
        within = jnp.einsum('shqk,shkv->shqv', weights.astype(jnp.float32), vf, precision=highest)
        carried = jnp.einsum('shqd,shdv->shqv', qf * query_scale, memory, precision=highest)
        k_scaled = (kf * key_scale).astype(jnp.bfloat16)
        memory = memory * block_decay + jnp.einsum('shkd,shkv->shdv', k_scaled.astype(jnp.float32), vf, precision=highest)
        return (memory, within + carried)
    start_memory = jnp.zeros((seq_count, head_count, head_width, values.shape[-1]), jnp.float32)
    outputs = lax.scan(advance, start_memory, (to_blocks(queries), to_blocks(key_rows), to_blocks(values)))[1]
    return outputs.transpose(1, 2, 0, 3, 4).reshape(seq_count, head_count, length, values.shape[-1])

def reference(tokens, in_gain, query_weight, key_weight, value_weight, gate_weight, log_decay, norm_gain, out_weight, post_gain):
    seq_count, length, model_width = tokens.shape
    tok_f32 = tokens.astype(jnp.float32)
    normed = (tok_f32 * lax.rsqrt(lax.optimization_barrier(jnp.mean(tok_f32 * tok_f32, axis=-1, keepdims=True)) + rms_eps) * in_gain).astype(jnp.bfloat16)
    flat_rows = normed.reshape(seq_count * length, model_width)

    def project(weight_mat):
        result = jnp.dot(flat_rows, weight_mat, preferred_element_type=jnp.float32).astype(jnp.bfloat16)
        return result.reshape(seq_count, length, HEADS, HEAD_DIM).transpose(0, 2, 1, 3)
    positions = jnp.arange(length, dtype=jnp.int32)
    queries = rotate(project(query_weight), positions).astype(jnp.bfloat16)
    key_rows = (rotate(project(key_weight), positions) * HEAD_DIM ** (-0.5)).astype(jnp.bfloat16)
    values = project(value_weight)
    gating = jnp.dot(flat_rows, gate_weight, preferred_element_type=jnp.float32).astype(jnp.bfloat16)
    gating = gating.reshape(seq_count, length, RET_WIDTH)
    retained = retain(queries, key_rows, values, log_decay)
    center = lax.optimization_barrier(jnp.mean(retained, axis=-1, keepdims=True))
    spread = lax.optimization_barrier(jnp.mean(jnp.square(retained - center), axis=-1, keepdims=True))
    normal = ((retained - center) * lax.rsqrt(spread + group_eps)).transpose(0, 2, 1, 3).reshape(seq_count, length, RET_WIDTH)
    gated = (normal * norm_gain * jax.nn.silu(gating.astype(jnp.float32))).astype(jnp.bfloat16)
    premix = jnp.dot(gated.reshape(seq_count * length, RET_WIDTH), out_weight, preferred_element_type=jnp.float32)
    mixed = premix * lax.rsqrt(lax.optimization_barrier(jnp.mean(premix * premix, axis=-1, keepdims=True)) + rms_eps) * post_gain
    return mixed.astype(jnp.bfloat16).reshape(seq_count, length, model_width)
```

```python
import functools

import jax
import jax.numpy as jnp
import numpy as np
from jax import lax
from jax.experimental import pallas as pl
from jax.experimental.pallas import tpu as pltpu
from jax.sharding import PartitionSpec as P

HEAD_DIM = 128
SUB = 128
NY = 4
rms_eps = 1e-06
group_eps = 1e-05
rope_base = 10000.0
MESH = pl.DeviceIdType.MESH
F32 = jnp.float32
BF16 = jnp.bfloat16


def kernel(
    tp, sp,
    tok, gain_h, wq_h, wk_h, wv_h, wg_h, decay, ngain_h, wo_h, pgain_h, inv_h,
    out,
    gain, ngain, pgain, inv, tokv, gath, wkv, wqg, wo, cosv, sinv, mask, qs, ks, vs, gs,
    within, s1_out, s1_in, s2_out, s2_in, s3_out, carry, excl, g_out, g_in, premix, outv,
    x_send, p_send, t_recv, s1_send, s1_recv, s2_send, s2_recv, s3_send, s3_recv,
    g_send, g_recv, w_sem, in_sem, o_sem,
):
    seqs, rows, width = tok.shape
    length = rows * tp
    chips = tp // 2
    pair = 2 * rows
    nz = sp // NY
    part = HEAD_DIM // NY
    s, t = lax.axis_index("sp"), lax.axis_index("tp")
    z, y = lax.div(s, NY), lax.rem(s, NY)
    chip, core = lax.div(t, 2), lax.rem(t, 2)
    other = chip * 2 + 1 - core
    left, right, far = lax.rem(chip + 3, chips), lax.rem(chip + 1, chips), lax.rem(chip + 2, chips)
    relay_from, relay_to = lax.rem(chip + 3 + 2 * core, chips), lax.rem(chip + 1 + 2 * core, chips)

    loads_in = [pltpu.make_async_copy(tok.at[q], tokv.at[q], in_sem.at[q]) for q in range(seqs)]
    for load in loads_in:
        load.start()
    halves = (slice(0, HEAD_DIM), slice(HEAD_DIM, 2 * HEAD_DIM))
    loads = [
        pltpu.make_async_copy(a, b, w_sem.at[i])
        for i, (a, b) in enumerate(
            (
                (gain_h, gain), (inv_h, inv), (ngain_h, ngain), (pgain_h, pgain),
                (wk_h, wkv.at[:, halves[0]]), (wv_h, wkv.at[:, halves[1]]),
                (wq_h, wqg.at[:, halves[0]]), (wg_h, wqg.at[:, halves[1]]), (wo_h, wo),
            )
        )
    ]
    for load in loads:
        load.start()

    barrier = pltpu.get_barrier_semaphore()
    for j in range(1, tp):
        pl.semaphore_signal(
            barrier, inc=1, device_id={"tp": lax.rem(t + j, tp)}, device_id_type=MESH
        )
    for j in range(1, NY):
        pl.semaphore_signal(
            barrier, inc=1, device_id={"sp": z * NY + lax.rem(y + j, NY)}, device_id_type=MESH
        )
    for j in range(1, nz):
        pl.semaphore_signal(
            barrier, inc=1, device_id={"sp": lax.rem(z + j, nz) * NY + y}, device_id_type=MESH
        )

    def at_rows(who, n):
        return pl.ds(pl.multiple_of(who * n, n), n)

    loads[0].wait()
    for load in loads_in:
        load.wait()

    def normalise(i, _):
        q, at = lax.div(i, rows // 16), pl.multiple_of(lax.rem(i, rows // 16) * 16, 16)
        x = tokv[q, pl.ds(at, 16), :].astype(F32)
        scale = lax.rsqrt(jnp.mean(x * x, axis=-1, keepdims=True) + rms_eps)
        gath[q, pl.ds(pl.multiple_of(t * rows + at, 16), 16), :] = (x * scale * gain[...]).astype(BF16)
        return 0

    lax.fori_loop(0, seqs * (rows // 16), normalise, 0, unroll=2)
    pl.semaphore_wait(barrier, tp - 1 + NY - 1 + nz - 1)

    def block_copy(q, who, dest, sem):
        return pltpu.make_async_remote_copy(
            gath.at[q, at_rows(who, rows), :], gath.at[q, at_rows(who, rows), :],
            sem, t_recv.at[q, who], device_id={"tp": dest}, device_id_type=MESH,
        )

    def to_right(q):
        return block_copy(q, t, right * 2 + core, x_send.at[q, 0])

    def to_left(q):
        return block_copy(q, t, left * 2 + core, x_send.at[q, 1])

    def relay(q):
        return block_copy(q, relay_from * 2 + core, relay_to * 2 + core, x_send.at[q, 2])

    def to_core(q, k):
        return block_copy(q, k * 2 + core, other, p_send.at[q, k])

    def arrived(q, who):
        block_copy(q, who, other, x_send.at[q, 0]).wait_recv()

    def send_own(q):
        to_right(q).start()
        to_left(q).start()
        to_core(q, chip).start()

    send_own(0)
    send_own(1)

    loads[1].wait()
    place = (s * length + lax.broadcasted_iota(jnp.int32, (length, HEAD_DIM), 0)).astype(F32)
    angle = place * inv[...]
    cosv[...] = jnp.cos(angle)
    lane = lax.broadcasted_iota(jnp.int32, (length, HEAD_DIM), 1)
    sine = jnp.sin(angle)
    sinv[...] = jnp.where(lane < HEAD_DIM // 2, -sine, sine)

    def fill(i, _):
        at = pl.multiple_of(i * 32, 32)
        gap = (
            at + lax.broadcasted_iota(jnp.int32, (32, length), 0)
            - lax.broadcasted_iota(jnp.int32, (32, length), 1)
        )
        weight = jnp.exp(decay[0] * jnp.maximum(gap, 0).astype(F32))
        mask[pl.ds(at, 32), :] = jnp.where(gap >= 0, weight, 0.0)
        return 0

    lax.fori_loop(0, length // 32, fill, 0)
    for load in loads[2:]:
        load.wait()

    def rotate(x, span):
        x = x.astype(BF16).astype(F32)
        return x * cosv[span, :] + pltpu.roll(x, HEAD_DIM // 2, 1) * sinv[span, :]

    def project_kv(q, k):
        span = at_rows(k, pair)
        r = jnp.dot(gath[q, span, :], wkv[...], preferred_element_type=F32)
        ks[q, span, :] = (rotate(r[:, halves[0]], span) * HEAD_DIM ** (-0.5)).astype(BF16)
        vs[q, span, :] = r[:, halves[1]].astype(BF16)

    def project_qg(q, k):
        span = at_rows(k, pair)
        r = jnp.dot(gath[q, span, :], wqg[...], preferred_element_type=F32)
        qs[q, span, :] = rotate(r[:, halves[0]], span).astype(BF16)
        gs[q, span, :] = r[:, halves[1]].astype(BF16)

    def power(n):
        return jnp.exp(jnp.full((1, 1), decay[0] * n, F32))

    def s1_copy(q, j):
        peer = lax.rem(y + j, NY)
        return pltpu.make_async_remote_copy(
            s1_out.at[q, at_rows(peer, part), :], s1_in.at[q, y],
            s1_send.at[q, j], s1_recv.at[q, y],
            device_id={"sp": z * NY + peer}, device_id_type=MESH,
        )

    def s1_wait(q, j):
        peer = lax.rem(y + j, NY)
        pltpu.make_async_remote_copy(
            s1_out.at[q, at_rows(peer, part), :], s1_in.at[q, peer],
            s1_send.at[q, j], s1_recv.at[q, peer],
            device_id={"sp": z * NY + peer}, device_id_type=MESH,
        ).wait_recv()

    def make_state(q):
        spot = lax.broadcasted_iota(jnp.int32, (length, HEAD_DIM), 0)
        fade = jnp.exp(decay[0] * (length - 1 - spot).astype(F32))
        scaled = (ks[q].astype(F32) * fade).astype(BF16)
        total = lax.dot_general(
            scaled, vs[q], (((0,), (0,)), ((), ())), preferred_element_type=F32
        )
        s1_out[q] = total.astype(BF16)
        for j in range(1, NY):
            s1_copy(q, j).start()
        s1_in[q, y] = s1_out[q, at_rows(y, part), :]

    def s2_copy(q, d):
        return pltpu.make_async_remote_copy(
            s2_out.at[q], s2_in.at[q, d], s2_send.at[q, d], s2_recv.at[q, d],
            device_id={"sp": lax.rem(z + d, nz) * NY + y}, device_id_type=MESH,
        )

    def plane_total(q):
        for j in range(1, NY):
            s1_wait(q, j)
        step = power(length)
        total = s1_in[q, 0].astype(F32)
        for k in range(1, NY):
            total = total * step + s1_in[q, k].astype(F32)
        s2_out[q] = total.astype(BF16)
        for d in range(1, nz):
            @pl.when(z + d < nz)
            def _():
                s2_copy(q, d).start()

    def s3_copy(q, j):
        peer = lax.rem(y + j, NY)
        return pltpu.make_async_remote_copy(
            s3_out.at[q, peer], excl.at[q, at_rows(y, part), :],
            s3_send.at[q, j], s3_recv.at[q, y],
            device_id={"sp": z * NY + peer}, device_id_type=MESH,
        )

    def s3_wait(q, j):
        peer = lax.rem(y + j, NY)
        pltpu.make_async_remote_copy(
            s3_out.at[q, peer], excl.at[q, at_rows(peer, part), :],
            s3_send.at[q, j], s3_recv.at[q, peer],
            device_id={"sp": z * NY + peer}, device_id_type=MESH,
        ).wait_recv()

    def hand_back(q):
        carry[...] = jnp.zeros_like(carry)
        for d in range(1, nz):
            @pl.when(z >= d)
            def _():
                s2_copy(q, d).wait_recv()
                carry[...] += power(length * NY * (d - 1)) * s2_in[q, d].astype(F32)
        step = power(length)
        before = carry[...]
        for k in range(NY):
            s3_out[q, k] = before.astype(BF16)
            before = before * step + s1_in[q, k].astype(F32)
        for j in range(1, NY):
            s3_copy(q, j).start()
        excl[q, at_rows(y, part), :] = s3_out[q, y]

    def inside(q):
        for i in range(length // SUB):
            here, upto = slice(i * SUB, (i + 1) * SUB), slice(0, (i + 1) * SUB)
            score = lax.dot_general(
                qs[q, here, :], ks[q, upto, :],
                (((1,), (1,)), ((), ())), preferred_element_type=F32,
            )
            weight = (score * mask[here, upto]).astype(BF16)
            within[q, here, :] = jnp.dot(weight, vs[q, upto, :], preferred_element_type=F32)

    def gated_copy(q, dest, source):
        return pltpu.make_async_remote_copy(
            g_out.at[q, at_rows(dest, rows), :],
            g_in.at[q, :, at_rows(source, HEAD_DIM)],
            g_send.at[q, dest], g_recv.at[q, source],
            device_id={"tp": dest}, device_id_type=MESH,
        )

    def finish(q):
        for j in range(1, NY):
            s3_wait(q, j)
        memory = excl[q]
        for k in (far, left, right, chip):
            here = at_rows(k, pair)
            spot = k * pair + 1 + lax.broadcasted_iota(jnp.int32, (pair, HEAD_DIM), 0)
            reach = jnp.exp(decay[0] * spot.astype(F32))
            query = (qs[q, here, :].astype(F32) * reach).astype(BF16)
            kept = within[q, here, :] + jnp.dot(query, memory, preferred_element_type=F32)
            kept = kept - jnp.mean(kept, axis=-1, keepdims=True)
            spread = jnp.mean(kept * kept, axis=-1, keepdims=True)
            normal = kept * lax.rsqrt(spread + group_eps) * ngain[...]
            gate = gs[q, here, :].astype(F32)
            g_out[q, here, :] = (normal * (gate * jax.nn.sigmoid(gate))).astype(BF16)
            if k is chip:
                gated_copy(q, other, t).start()
                g_in[q, :, at_rows(t, HEAD_DIM)] = g_out[q, at_rows(t, rows), :]
            else:
                gated_copy(q, k * 2 + core, t).start()
                gated_copy(q, k * 2 + 1 - core, t).start()

    def gated_wait(q):
        for j in range(1, tp):
            source = lax.rem(t + j, tp)
            gated_copy(q, other, source).wait_recv()

    def emit(lo, hi):
        n = (hi - lo) * rows
        for q in range(lo, hi):
            gated_wait(q)
        step = 512
        g = g_in[lo:hi].reshape(n, g_in.shape[2])
        for c in range(width // step):
            cut = slice(c * step, (c + 1) * step)
            premix[0:n, cut] = jnp.dot(g, wo[:, cut], preferred_element_type=F32)

        def norm(i, _):
            at = pl.multiple_of(i * 16, 16)
            x = premix[pl.ds(at, 16), :]
            scale = lax.rsqrt(jnp.mean(x * x, axis=-1, keepdims=True) + rms_eps)
            q = lo + lax.div(i, rows // 16)
            to = pl.multiple_of(lax.rem(i, rows // 16) * 16, 16)
            outv[q, pl.ds(to, 16), :] = (x * scale * pgain[...]).astype(BF16)
            return 0

        lax.fori_loop(0, n // 16, norm, 0, unroll=2)
        for q in range(lo, hi):
            pltpu.make_async_copy(outv.at[q], out.at[q], o_sem.at[q]).start()

    def take(q):
        arrived(q, relay_from * 2 + core)
        relay(q).start()

    def spread_on(q):
        to_core(q, relay_from).start()
        arrived(q, relay_to * 2 + core)
        to_core(q, relay_to).start()

    def near(q):
        arrived(q, other)
        project_kv(q, chip)
        project_qg(q, chip)
        arrived(q, left * 2 + 1 - core)
        project_kv(q, left)
        project_qg(q, left)
        arrived(q, right * 2 + 1 - core)
        project_kv(q, right)
        project_qg(q, right)

    take(0)
    send_own(2)
    spread_on(0)
    near(0)

    def step(q, _):
        @pl.when(q < seqs - 1)
        def _():
            take(q + 1)

            @pl.when(q < seqs - 3)
            def _():
                send_own(q + 3)

            spread_on(q + 1)

        arrived(q, far * 2 + core)
        to_core(q, far).start()

        @pl.when(q > 0)
        def _():
            hand_back(q - 1)

        arrived(q, far * 2 + 1 - core)
        project_kv(q, far)
        make_state(q)
        project_qg(q, far)
        inside(q)

        @pl.when(q < seqs - 1)
        def _():
            plane_total(q)
            near(q + 1)
        return 0

    lax.fori_loop(0, seqs, step, 0)
    end = seqs - 1
    finish(0)
    plane_total(end)

    def rest(q, _):
        finish(q)
        return 0

    lax.fori_loop(1, end, rest, 0)
    hand_back(end)
    emit(0, end)
    finish(end)
    emit(end, seqs)

    def drain(q, _):
        to_right(q).wait_send()
        to_left(q).wait_send()
        relay(q).wait_send()
        for k in range(chips):
            to_core(q, k).wait_send()
        for j in range(1, NY):
            s1_copy(q, j).wait_send()
            s3_copy(q, j).wait_send()
        for d in range(1, nz):
            @pl.when(z + d < nz)
            def _():
                s2_copy(q, d).wait_send()
        for j in range(1, tp):
            gated_copy(q, lax.rem(t + j, tp), t).wait_send()
        return 0

    lax.fori_loop(0, seqs, drain, 0)
    for q in range(seqs):
        pltpu.make_async_copy(outv.at[q], out.at[q], o_sem.at[q]).wait()


def hand_over(source, out, held, in_sem, out_sem):
    pieces = range(source.shape[0])
    into = [pltpu.make_async_copy(source.at[i], held.at[i], in_sem.at[i]) for i in pieces]
    back = [pltpu.make_async_copy(held.at[i], out.at[i], out_sem.at[i]) for i in pieces]
    for copy in into:
        copy.start()
    for i in pieces:
        into[i].wait()
        back[i].start()
    for copy in back:
        copy.wait()


def solution(mesh):
    tp, sp = mesh.shape["tp"], mesh.shape["sp"]

    def body(tok, gain, wq, wk, wv, wg, decay, ngain, wo, pgain):
        seqs, rows, width = tok.shape
        cols = wq.shape[1]
        length = rows * tp
        nz = sp // NY
        part = HEAD_DIM // NY
        half = HEAD_DIM // 2
        inv = np.float32(rope_base) ** (-np.arange(half, dtype=np.float32) / half)
        inv = jnp.asarray(np.concatenate([inv, inv])[None, :], F32)
        dma = pltpu.SemaphoreType.DMA
        hbm = pl.BlockSpec(memory_space=pltpu.HBM)
        vmem = pltpu.VMEM
        wide = vmem((seqs, length, cols), BF16)
        mixed = pl.pallas_call(
            functools.partial(kernel, tp, sp),
            out_shape=jax.ShapeDtypeStruct(tok.shape, BF16),
            in_specs=[
                hbm, hbm, hbm, hbm, hbm, hbm,
                pl.BlockSpec(memory_space=pltpu.SMEM), hbm, hbm, hbm, hbm,
            ],
            out_specs=hbm,
            scratch_shapes=[
                vmem((1, width), F32), vmem((1, cols), F32),
                vmem((1, width), F32), vmem((1, HEAD_DIM), F32),
                vmem(tok.shape, BF16),
                vmem((seqs, length, width), BF16),
                vmem((width, 2 * cols), BF16), vmem((width, 2 * cols), BF16),
                vmem(wo.shape, BF16),
                vmem((length, HEAD_DIM), F32), vmem((length, HEAD_DIM), F32),
                vmem((length, length), F32),
                wide, wide, wide, wide,
                vmem((seqs, length, cols), F32),
                vmem((seqs, HEAD_DIM, HEAD_DIM), BF16),
                vmem((seqs, NY, part, HEAD_DIM), BF16),
                vmem((seqs, part, HEAD_DIM), BF16),
                vmem((seqs, nz, part, HEAD_DIM), BF16),
                vmem((seqs, NY, part, HEAD_DIM), BF16),
                vmem((part, HEAD_DIM), F32),
                vmem((seqs, HEAD_DIM, HEAD_DIM), BF16),
                wide,
                vmem((seqs, rows, cols * tp), BF16),
                vmem((seqs * rows, width), F32),
                vmem(tok.shape, BF16),
                dma((seqs, 3)), dma((seqs, tp)), dma((seqs, tp)),
                dma((seqs, NY)), dma((seqs, NY)), dma((seqs, nz)), dma((seqs, nz)),
                dma((seqs, NY)), dma((seqs, NY)),
                dma((seqs, tp)), dma((seqs, tp)),
                dma((9,)), dma((seqs,)), dma((seqs,)),
            ],
            compiler_params=pltpu.CompilerParams(
                collective_id=0, has_side_effects=True, vmem_limit_bytes=59 * 2**20
            ),
            name="retention",
        )(
            tok, gain[None, :], wq, wk, wv, wg, decay, ngain[None, :], wo, pgain[None, :], inv
        )
        return pl.pallas_call(
            hand_over,
            out_shape=jax.ShapeDtypeStruct(tok.shape, BF16),
            in_specs=[hbm],
            out_specs=hbm,
            scratch_shapes=[pltpu.VMEM(tok.shape, BF16), dma((seqs,)), dma((seqs,))],
            compiler_params=pltpu.CompilerParams(vmem_limit_bytes=59 * 2**20),
            name="hand_over",
        )(mixed)

    placed = (
        P(None, ("sp", "tp"), None),
        P(),
        P(None, "tp"),
        P(None, "tp"),
        P(None, "tp"),
        P(None, "tp"),
        P("tp"),
        P("tp"),
        P(),
        P(),
    )
    return jax.shard_map(
        body, mesh=mesh, in_specs=placed, out_specs=P(None, ("sp", "tp"), None), check_vma=False
    )
```

```python
import functools

import jax
import jax.numpy as jnp
import numpy as np
from jax import lax
from jax.experimental import pallas as pl
from jax.experimental.pallas import tpu as pltpu
from jax.sharding import PartitionSpec as P

HEAD_DIM = 128
SUB = 128
NY = 4
rms_eps = 1e-06
group_eps = 1e-05
rope_base = 10000.0
MESH = pl.DeviceIdType.MESH
F32 = jnp.float32
BF16 = jnp.bfloat16


def kernel(
    tp, sp,
    tok, gain_h, wq_h, wk_h, wv_h, wg_h, decay, ngain_h, wo_h, pgain_h, inv_h,
    out,
    gain, pgain, inv, heads, tokv, gath, w, wo, cosv, sinv, mask, fade, reach,
    qs, qr, ks, vs, sg, within, s1_out, s1_in, s2_out, s2_in, s3_out, carry, excl,
    g_out, g_in, premix, outv,
    x_send, p_send, t_recv, wx_send, wx_recv, wy_send, wy_recv, h_send, h_recv,
    s1_send, s1_recv, s2_send, s2_recv, s3_send, s3_recv, g_send, g_recv,
    w_sem, o_sem, in_sem, out_sem,
):
    seqs, rows, width = tok.shape
    pair = 2 * rows
    length = 2 * pair
    line = rows * tp
    nz = sp // NY
    part = HEAD_DIM // NY
    direct = width // 4
    piece = (width - direct) // NY
    s, t = lax.axis_index("sp"), lax.axis_index("tp")
    z, y = lax.div(s, NY), lax.rem(s, NY)
    chip, core = lax.div(t, 2), lax.rem(t, 2)
    group, side = lax.div(chip, 2), lax.rem(chip, 2)
    base = group * 4
    me = side * 2 + core
    twin = side * 2 + 1 - core
    across = (1 - side) * 2 + core
    across_twin = (1 - side) * 2 + 1 - core
    mirror = (3 - chip) * 2 + core
    slot = y * 2 + group

    loads_in = [pltpu.make_async_copy(tok.at[q], tokv.at[q], in_sem.at[q]) for q in range(seqs)]
    cuts = [slice(i * HEAD_DIM, (i + 1) * HEAD_DIM) for i in range(4)]
    loads_w = [
        pltpu.make_async_copy(a, w.at[0, :, cuts[i]], w_sem.at[i])
        for i, a in enumerate((wk_h, wv_h, wq_h, wg_h))
    ]
    loads = [
        pltpu.make_async_copy(a, b, w_sem.at[4 + i])
        for i, (a, b) in enumerate(
            ((ngain_h, heads.at[0, 1:2, :]), (gain_h, gain), (inv_h, inv), (pgain_h, pgain))
        )
    ]

    def head_of(u, flip):
        c = group * 2 + u // 2
        return ((3 - c) if flip else c) * 2 + u % 2

    loads_o = [
        pltpu.make_async_copy(
            wo_h.at[pl.ds(pl.multiple_of(head_of(i // 2, i % 2) * HEAD_DIM, HEAD_DIM), HEAD_DIM), :],
            wo.at[i * HEAD_DIM:(i + 1) * HEAD_DIM, :], o_sem.at[i],
        )
        for i in range(8)
    ]
    for load in loads_w + loads_in + loads + loads_o:
        load.start()

    barrier = pltpu.get_barrier_semaphore()

    def greet(dest):
        pl.semaphore_signal(barrier, inc=1, device_id=dest, device_id_type=MESH)

    for u in (twin, across, across_twin):
        greet({"tp": base + u})
    for j in range(1, NY):
        greet({"sp": z * NY + lax.rem(y + j, NY)})
    for j in range(NY):
        greet({"sp": z * NY + lax.rem(y + j, NY), "tp": mirror})
    for j in range(1, nz):
        greet({"sp": lax.rem(z + j, nz) * NY + y})

    def at_rows(who, n):
        return pl.ds(pl.multiple_of(who * n, n), n)

    def cross(i):
        span = pl.ds(pl.multiple_of(direct + y * piece, 128), piece)
        return pltpu.make_async_remote_copy(
            w.at[0, span, cuts[i]], w.at[1, span, cuts[i]], wx_send.at[0, i], wx_recv.at[0, i],
            device_id={"tp": mirror}, device_id_type=MESH,
        )

    def straight(i):
        return pltpu.make_async_remote_copy(
            w.at[0, 0:direct, cuts[i]], w.at[1, 0:direct, cuts[i]],
            wx_send.at[1, i], wx_recv.at[1, i],
            device_id={"tp": mirror}, device_id_type=MESH,
        )

    def along(i, j, mine):
        peer = lax.rem(y + j, NY)
        owner = y if mine else peer
        span = pl.ds(pl.multiple_of(direct + owner * piece, 128), piece)
        return pltpu.make_async_remote_copy(
            w.at[1, span, cuts[i]], w.at[1, span, cuts[i]], wy_send.at[i, j], wy_recv.at[i, owner],
            device_id={"sp": z * NY + peer}, device_id_type=MESH,
        )

    def pass_on(i):
        cross(i).wait_recv()
        for j in range(1, NY):
            along(i, j, True).start()

    def have(i):
        straight(i).wait_recv()
        for j in range(1, NY):
            along(i, j, False).wait_recv()

    def head_copy():
        return pltpu.make_async_remote_copy(
            heads.at[0], heads.at[1], h_send, h_recv, device_id={"tp": mirror}, device_id_type=MESH,
        )

    loads[0].wait()
    heads[0, 0:1, :] = jnp.full((1, HEAD_DIM), decay[0], F32)
    for load in loads_w:
        load.wait()
    with jax.named_scope("barrier"):
        pl.semaphore_wait(barrier, 3 + NY - 1 + NY + nz - 1)
    for i in range(4):
        cross(i).start()
    for i in range(4):
        straight(i).start()
    head_copy().start()

    def block_copy(q, u, dest, sem):
        return pltpu.make_async_remote_copy(
            gath.at[q, at_rows(u, rows), :], gath.at[q, at_rows(u, rows), :],
            sem, t_recv.at[q, u], device_id={"tp": base + dest}, device_id_type=MESH,
        )

    def to_across(q):
        return block_copy(q, me, across, x_send.at[q])

    def to_twin(q, own):
        return block_copy(q, me if own else across, twin, p_send.at[q, 0 if own else 1])

    def arrived(q, u):
        block_copy(q, u, twin, x_send.at[q]).wait_recv()

    def normalise(q):
        def norm(i, _):
            at = pl.multiple_of(i * 16, 16)
            x = tokv[q, pl.ds(at, 16), :].astype(F32)
            scale = lax.rsqrt(jnp.mean(x * x, axis=-1, keepdims=True) + rms_eps)
            to = pl.ds(pl.multiple_of(me * rows + at, 16), 16)
            gath[q, to, :] = (x * scale * gain[...]).astype(BF16)
            return 0

        lax.fori_loop(0, rows // 16, norm, 0, unroll=2)

    def send(q):
        to_across(q).start()
        to_twin(q, True).start()

    with jax.named_scope("norm"):
        loads[1].wait()
        for q in range(seqs):
            loads_in[q].wait()
            normalise(q)
            if q > 0:
                send(q - 1)
        send(seqs - 1)

    with jax.named_scope("tables"):
        loads[2].wait()
        place = s * line + group * length + lax.broadcasted_iota(jnp.int32, (length, HEAD_DIM), 0)
        angle = place.astype(F32) * inv[...]
        cosv[...] = jnp.cos(angle)
        lane = lax.broadcasted_iota(jnp.int32, (length, HEAD_DIM), 1)
        sine = jnp.sin(angle)
        sinv[...] = jnp.where(lane < HEAD_DIM // 2, -sine, sine)

    def tables(h):
        rate = heads[h, 0:1, :]
        spot = lax.broadcasted_iota(jnp.int32, (length, HEAD_DIM), 0)
        fade[h] = jnp.exp(rate * (length - 1 - spot).astype(F32))
        reach[h] = jnp.exp(rate * (1 + spot).astype(F32))
        for c in range(length // HEAD_DIM):
            gap = spot - c * HEAD_DIM - lax.broadcasted_iota(jnp.int32, (length, HEAD_DIM), 1)
            weight = jnp.exp(rate * jnp.maximum(gap, 0).astype(F32))
            mask[h, :, c * HEAD_DIM:(c + 1) * HEAD_DIM] = jnp.where(gap >= 0, weight, 0.0)

    with jax.named_scope("tables0"):
        tables(0)

    def rotate(x, span):
        x = x.astype(BF16).astype(F32)
        return x * cosv[span, :] + pltpu.roll(x, HEAD_DIM // 2, 1) * sinv[span, :]

    def project_kv(h, q, span):
        r = jnp.dot(gath[q, span, :], w[h, :, 0:256], preferred_element_type=F32)
        ks[h, q, span, :] = (rotate(r[:, cuts[0]], span) * HEAD_DIM ** (-0.5)).astype(BF16)
        vs[h, q, span, :] = r[:, cuts[1]].astype(BF16)

    def project_qg(h, q, span):
        r = jnp.dot(gath[q, span, :], w[h, :, 256:512], preferred_element_type=F32)
        query = rotate(r[:, cuts[0]], span).astype(BF16)
        qs[h, q, span, :] = query
        qr[h, q, span, :] = (query.astype(F32) * reach[h, span, :]).astype(BF16)
        gate = r[:, cuts[1]].astype(BF16).astype(F32)
        sg[h, q, span, :] = heads[h, 1:2, :] * (gate * jax.nn.sigmoid(gate))

    everything = slice(0, length)
    own_rows = at_rows(side, pair)
    far_rows = at_rows(1 - side, pair)

    def power(n):
        return jnp.exp(jnp.full((1, 1), decay[0] * n, F32))

    def s1_copy(q, h, j, mine):
        peer = lax.rem(y + j, NY)
        dest = {"sp": z * NY + peer, "tp": mirror} if h else {"sp": z * NY + peer}
        arrival = slot if mine else peer * 2 + (1 - group if h else group)
        return pltpu.make_async_remote_copy(
            s1_out.at[h, q, at_rows(peer, part), :], s1_in.at[q, arrival],
            s1_send.at[h, q, j], s1_recv.at[q, arrival], device_id=dest, device_id_type=MESH,
        )

    def make_state(q):
        for h in range(2):
            scaled = (ks[h, q].astype(F32) * fade[h]).astype(BF16)
            total = lax.dot_general(
                scaled, vs[h, q], (((0,), (0,)), ((), ())), preferred_element_type=F32
            )
            s1_out[h, q] = total.astype(BF16)
        for j in range(NY):
            s1_copy(q, 1, j, True).start()
            if j:
                s1_copy(q, 0, j, True).start()
        s1_in[q, slot] = s1_out[0, q, at_rows(y, part), :]

    def s2_copy(q, d):
        return pltpu.make_async_remote_copy(
            s2_out.at[q], s2_in.at[q, d], s2_send.at[q, d], s2_recv.at[q, d],
            device_id={"sp": lax.rem(z + d, nz) * NY + y}, device_id_type=MESH,
        )

    def plane_total(q):
        for j in range(NY):
            s1_copy(q, 1, j, False).wait_recv()
            if j:
                s1_copy(q, 0, j, False).wait_recv()
        step = power(length)
        total = s1_in[q, 0].astype(F32)
        for k in range(1, 2 * NY):
            total = total * step + s1_in[q, k].astype(F32)
        s2_out[q] = total.astype(BF16)
        for d in range(1, nz):
            @pl.when(z + d < nz)
            def _():
                s2_copy(q, d).start()

    def s3_copy(q, h, j, mine):
        peer = lax.rem(y + j, NY)
        dest = {"sp": z * NY + peer, "tp": mirror} if h else {"sp": z * NY + peer}
        owner = y if mine else peer
        return pltpu.make_async_remote_copy(
            s3_out.at[q, peer * 2 + (1 - group if h else group)],
            excl.at[h, q, at_rows(owner, part), :],
            s3_send.at[h, q, j], s3_recv.at[h, q, owner], device_id=dest, device_id_type=MESH,
        )

    def hand_back(q):
        carry[...] = jnp.zeros_like(carry)
        for d in range(1, nz):
            @pl.when(z >= d)
            def _():
                s2_copy(q, d).wait_recv()
                carry[...] += power(line * NY * (d - 1)) * s2_in[q, d].astype(F32)
        step = power(length)
        before = carry[...]
        for k in range(2 * NY):
            s3_out[q, k] = before.astype(BF16)
            before = before * step + s1_in[q, k].astype(F32)
        for j in range(NY):
            s3_copy(q, 1, j, True).start()
            if j:
                s3_copy(q, 0, j, True).start()
        excl[0, q, at_rows(y, part), :] = s3_out[q, slot]

    def inside(q):
        for h in range(2):
            for i in range(length // SUB):
                here, upto = slice(i * SUB, (i + 1) * SUB), slice(0, (i + 1) * SUB)
                score = lax.dot_general(
                    qs[h, q, here, :], ks[h, q, upto, :],
                    (((1,), (1,)), ((), ())), preferred_element_type=F32,
                )
                weight = (score * mask[h, here, upto]).astype(BF16)
                within[h, q, here, :] = jnp.dot(
                    weight, vs[h, q, upto, :], preferred_element_type=F32
                )

    def gated_copy(q, dest, source):
        return pltpu.make_async_remote_copy(
            g_out.at[q, at_rows(dest, rows), :], g_in.at[q, :, at_rows(source, 2 * HEAD_DIM)],
            g_send.at[q, dest], g_recv.at[q, source],
            device_id={"tp": base + dest}, device_id_type=MESH,
        )

    def finish(q):
        for j in range(NY):
            s3_copy(q, 1, j, False).wait_recv()
            if j:
                s3_copy(q, 0, j, False).wait_recv()
        for k in range(2):
            here = at_rows((1 - side) if k == 0 else side, pair)
            for h in range(2):
                kept = within[h, q, here, :] + jnp.dot(
                    qr[h, q, here, :], excl[h, q], preferred_element_type=F32
                )
                kept = kept - jnp.mean(kept, axis=-1, keepdims=True)
                spread = jnp.mean(kept * kept, axis=-1, keepdims=True)
                normal = kept * lax.rsqrt(spread + group_eps) * sg[h, q, here, :]
                g_out[q, here, cuts[h]] = normal.astype(BF16)
            if k == 0:
                gated_copy(q, across, me).start()
                gated_copy(q, across_twin, me).start()
            else:
                gated_copy(q, twin, me).start()
                g_in[q, :, at_rows(me, 2 * HEAD_DIM)] = g_out[q, at_rows(me, rows), :]

    def gated_wait(q):
        for u in (twin, across, across_twin):
            gated_copy(q, twin, u).wait_recv()

    def emit(lo, hi):
        n = (hi - lo) * rows
        with jax.named_scope("gated_wait"):
            for q in range(lo, hi):
                gated_wait(q)
        step = 512
        g = g_in[lo:hi].reshape(n, g_in.shape[2])
        for c in range(width // step):
            cut = slice(c * step, (c + 1) * step)
            premix[0:n, cut] = jnp.dot(g, wo[:, cut], preferred_element_type=F32)

        def norm(i, _):
            at = pl.multiple_of(i * 16, 16)
            x = premix[pl.ds(at, 16), :]
            scale = lax.rsqrt(jnp.mean(x * x, axis=-1, keepdims=True) + rms_eps)
            q = lo + lax.div(i, rows // 16)
            to = pl.multiple_of(lax.rem(i, rows // 16) * 16, 16)
            outv[q, pl.ds(to, 16), :] = (x * scale * pgain[...]).astype(BF16)
            return 0

        lax.fori_loop(0, n // 16, norm, 0, unroll=2)
        for q in range(lo, hi):
            pltpu.make_async_copy(outv.at[q], out.at[q], out_sem.at[q]).start()

    def scoped(name, function, *args):
        with jax.named_scope(name):
            function(*args)

    def over(lo, hi, function):
        def run(q, _):
            function(q)
            return 0

        lax.fori_loop(lo, hi, run, 0)

    def near(q):
        arrived(q, twin)
        project_kv(0, q, own_rows)
        project_qg(0, q, own_rows)

    def take(q):
        with jax.named_scope("take"):
            arrived(q, across)
        to_twin(q, False).start()

    def rest(q):
        with jax.named_scope("take2"):
            arrived(q, across_twin)
        project_kv(0, q, far_rows)
        project_qg(0, q, far_rows)

    scoped("near01", over, 0, 2, near)
    scoped("pass0", pass_on, 0)
    scoped("near23", over, 2, seqs, near)
    scoped("pass1", pass_on, 1)
    with jax.named_scope("tables1"):
        head_copy().wait_recv()
        tables(1)
    for load in loads[3:] + loads_o:
        load.wait()
    scoped("pass2", pass_on, 2)
    take(0)
    scoped("pass3", pass_on, 3)
    scoped("rest0", rest, 0)
    take(1)
    scoped("rest1", rest, 1)
    with jax.named_scope("havekv"):
        have(0)
        have(1)

    def early(q):
        project_kv(1, q, everything)
        make_state(q)

    scoped("early", over, 0, 2, early)

    def lone(q):
        project_kv(1, q, own_rows)

    scoped("lone", over, 2, seqs, lone)
    scoped("plane0", plane_total, 0)
    take(2)
    scoped("plane1", plane_total, 1)
    scoped("rest2", rest, 2)
    project_kv(1, 2, far_rows)
    scoped("state2", make_state, 2)
    with jax.named_scope("haveqg"):
        have(2)
        have(3)

    def later(q):
        project_qg(1, q, everything)

    scoped("later", over, 0, seqs - 1, later)
    project_qg(1, seqs - 1, own_rows)
    scoped("back0", hand_back, 0)
    end = seqs - 1
    take(end)
    scoped("plane2", plane_total, 2)
    with jax.named_scope("rest3"):
        arrived(end, across_twin)
        for h in range(2):
            project_kv(h, end, far_rows)
        make_state(end)
    scoped("back1", hand_back, 1)
    with jax.named_scope("qg3"):
        for h in range(2):
            project_qg(h, end, far_rows)
    scoped("back2", hand_back, 2)
    scoped("inside01", over, 0, 2, inside)
    scoped("plane3", plane_total, end)
    scoped("inside23", over, 2, seqs, inside)
    scoped("finish01", over, 0, 2, finish)
    scoped("back3", hand_back, end)
    scoped("finish2", over, 2, end, finish)
    scoped("emit0", emit, 0, end)
    scoped("finish3", finish, end)
    scoped("emit3", emit, end, seqs)

    def drain(q):
        to_across(q).wait_send()
        to_twin(q, True).wait_send()
        to_twin(q, False).wait_send()
        for j in range(NY):
            s1_copy(q, 1, j, True).wait_send()
            s3_copy(q, 1, j, True).wait_send()
            if j:
                s1_copy(q, 0, j, True).wait_send()
                s3_copy(q, 0, j, True).wait_send()
        for d in range(1, nz):
            @pl.when(z + d < nz)
            def _():
                s2_copy(q, d).wait_send()
        for u in (twin, across, across_twin):
            gated_copy(q, u, me).wait_send()

    with jax.named_scope("drain"):
        over(0, seqs, drain)
        for i in range(4):
            cross(i).wait_send()
            straight(i).wait_send()
            for j in range(1, NY):
                along(i, j, True).wait_send()
        head_copy().wait_send()
        for q in range(seqs):
            pltpu.make_async_copy(outv.at[q], out.at[q], out_sem.at[q]).wait()


def hand_over(source, out, held, in_sem, out_sem):
    pieces = range(source.shape[0])
    into = [pltpu.make_async_copy(source.at[i], held.at[i], in_sem.at[i]) for i in pieces]
    back = [pltpu.make_async_copy(held.at[i], out.at[i], out_sem.at[i]) for i in pieces]
    for copy in into:
        copy.start()
    for i in pieces:
        into[i].wait()
        back[i].start()
    for copy in back:
        copy.wait()


def solution(mesh):
    tp, sp = mesh.shape["tp"], mesh.shape["sp"]

    def body(tok, gain, wq, wk, wv, wg, decay, ngain, wo, pgain):
        seqs, rows, width = tok.shape
        length = rows * 4
        nz = sp // NY
        part = HEAD_DIM // NY
        half = HEAD_DIM // 2
        inv = np.float32(rope_base) ** (-np.arange(half, dtype=np.float32) / half)
        inv = jnp.asarray(np.concatenate([inv, inv])[None, :], F32)
        dma = pltpu.SemaphoreType.DMA
        hbm = pl.BlockSpec(memory_space=pltpu.HBM)
        vmem = pltpu.VMEM
        wide = vmem((2, seqs, length, HEAD_DIM), BF16)
        mixed = pl.pallas_call(
            functools.partial(kernel, tp, sp),
            out_shape=jax.ShapeDtypeStruct(tok.shape, BF16),
            in_specs=[
                hbm, hbm, hbm, hbm, hbm, hbm,
                pl.BlockSpec(memory_space=pltpu.SMEM), hbm, hbm, hbm, hbm,
            ],
            out_specs=hbm,
            scratch_shapes=[
                vmem((1, width), F32), vmem((1, width), F32), vmem((1, HEAD_DIM), F32),
                vmem((2, 8, HEAD_DIM), F32),
                vmem(tok.shape, BF16),
                vmem((seqs, length, width), BF16),
                vmem((2, width, 4 * HEAD_DIM), BF16),
                vmem(wo.shape, BF16),
                vmem((length, HEAD_DIM), F32), vmem((length, HEAD_DIM), F32),
                vmem((2, length, length), F32),
                vmem((2, length, HEAD_DIM), F32), vmem((2, length, HEAD_DIM), F32),
                wide, wide, wide, wide,
                vmem((2, seqs, length, HEAD_DIM), F32),
                vmem((2, seqs, length, HEAD_DIM), F32),
                vmem((2, seqs, HEAD_DIM, HEAD_DIM), BF16),
                vmem((seqs, 2 * NY, part, HEAD_DIM), BF16),
                vmem((seqs, part, HEAD_DIM), BF16),
                vmem((seqs, nz, part, HEAD_DIM), BF16),
                vmem((seqs, 2 * NY, part, HEAD_DIM), BF16),
                vmem((part, HEAD_DIM), F32),
                vmem((2, seqs, HEAD_DIM, HEAD_DIM), BF16),
                vmem((seqs, length, 2 * HEAD_DIM), BF16),
                vmem((seqs, rows, HEAD_DIM * tp), BF16),
                vmem((seqs * rows, width), F32),
                vmem(tok.shape, BF16),
                dma((seqs,)), dma((seqs, 2)), dma((seqs, 4)),
                dma((2, 4)), dma((2, 4)), dma((4, NY)), dma((4, NY)),
                dma(()), dma(()),
                dma((2, seqs, NY)), dma((seqs, 2 * NY)), dma((seqs, nz)), dma((seqs, nz)),
                dma((2, seqs, NY)), dma((2, seqs, NY)),
                dma((seqs, 4)), dma((seqs, 4)),
                dma((8,)), dma((8,)), dma((seqs,)), dma((seqs,)),
            ],
            compiler_params=pltpu.CompilerParams(
                collective_id=0, has_side_effects=True, vmem_limit_bytes=59 * 2**20
            ),
            name="retention",
        )(
            tok, gain[None, :], wq, wk, wv, wg, decay, ngain[None, :], wo, pgain[None, :], inv
        )
        return pl.pallas_call(
            hand_over,
            out_shape=jax.ShapeDtypeStruct(tok.shape, BF16),
            in_specs=[hbm],
            out_specs=hbm,
            scratch_shapes=[pltpu.VMEM(tok.shape, BF16), dma((seqs,)), dma((seqs,))],
            compiler_params=pltpu.CompilerParams(vmem_limit_bytes=59 * 2**20),
            name="hand_over",
        )(mixed)

    placed = (
        P(None, ("sp", "tp"), None),
        P(),
        P(None, "tp"),
        P(None, "tp"),
        P(None, "tp"),
        P(None, "tp"),
        P("tp"),
        P("tp"),
        P(),
        P(),
    )
    return jax.shard_map(
        body, mesh=mesh, in_specs=placed, out_specs=P(None, ("sp", "tp"), None), check_vma=False
    )
```

```python
import functools

import jax
import jax.numpy as jnp
import numpy as np
from jax import lax
from jax.experimental import pallas as pl
from jax.experimental.pallas import tpu as pltpu
from jax.sharding import PartitionSpec as P

HEAD_DIM = 128
SUB = 128
NY = 4
rms_eps = 1e-06
group_eps = 1e-05
rope_base = 10000.0
MESH = pl.DeviceIdType.MESH
F32 = jnp.float32
BF16 = jnp.bfloat16


def kernel(
    tp, sp,
    tok, gain_h, wq_h, wk_h, wv_h, wg_h, decay, ngain_h, wo_h, pgain_h, inv_h,
    out,
    gain, pgain, inv, heads, tokv, gath, w, wo, cosv, sinv, mask, fade, reach,
    qs, qr, ks, vs, sg, within, s1_out, s1_in, s2_out, s2_in, s3_out, excl,
    g_out, g_in, premix, outv,
    x_send, p_send, t_recv, w_send, wx_recv, h_recv,
    s_send, s1_recv, s2_recv, s3_recv, g_send, g_recv,
    w_sem, o_sem, in_sem, out_sem,
):
    seqs, rows, width = tok.shape
    pair = 2 * rows
    length = 2 * pair
    line = rows * tp
    nz = sp // NY
    part = HEAD_DIM // NY
    direct = width // 4
    piece = (width - direct) // NY
    s, t = lax.axis_index("sp"), lax.axis_index("tp")
    z, y = lax.div(s, NY), lax.rem(s, NY)
    chip, core = lax.div(t, 2), lax.rem(t, 2)
    group, side = lax.div(chip, 2), lax.rem(chip, 2)
    base = group * 4
    me = side * 2 + core
    twin = side * 2 + 1 - core
    across = (1 - side) * 2 + core
    across_twin = (1 - side) * 2 + 1 - core
    mirror = (3 - chip) * 2 + core
    slot = y * 2 + group

    loads_in = [pltpu.make_async_copy(tok.at[q], tokv.at[q], in_sem.at[q]) for q in range(seqs)]
    cuts = [slice(i * HEAD_DIM, (i + 1) * HEAD_DIM) for i in range(4)]
    loads_w = [
        pltpu.make_async_copy(a, w.at[0, :, cuts[i]], w_sem.at[i])
        for i, a in enumerate((wk_h, wv_h, wq_h, wg_h))
    ]
    loads = [
        pltpu.make_async_copy(a, b, w_sem.at[4 + i])
        for i, (a, b) in enumerate(
            ((ngain_h, heads.at[0, 1:2, :]), (gain_h, gain), (inv_h, inv), (pgain_h, pgain))
        )
    ]

    def head_of(u, flip):
        c = group * 2 + u // 2
        return ((3 - c) if flip else c) * 2 + u % 2

    loads_o = [
        pltpu.make_async_copy(
            wo_h.at[pl.ds(pl.multiple_of(head_of(i // 2, i % 2) * HEAD_DIM, HEAD_DIM), HEAD_DIM), :],
            wo.at[i * HEAD_DIM:(i + 1) * HEAD_DIM, :], o_sem,
        )
        for i in range(8)
    ]
    for load in loads_in[:1] + loads[:3] + loads_in[1:] + loads_w + loads[3:] + loads_o:
        load.start()

    barrier = pltpu.get_barrier_semaphore()

    def greet(dest):
        pl.semaphore_signal(barrier, inc=1, device_id=dest, device_id_type=MESH)

    for u in (twin, across, across_twin):
        greet({"tp": base + u})
    for j in range(1, NY):
        greet({"sp": z * NY + lax.rem(y + j, NY)})
    for j in range(NY):
        greet({"sp": z * NY + lax.rem(y + j, NY), "tp": mirror})
    for j in range(1, nz):
        greet({"sp": lax.rem(z + j, nz) * NY + y})

    def at_rows(who, n):
        return pl.ds(pl.multiple_of(who * n, n), n)

    def cross(i):
        span = pl.ds(pl.multiple_of(direct + y * piece, 128), piece)
        return pltpu.make_async_remote_copy(
            w.at[0, span, cuts[i]], w.at[1, span, cuts[i]], w_send, wx_recv.at[i],
            device_id={"tp": mirror}, device_id_type=MESH,
        )

    def straight(i):
        return pltpu.make_async_remote_copy(
            w.at[0, 0:direct, cuts[i]], w.at[1, 0:direct, cuts[i]],
            w_send, wx_recv.at[4 + i // 2],
            device_id={"tp": mirror}, device_id_type=MESH,
        )

    def along(i, j):
        peer = lax.rem(y + j, NY)
        span = pl.ds(pl.multiple_of(direct + y * piece, 128), piece)
        return pltpu.make_async_remote_copy(
            w.at[1, span, cuts[i]], w.at[1, span, cuts[i]], w_send, wx_recv.at[4 + i // 2],
            device_id={"sp": z * NY + peer}, device_id_type=MESH,
        )

    def pass_on(i):
        cross(i).wait_recv()
        for j in range(1, NY):
            along(i, j).start()

    def have(k):
        took = w.at[1, 0:width - piece, 256 * k:256 * (k + 1)]
        pltpu.make_async_remote_copy(
            took, took, w_send, wx_recv.at[4 + k], device_id={"tp": mirror}, device_id_type=MESH,
        ).wait_recv()

    def head_copy():
        return pltpu.make_async_remote_copy(
            heads.at[0], heads.at[1], w_send, h_recv, device_id={"tp": mirror}, device_id_type=MESH,
        )

    def block_copy(q, u, dest, sem):
        return pltpu.make_async_remote_copy(
            gath.at[q, at_rows(u, rows), :], gath.at[q, at_rows(u, rows), :],
            sem, t_recv.at[q, u], device_id={"tp": base + dest}, device_id_type=MESH,
        )

    def to_across(q):
        return block_copy(q, me, across, x_send)

    def to_twin(q, own):
        return block_copy(q, me if own else across, twin, p_send)

    def arrived(q, u):
        block_copy(q, u, twin, x_send).wait_recv()

    def normalise(q):
        def norm(i, _):
            at = pl.multiple_of(i * 16, 16)
            x = tokv[q, pl.ds(at, 16), :].astype(F32)
            scale = lax.rsqrt(jnp.mean(x * x, axis=-1, keepdims=True) + rms_eps)
            to = pl.ds(pl.multiple_of(me * rows + at, 16), 16)
            gath[q, to, :] = (x * scale * gain[...]).astype(BF16)
            return 0

        lax.fori_loop(0, rows // 16, norm, 0, unroll=2)

    def send(q):
        to_across(q).start()
        to_twin(q, True).start()

    with jax.named_scope("norm"):
        loads[0].wait()
        heads[0, 0:1, :] = jnp.full((1, HEAD_DIM), decay[0], F32)
        loads[1].wait()
        for q in range(2):
            loads_in[q].wait()
            normalise(q)
    with jax.named_scope("barrier"):
        pl.semaphore_wait(barrier, 3 + NY - 1 + NY + nz - 1)
    send(0)
    head_copy().start()
    with jax.named_scope("norm2"):
        loads_in[2].wait()
        normalise(2)
        send(1)
        for i in range(4):
            loads_w[i].wait()
            cross(i).start()
        for i in range(4):
            straight(i).start()
        loads_in[3].wait()
        normalise(3)
        send(2)
        send(3)

    with jax.named_scope("tables"):
        loads[2].wait()
        place = s * line + group * length + lax.broadcasted_iota(jnp.int32, (length, HEAD_DIM), 0)
        angle = place.astype(F32) * inv[...]
        cosv[...] = jnp.cos(angle)
        lane = lax.broadcasted_iota(jnp.int32, (length, HEAD_DIM), 1)
        sine = jnp.sin(angle)
        sinv[...] = jnp.where(lane < HEAD_DIM // 2, -sine, sine)

    def tables(h):
        rate = heads[h, 0:1, :]
        spot = lax.broadcasted_iota(jnp.int32, (length, HEAD_DIM), 0)
        fade[h] = jnp.exp(rate * (length - 1 - spot).astype(F32))
        reach[h] = jnp.exp(rate * (1 + spot).astype(F32))
        for c in range(length // HEAD_DIM):
            gap = spot - c * HEAD_DIM - lax.broadcasted_iota(jnp.int32, (length, HEAD_DIM), 1)
            weight = jnp.exp(rate * jnp.maximum(gap, 0).astype(F32))
            mask[h, :, c * HEAD_DIM:(c + 1) * HEAD_DIM] = jnp.where(gap >= 0, weight, 0.0)

    with jax.named_scope("tables0"):
        tables(0)

    def rotate(x, span):
        x = x.astype(BF16).astype(F32)
        return x * cosv[span, :] + pltpu.roll(x, HEAD_DIM // 2, 1) * sinv[span, :]

    def project_kv(h, q, span):
        r = jnp.dot(gath[q, span, :], w[h, :, 0:256], preferred_element_type=F32)
        ks[h, q, span, :] = (rotate(r[:, cuts[0]], span) * HEAD_DIM ** (-0.5)).astype(BF16)
        vs[h, q, span, :] = r[:, cuts[1]].astype(BF16)

    def project_qg(h, q, span):
        r = jnp.dot(gath[q, span, :], w[h, :, 256:512], preferred_element_type=F32)
        query = rotate(r[:, cuts[0]], span).astype(BF16)
        qs[h, q, span, :] = query
        qr[h, q, span, :] = (query.astype(F32) * reach[h, span, :]).astype(BF16)
        gate = r[:, cuts[1]].astype(BF16).astype(F32)
        sg[h, q, span, :] = heads[h, 1:2, :] * (gate * jax.nn.sigmoid(gate))

    everything = slice(0, length)
    own_rows = at_rows(side, pair)
    far_rows = at_rows(1 - side, pair)

    def power(n):
        return jnp.exp(jnp.full((1, 1), decay[0] * n, F32))

    def s1_copy(q, h, j):
        peer = lax.rem(y + j, NY)
        dest = {"sp": z * NY + peer, "tp": mirror} if h else {"sp": z * NY + peer}
        return pltpu.make_async_remote_copy(
            s1_out.at[h, q, at_rows(peer, part), :], s1_in.at[q, slot],
            s_send.at[0], s1_recv.at[q], device_id=dest, device_id_type=MESH,
        )

    def make_state(q):
        for h in range(2):
            scaled = (ks[h, q].astype(F32) * fade[h]).astype(BF16)
            total = lax.dot_general(
                scaled, vs[h, q], (((0,), (0,)), ((), ())), preferred_element_type=F32
            )
            s1_out[h, q] = total.astype(BF16)
        for j in range(NY):
            s1_copy(q, 1, j).start()
            if j:
                s1_copy(q, 0, j).start()
        s1_in[q, slot] = s1_out[0, q, at_rows(y, part), :]

    def s2_copy(q, d):
        return pltpu.make_async_remote_copy(
            s2_out.at[q], s2_in.at[q, d - 1], s_send.at[1], s2_recv.at[q],
            device_id={"sp": lax.rem(z + d, nz) * NY + y}, device_id_type=MESH,
        )

    def plane_total(q):
        took = s1_in.at[q, 0:2 * NY - 1]
        pltpu.make_async_remote_copy(
            took, took, s_send.at[0], s1_recv.at[q], device_id={"tp": mirror}, device_id_type=MESH,
        ).wait_recv()
        step = power(length)
        total = s1_in[q, 0].astype(F32)
        for k in range(1, 2 * NY):
            total = total * step + s1_in[q, k].astype(F32)
        s2_out[q] = total.astype(BF16)
        for d in range(1, nz):
            s2_copy(q, d).start()

    def s3_copy(q, h, j):
        peer = lax.rem(y + j, NY)
        dest = {"sp": z * NY + peer, "tp": mirror} if h else {"sp": z * NY + peer}
        return pltpu.make_async_remote_copy(
            s3_out.at[q, peer * 2 + (1 - group if h else group)],
            excl.at[h, q, at_rows(y, part), :],
            s_send.at[2], s3_recv.at[q], device_id=dest, device_id_type=MESH,
        )

    def hand_back(q):
        pltpu.make_async_remote_copy(
            s2_in.at[q], s2_in.at[q], s_send.at[1], s2_recv.at[q],
            device_id={"tp": mirror}, device_id_type=MESH,
        ).wait_recv()
        before = jnp.zeros((part, HEAD_DIM), F32)
        for d in range(1, nz):
            rate = power(line * NY * (d - 1)) * jnp.where(z >= d, 1.0, 0.0)
            before = before + rate * s2_in[q, d - 1].astype(F32)
        step = power(length)
        for k in range(2 * NY):
            s3_out[q, k] = before.astype(BF16)
            before = before * step + s1_in[q, k].astype(F32)
        for j in range(NY):
            s3_copy(q, 1, j).start()
            if j:
                s3_copy(q, 0, j).start()
        excl[0, q, at_rows(y, part), :] = s3_out[q, slot]

    def inside(q):
        for h in range(2):
            for i in range(length // SUB):
                here, upto = slice(i * SUB, (i + 1) * SUB), slice(0, (i + 1) * SUB)
                score = lax.dot_general(
                    qs[h, q, here, :], ks[h, q, upto, :],
                    (((1,), (1,)), ((), ())), preferred_element_type=F32,
                )
                weight = (score * mask[h, here, upto]).astype(BF16)
                within[h, q, here, :] = jnp.dot(
                    weight, vs[h, q, upto, :], preferred_element_type=F32
                )

    def gated_copy(q, dest, source):
        return pltpu.make_async_remote_copy(
            g_out.at[q, at_rows(dest, rows), :], g_in.at[q, :, at_rows(source, 2 * HEAD_DIM)],
            g_send, g_recv.at[q],
            device_id={"tp": base + dest}, device_id_type=MESH,
        )

    def finish(q):
        took = s1_in.at[q, 0:2 * NY - 1]
        pltpu.make_async_remote_copy(
            took, took, s_send.at[2], s3_recv.at[q], device_id={"tp": mirror}, device_id_type=MESH,
        ).wait_recv()
        for k in range(2):
            here = at_rows((1 - side) if k == 0 else side, pair)
            for h in range(2):
                kept = within[h, q, here, :] + jnp.dot(
                    qr[h, q, here, :], excl[h, q], preferred_element_type=F32
                )
                kept = kept - jnp.mean(kept, axis=-1, keepdims=True)
                spread = jnp.mean(kept * kept, axis=-1, keepdims=True)
                normal = kept * lax.rsqrt(spread + group_eps) * sg[h, q, here, :]
                g_out[q, here, cuts[h]] = normal.astype(BF16)
            if k == 0:
                gated_copy(q, across, me).start()
                gated_copy(q, across_twin, me).start()
            else:
                gated_copy(q, twin, me).start()
                g_in[q, :, at_rows(me, 2 * HEAD_DIM)] = g_out[q, at_rows(me, rows), :]

    def gated_wait(q):
        took = g_in.at[q, :, 0:6 * HEAD_DIM]
        pltpu.make_async_remote_copy(
            took, took, g_send, g_recv.at[q], device_id={"tp": mirror}, device_id_type=MESH,
        ).wait_recv()

    def emit(lo, hi):
        n = (hi - lo) * rows
        with jax.named_scope("gated_wait"):
            for q in range(lo, hi):
                gated_wait(q)
        step = 512
        g = g_in[lo:hi].reshape(n, g_in.shape[2])
        for c in range(width // step):
            cut = slice(c * step, (c + 1) * step)
            premix[0:n, cut] = jnp.dot(g, wo[:, cut], preferred_element_type=F32)

        def norm(i, _):
            at = pl.multiple_of(i * 16, 16)
            x = premix[pl.ds(at, 16), :]
            scale = lax.rsqrt(jnp.mean(x * x, axis=-1, keepdims=True) + rms_eps)
            q = lo + lax.div(i, rows // 16)
            to = pl.multiple_of(lax.rem(i, rows // 16) * 16, 16)
            outv[q, pl.ds(to, 16), :] = (x * scale * pgain[...]).astype(BF16)
            return 0

        lax.fori_loop(0, n // 16, norm, 0, unroll=2)
        for q in range(lo, hi):
            pltpu.make_async_copy(outv.at[q], out.at[q], out_sem).start()

    def scoped(name, function, *args):
        with jax.named_scope(name):
            function(*args)

    def over(lo, hi, function):
        def run(q, _):
            function(q)
            return 0

        lax.fori_loop(lo, hi, run, 0)

    def near(q):
        arrived(q, twin)
        project_kv(0, q, own_rows)
        project_qg(0, q, own_rows)

    def take(q):
        with jax.named_scope("take"):
            arrived(q, across)
        to_twin(q, False).start()

    def rest(q):
        with jax.named_scope("take2"):
            arrived(q, across_twin)
        project_kv(0, q, far_rows)
        project_qg(0, q, far_rows)

    end = seqs - 1
    scoped("near01", over, 0, 2, near)
    scoped("pass0", pass_on, 0)
    scoped("near23", over, 2, seqs, near)
    scoped("pass1", pass_on, 1)
    with jax.named_scope("tables1"):
        head_copy().wait_recv()
        tables(1)
    loads[3].wait()
    pltpu.make_async_copy(wo_h, wo, o_sem).wait()
    scoped("pass2", pass_on, 2)
    take(0)
    scoped("pass3", pass_on, 3)
    scoped("rest0", rest, 0)
    take(1)
    scoped("rest1", rest, 1)
    with jax.named_scope("havekv"):
        have(0)

    def early(q):
        project_kv(1, q, everything)
        make_state(q)

    def lone(q):
        project_kv(1, q, own_rows)

    def later(q):
        project_qg(1, q, everything)

    scoped("early", over, 0, 2, early)
    take(2)
    scoped("lone", over, 2, seqs, lone)
    scoped("rest2", rest, 2)
    project_kv(1, 2, far_rows)
    scoped("state2", make_state, 2)
    with jax.named_scope("haveqg"):
        have(1)
    scoped("later", over, 0, seqs - 1, later)
    scoped("plane0", plane_total, 0)
    scoped("plane1", plane_total, 1)
    project_qg(1, end, own_rows)
    take(end)
    scoped("inside01", over, 0, 2, inside)
    with jax.named_scope("take2e"):
        arrived(end, across_twin)
    with jax.named_scope("rest3"):
        for h in range(2):
            project_kv(h, end, far_rows)
        make_state(end)
    scoped("plane2", plane_total, 2)
    scoped("back0", hand_back, 0)
    scoped("back1", hand_back, 1)
    with jax.named_scope("qg3"):
        for h in range(2):
            project_qg(h, end, far_rows)
    scoped("inside23", over, 2, seqs, inside)
    scoped("plane3", plane_total, end)
    scoped("back2", hand_back, 2)
    scoped("finish01", over, 0, 2, finish)
    scoped("back3", hand_back, end)
    scoped("finish23", over, 2, seqs, finish)
    scoped("emit0", emit, 0, end)
    scoped("emit3", emit, end, seqs)

    def sent(took, sem):
        pltpu.make_async_remote_copy(
            took, took, sem, h_recv, device_id={"tp": mirror}, device_id_type=MESH,
        ).wait_send()

    with jax.named_scope("drain"):
        sent(tokv, x_send)
        sent(gath.at[:, 0:2 * rows, :], p_send)
        sent(w.at[0, :, :], w_send)
        sent(heads.at[0], w_send)
        sent(s1_in.at[:, 0:2 * NY - 1], s_send.at[0])
        sent(s2_in, s_send.at[1])
        sent(s3_out.at[:, 0:2 * NY - 1], s_send.at[2])
        sent(g_in.at[:, :, 0:6 * HEAD_DIM], g_send)
        pltpu.make_async_copy(outv, out, out_sem).wait()


def hand_over(source, out, held, in_sem, out_sem):
    pieces = range(source.shape[0])
    into = [pltpu.make_async_copy(source.at[i], held.at[i], in_sem.at[i]) for i in pieces]
    back = [pltpu.make_async_copy(held.at[i], out.at[i], out_sem.at[i]) for i in pieces]
    for copy in into:
        copy.start()
    for i in pieces:
        into[i].wait()
        back[i].start()
    for copy in back:
        copy.wait()


def solution(mesh):
    tp, sp = mesh.shape["tp"], mesh.shape["sp"]

    def body(tok, gain, wq, wk, wv, wg, decay, ngain, wo, pgain):
        seqs, rows, width = tok.shape
        length = rows * 4
        nz = sp // NY
        part = HEAD_DIM // NY
        half = HEAD_DIM // 2
        inv = np.float32(rope_base) ** (-np.arange(half, dtype=np.float32) / half)
        inv = jnp.asarray(np.concatenate([inv, inv])[None, :], F32)
        dma = pltpu.SemaphoreType.DMA
        hbm = pl.BlockSpec(memory_space=pltpu.HBM)
        vmem = pltpu.VMEM
        wide = vmem((2, seqs, length, HEAD_DIM), BF16)
        mixed = pl.pallas_call(
            functools.partial(kernel, tp, sp),
            out_shape=jax.ShapeDtypeStruct(tok.shape, BF16),
            in_specs=[
                hbm, hbm, hbm, hbm, hbm, hbm,
                pl.BlockSpec(memory_space=pltpu.SMEM), hbm, hbm, hbm, hbm,
            ],
            out_specs=hbm,
            scratch_shapes=[
                vmem((1, width), F32), vmem((1, width), F32), vmem((1, HEAD_DIM), F32),
                vmem((2, 8, HEAD_DIM), F32),
                vmem(tok.shape, BF16),
                vmem((seqs, length, width), BF16),
                vmem((2, width, 4 * HEAD_DIM), BF16),
                vmem(wo.shape, BF16),
                vmem((length, HEAD_DIM), F32), vmem((length, HEAD_DIM), F32),
                vmem((2, length, length), F32),
                vmem((2, length, HEAD_DIM), F32), vmem((2, length, HEAD_DIM), F32),
                wide, wide, wide, wide,
                vmem((2, seqs, length, HEAD_DIM), F32),
                vmem((2, seqs, length, HEAD_DIM), F32),
                vmem((2, seqs, HEAD_DIM, HEAD_DIM), BF16),
                vmem((seqs, 2 * NY, part, HEAD_DIM), BF16),
                vmem((seqs, part, HEAD_DIM), BF16),
                vmem((seqs, nz - 1, part, HEAD_DIM), BF16),
                vmem((seqs, 2 * NY, part, HEAD_DIM), BF16),
                vmem((2, seqs, HEAD_DIM, HEAD_DIM), BF16),
                vmem((seqs, length, 2 * HEAD_DIM), BF16),
                vmem((seqs, rows, HEAD_DIM * tp), BF16),
                vmem((seqs * rows, width), F32),
                vmem(tok.shape, BF16),
                dma(()), dma(()), dma((seqs, 4)), dma(()), dma((6,)), dma(()),
                dma((3,)), dma((seqs,)), dma((seqs,)), dma((seqs,)), dma(()), dma((seqs,)),
                dma((8,)), dma(()), dma((seqs,)), dma(()),
            ],
            compiler_params=pltpu.CompilerParams(
                collective_id=0, has_side_effects=True, vmem_limit_bytes=59 * 2**20
            ),
            name="retention",
        )(
            tok, gain[None, :], wq, wk, wv, wg, decay, ngain[None, :], wo, pgain[None, :], inv
        )
        return pl.pallas_call(
            hand_over,
            out_shape=jax.ShapeDtypeStruct(tok.shape, BF16),
            in_specs=[hbm],
            out_specs=hbm,
            scratch_shapes=[pltpu.VMEM(tok.shape, BF16), dma((seqs,)), dma((seqs,))],
            compiler_params=pltpu.CompilerParams(vmem_limit_bytes=59 * 2**20),
            name="hand_over",
        )(mixed)

    placed = (
        P(None, ("sp", "tp"), None),
        P(),
        P(None, "tp"),
        P(None, "tp"),
        P(None, "tp"),
        P(None, "tp"),
        P("tp"),
        P("tp"),
        P(),
        P(),
    )
    return jax.shard_map(
        body, mesh=mesh, in_specs=placed, out_specs=P(None, ("sp", "tp"), None), check_vma=False
    )
```

```python
import functools

import jax
import jax.numpy as jnp
import numpy as np
from jax import lax
from jax.experimental import pallas as pl
from jax.experimental.pallas import tpu as pltpu
from jax.sharding import PartitionSpec as P

HEAD_DIM = 128
SUB = 128
NY = 4
rms_eps = 1e-06
group_eps = 1e-05
rope_base = 10000.0
MESH = pl.DeviceIdType.MESH
F32 = jnp.float32
BF16 = jnp.bfloat16


def kernel(
    tp, sp,
    tok, gain_h, wq_h, wk_h, wv_h, wg_h, decay, ngain_h, wo_h, pgain_h, inv_h,
    out,
    gain, pgain, inv, heads, tokv, raw, gath, w, wo, cosv, sinv, mask, fade, reach,
    qs, qr, ks, vs, sg, within, s1_out, s1_in, s2_out, s2_in, s3_out, excl,
    g_out, g_in, premix,
    x_send, p_send, t_recv, w_send, wx_recv, h_recv,
    s_send, s1_recv, s2_recv, s3_recv, g_send, g_recv,
    w_sem, o_sem, in_sem,
):
    seqs, rows, width = tok.shape
    pair = 2 * rows
    length = 2 * pair
    line = rows * tp
    nz = sp // NY
    part = HEAD_DIM // NY
    direct = width // 4
    piece = (width - direct) // NY
    s, t = lax.axis_index("sp"), lax.axis_index("tp")
    z, y = lax.div(s, NY), lax.rem(s, NY)
    chip, core = lax.div(t, 2), lax.rem(t, 2)
    group, side = lax.div(chip, 2), lax.rem(chip, 2)
    base = group * 4
    me = side * 2 + core
    twin = side * 2 + 1 - core
    across = (1 - side) * 2 + core
    across_twin = (1 - side) * 2 + 1 - core
    mirror = (3 - chip) * 2 + core
    slot = y * 2 + group

    def at_rows(who, n):
        return pl.ds(pl.multiple_of(who * n, n), n)

    loads_in = [
        pltpu.make_async_copy(
            tok.at[q], tokv.at[q - 1] if q else raw.at[at_rows(me, rows), :], in_sem.at[q]
        )
        for q in range(seqs)
    ]

    cuts = [slice(i * HEAD_DIM, (i + 1) * HEAD_DIM) for i in range(4)]
    loads_w = [
        pltpu.make_async_copy(a, w.at[0, :, cuts[i]], w_sem.at[i])
        for i, a in enumerate((wk_h, wv_h, wq_h, wg_h))
    ]
    loads = [
        pltpu.make_async_copy(a, b, w_sem.at[4 + i])
        for i, (a, b) in enumerate(
            ((ngain_h, heads.at[0, 1:2, :]), (gain_h, gain), (inv_h, inv), (pgain_h, pgain))
        )
    ]

    def head_of(u, flip):
        c = group * 2 + u // 2
        return ((3 - c) if flip else c) * 2 + u % 2

    loads_o = [
        pltpu.make_async_copy(
            wo_h.at[pl.ds(pl.multiple_of(head_of(i // 2, i % 2) * HEAD_DIM, HEAD_DIM), HEAD_DIM), :],
            wo.at[i * HEAD_DIM:(i + 1) * HEAD_DIM, :], o_sem,
        )
        for i in range(8)
    ]
    for load in loads_in[:1] + loads[:3] + loads_in[1:] + loads_w + loads[3:] + loads_o:
        load.start()

    barrier = pltpu.get_barrier_semaphore()

    def greet(dest):
        pl.semaphore_signal(barrier, inc=1, device_id=dest, device_id_type=MESH)

    for u in (twin, across, across_twin):
        greet({"tp": base + u})
    for j in range(1, NY):
        greet({"sp": z * NY + lax.rem(y + j, NY)})
    for j in range(NY):
        greet({"sp": z * NY + lax.rem(y + j, NY), "tp": mirror})
    for j in range(1, nz):
        greet({"sp": lax.rem(z + j, nz) * NY + y})

    def cross(i):
        span = pl.ds(pl.multiple_of(direct + y * piece, 128), piece)
        return pltpu.make_async_remote_copy(
            w.at[0, span, cuts[i]], w.at[1, span, cuts[i]], w_send, wx_recv.at[i],
            device_id={"tp": mirror}, device_id_type=MESH,
        )

    def straight(i):
        return pltpu.make_async_remote_copy(
            w.at[0, 0:direct, cuts[i]], w.at[1, 0:direct, cuts[i]],
            w_send, wx_recv.at[4 + i // 2],
            device_id={"tp": mirror}, device_id_type=MESH,
        )

    def along(i, j):
        peer = lax.rem(y + j, NY)
        span = pl.ds(pl.multiple_of(direct + y * piece, 128), piece)
        return pltpu.make_async_remote_copy(
            w.at[1, span, cuts[i]], w.at[1, span, cuts[i]], w_send, wx_recv.at[4 + i // 2],
            device_id={"sp": z * NY + peer}, device_id_type=MESH,
        )

    def pass_on(i):
        cross(i).wait_recv()
        for j in range(1, NY):
            along(i, j).start()

    def have(k):
        took = w.at[1, 0:width - piece, 256 * k:256 * (k + 1)]
        pltpu.make_async_remote_copy(
            took, took, w_send, wx_recv.at[4 + k], device_id={"tp": mirror}, device_id_type=MESH,
        ).wait_recv()

    def head_copy():
        return pltpu.make_async_remote_copy(
            heads.at[0], heads.at[1], w_send, h_recv, device_id={"tp": mirror}, device_id_type=MESH,
        )

    def block_copy(q, u, dest, sem):
        held = raw.at[at_rows(u, rows), :] if q is None else gath.at[q, at_rows(u, rows), :]
        return pltpu.make_async_remote_copy(
            held, held, sem, t_recv.at[0 if q is None else q, u],
            device_id={"tp": base + dest}, device_id_type=MESH,
        )

    def raw_own(dest, sem):
        return pltpu.make_async_remote_copy(
            tok.at[0], raw.at[at_rows(me, rows), :], sem, t_recv.at[0, me],
            device_id={"tp": base + dest}, device_id_type=MESH,
        )

    def arrived(q, u):
        block_copy(q, u, twin, x_send).wait_recv()

    def normalise(source, q, u):
        def norm(i, _):
            x = source(pl.multiple_of(i * 16, 16)).astype(F32)
            scale = lax.rsqrt(jnp.mean(x * x, axis=-1, keepdims=True) + rms_eps)
            to = pl.ds(pl.multiple_of(u * rows + i * 16, 16), 16)
            gath[q, to, :] = (x * scale * gain[...]).astype(BF16)
            return 0

        lax.fori_loop(0, rows // 16, norm, 0, unroll=2)

    def norm_own(q):
        loads_in[q].wait()
        normalise(lambda at: tokv[q - 1, pl.ds(at, 16), :], q, me)

    def norm_raw(u):
        normalise(lambda at: raw[pl.ds(pl.multiple_of(u * rows + at, 16), 16), :], 0, u)

    def send(q):
        block_copy(q, me, across, x_send).start()
        block_copy(q, me, twin, p_send).start()

    with jax.named_scope("barrier"):
        pl.semaphore_wait(barrier, 3 + NY - 1 + NY + nz - 1)
    raw_own(across, x_send).start()
    raw_own(twin, p_send).start()
    with jax.named_scope("norm"):
        loads[0].wait()
        heads[0, 0:1, :] = jnp.full((1, HEAD_DIM), decay[0], F32)
        loads[1].wait()
        norm_own(1)
        head_copy().start()
        norm_own(2)
        send(1)
        for i in range(4):
            loads_w[i].wait()
            cross(i).start()
        for i in range(4):
            straight(i).start()
        norm_own(3)
        send(2)
        send(3)
        loads_in[0].wait()
        norm_raw(me)

    with jax.named_scope("tables"):
        loads[2].wait()
        place = s * line + group * length + lax.broadcasted_iota(jnp.int32, (length, HEAD_DIM), 0)
        angle = place.astype(F32) * inv[...]
        cosv[...] = jnp.cos(angle)
        lane = lax.broadcasted_iota(jnp.int32, (length, HEAD_DIM), 1)
        sine = jnp.sin(angle)
        sinv[...] = jnp.where(lane < HEAD_DIM // 2, -sine, sine)

    def tables(h):
        rate = heads[h, 0:1, :]
        spot = lax.broadcasted_iota(jnp.int32, (length, HEAD_DIM), 0)
        fade[h] = jnp.exp(rate * (length - 1 - spot).astype(F32))
        reach[h] = jnp.exp(rate * (1 + spot).astype(F32))
        for c in range(length // HEAD_DIM):
            gap = spot - c * HEAD_DIM - lax.broadcasted_iota(jnp.int32, (length, HEAD_DIM), 1)
            weight = jnp.exp(rate * jnp.maximum(gap, 0).astype(F32))
            mask[h, :, c * HEAD_DIM:(c + 1) * HEAD_DIM] = jnp.where(gap >= 0, weight, 0.0)

    with jax.named_scope("tables0"):
        tables(0)

    def rotate(x, span):
        x = x.astype(BF16).astype(F32)
        return x * cosv[span, :] + pltpu.roll(x, HEAD_DIM // 2, 1) * sinv[span, :]

    def project_kv(h, q, span):
        r = jnp.dot(gath[q, span, :], w[h, :, 0:256], preferred_element_type=F32)
        ks[h, q, span, :] = (rotate(r[:, cuts[0]], span) * HEAD_DIM ** (-0.5)).astype(BF16)
        vs[h, q, span, :] = r[:, cuts[1]].astype(BF16)

    def project_qg(h, q, span):
        r = jnp.dot(gath[q, span, :], w[h, :, 256:512], preferred_element_type=F32)
        query = rotate(r[:, cuts[0]], span).astype(BF16)
        qs[h, q, span, :] = query
        qr[h, q, span, :] = (query.astype(F32) * reach[h, span, :]).astype(BF16)
        gate = r[:, cuts[1]].astype(BF16).astype(F32)
        sg[h, q, span, :] = heads[h, 1:2, :] * (gate * jax.nn.sigmoid(gate))

    everything = slice(0, length)
    own_rows = at_rows(side, pair)
    far_rows = at_rows(1 - side, pair)

    def power(n):
        return jnp.exp(jnp.full((1, 1), decay[0] * n, F32))

    def s1_copy(q, h, j):
        peer = lax.rem(y + j, NY)
        dest = {"sp": z * NY + peer, "tp": mirror} if h else {"sp": z * NY + peer}
        return pltpu.make_async_remote_copy(
            s1_out.at[h, q, at_rows(peer, part), :], s1_in.at[q, slot],
            s_send.at[0], s1_recv.at[q], device_id=dest, device_id_type=MESH,
        )

    def make_state(q):
        for h in range(2):
            scaled = (ks[h, q].astype(F32) * fade[h]).astype(BF16)
            total = lax.dot_general(
                scaled, vs[h, q], (((0,), (0,)), ((), ())), preferred_element_type=F32
            )
            s1_out[h, q] = total.astype(BF16)
        for j in range(NY):
            s1_copy(q, 1, j).start()
            if j:
                s1_copy(q, 0, j).start()
        s1_in[q, slot] = s1_out[0, q, at_rows(y, part), :]

    def s2_copy(q, d):
        return pltpu.make_async_remote_copy(
            s2_out.at[q], s2_in.at[q, d - 1], s_send.at[1], s2_recv.at[q],
            device_id={"sp": lax.rem(z + d, nz) * NY + y}, device_id_type=MESH,
        )

    def plane_total(q):
        took = s1_in.at[q, 0:2 * NY - 1]
        pltpu.make_async_remote_copy(
            took, took, s_send.at[0], s1_recv.at[q], device_id={"tp": mirror}, device_id_type=MESH,
        ).wait_recv()
        step = power(length)
        total = s1_in[q, 0].astype(F32)
        for k in range(1, 2 * NY):
            total = total * step + s1_in[q, k].astype(F32)
        s2_out[q] = total.astype(BF16)
        for d in range(1, nz):
            s2_copy(q, d).start()

    def s3_copy(q, h, j):
        peer = lax.rem(y + j, NY)
        dest = {"sp": z * NY + peer, "tp": mirror} if h else {"sp": z * NY + peer}
        return pltpu.make_async_remote_copy(
            s3_out.at[q, peer * 2 + (1 - group if h else group)],
            excl.at[h, q, at_rows(y, part), :],
            s_send.at[2], s3_recv.at[q], device_id=dest, device_id_type=MESH,
        )

    def hand_back(q):
        pltpu.make_async_remote_copy(
            s2_in.at[q], s2_in.at[q], s_send.at[1], s2_recv.at[q],
            device_id={"tp": mirror}, device_id_type=MESH,
        ).wait_recv()
        before = jnp.zeros((part, HEAD_DIM), F32)
        for d in range(1, nz):
            rate = power(line * NY * (d - 1)) * jnp.where(z >= d, 1.0, 0.0)
            before = before + rate * s2_in[q, d - 1].astype(F32)
        step = power(length)
        for k in range(2 * NY):
            s3_out[q, k] = before.astype(BF16)
            before = before * step + s1_in[q, k].astype(F32)
        for j in range(NY):
            s3_copy(q, 1, j).start()
            if j:
                s3_copy(q, 0, j).start()
        excl[0, q, at_rows(y, part), :] = s3_out[q, slot]

    def inside(q):
        for h in range(2):
            for i in range(length // SUB):
                here, upto = slice(i * SUB, (i + 1) * SUB), slice(0, (i + 1) * SUB)
                score = lax.dot_general(
                    qs[h, q, here, :], ks[h, q, upto, :],
                    (((1,), (1,)), ((), ())), preferred_element_type=F32,
                )
                weight = (score * mask[h, here, upto]).astype(BF16)
                within[h, q, here, :] = jnp.dot(
                    weight, vs[h, q, upto, :], preferred_element_type=F32
                )

    def gated_copy(q, dest, source, near_by=0):
        return pltpu.make_async_remote_copy(
            g_out.at[q, at_rows(dest, rows), :], g_in.at[q, :, at_rows(source, 2 * HEAD_DIM)],
            g_send, g_recv.at[near_by, q],
            device_id={"tp": base + dest}, device_id_type=MESH,
        )

    def finish(q):
        took = s1_in.at[q, 0:2 * NY - 1]
        pltpu.make_async_remote_copy(
            took, took, s_send.at[2], s3_recv.at[q], device_id={"tp": mirror}, device_id_type=MESH,
        ).wait_recv()
        for k in range(2):
            here = at_rows((1 - side) if k == 0 else side, pair)
            for h in range(2):
                kept = within[h, q, here, :] + jnp.dot(
                    qr[h, q, here, :], excl[h, q], preferred_element_type=F32
                )
                kept = kept - jnp.mean(kept, axis=-1, keepdims=True)
                spread = jnp.mean(kept * kept, axis=-1, keepdims=True)
                normal = kept * lax.rsqrt(spread + group_eps) * sg[h, q, here, :]
                g_out[q, here, cuts[h]] = normal.astype(BF16)
            if k == 0:
                gated_copy(q, across, me).start()
                gated_copy(q, across_twin, me).start()
            else:
                gated_copy(q, twin, me, 1).start()
                g_in[q, :, at_rows(me, 2 * HEAD_DIM)] = g_out[q, at_rows(me, rows), :]

    def gated_wait(q, near_by):
        took = g_in.at[q, :, 0:(2 if near_by else 4) * HEAD_DIM]
        pltpu.make_async_remote_copy(
            took, took, g_send, g_recv.at[near_by, q],
            device_id={"tp": mirror}, device_id_type=MESH,
        ).wait_recv()

    step = 512
    side_cols = 4 * HEAD_DIM

    def closing(lo, n):
        def norm(i, _):
            at = pl.multiple_of(i * 16, 16)
            x = premix[pl.ds(at, 16), :]
            scale = lax.rsqrt(jnp.mean(x * x, axis=-1, keepdims=True) + rms_eps)
            q = lo + lax.div(i, rows // 16)
            to = pl.multiple_of(lax.rem(i, rows // 16) * 16, 16)
            out[q, pl.ds(to, 16), :] = (x * scale * pgain[...]).astype(BF16)
            return 0

        lax.fori_loop(0, n // 16, norm, 0, unroll=2)

    def emit(lo, hi):
        n = (hi - lo) * rows
        with jax.named_scope("gated_wait"):
            for q in range(lo, hi):
                gated_wait(q, 0)
                gated_wait(q, 1)
        g = g_in[lo:hi].reshape(n, g_in.shape[2])
        for c in range(width // step):
            cut = slice(c * step, (c + 1) * step)
            premix[0:n, cut] = jnp.dot(g, wo[:, cut], preferred_element_type=F32)
        closing(lo, n)

    def emit_half(q, which, near_by):
        gated_wait(q, near_by)
        span = at_rows(which, side_cols)
        for c in range(width // step):
            cut = slice(c * step, (c + 1) * step)
            term = jnp.dot(g_in[q, :, span], wo[span, cut], preferred_element_type=F32)
            premix[0:rows, cut] = term if near_by else premix[0:rows, cut] + term

    def scoped(name, function, *args):
        with jax.named_scope(name):
            function(*args)

    def over(lo, hi, function):
        def run(q, _):
            function(q)
            return 0

        lax.fori_loop(lo, hi, run, 0)

    def near(q):
        arrived(q, twin)
        project_kv(0, q, own_rows)
        project_qg(0, q, own_rows)

    def near_raw():
        arrived(None, twin)
        norm_raw(twin)
        project_kv(0, 0, own_rows)
        project_qg(0, 0, own_rows)

    def take(q):
        with jax.named_scope("take"):
            arrived(q, across)
        block_copy(q, across, twin, p_send).start()

    def rest(q):
        with jax.named_scope("take2"):
            arrived(q, across_twin)
        project_kv(0, q, far_rows)
        project_qg(0, q, far_rows)

    def rest_raw():
        norm_raw(across)
        with jax.named_scope("take2"):
            arrived(None, across_twin)
        norm_raw(across_twin)
        project_kv(0, 0, far_rows)
        project_qg(0, 0, far_rows)

    end = seqs - 1
    scoped("near0", near_raw)
    scoped("pass0", pass_on, 0)
    scoped("near123", over, 1, seqs, near)
    scoped("pass1", pass_on, 1)
    with jax.named_scope("tables1"):
        head_copy().wait_recv()
        tables(1)
    loads[3].wait()
    pltpu.make_async_copy(wo_h, wo, o_sem).wait()
    scoped("pass2", pass_on, 2)
    take(None)
    scoped("pass3", pass_on, 3)
    scoped("rest0", rest_raw)
    take(1)
    scoped("rest1", rest, 1)
    with jax.named_scope("havekv"):
        have(0)

    def early(q):
        project_kv(1, q, everything)
        make_state(q)

    def lone(q):
        project_kv(1, q, own_rows)

    def later(q):
        project_qg(1, q, everything)

    scoped("early", over, 0, 2, early)
    take(2)
    scoped("lone", over, 2, seqs, lone)
    scoped("rest2", rest, 2)
    project_kv(1, 2, far_rows)
    scoped("state2", make_state, 2)
    with jax.named_scope("haveqg"):
        have(1)
    scoped("later", over, 0, seqs - 1, later)
    scoped("plane0", plane_total, 0)
    scoped("plane1", plane_total, 1)
    project_qg(1, end, own_rows)
    take(end)
    scoped("inside01", over, 0, 2, inside)
    with jax.named_scope("take2e"):
        arrived(end, across_twin)
    with jax.named_scope("rest3"):
        for h in range(2):
            project_kv(h, end, far_rows)
        make_state(end)
    scoped("plane2", plane_total, 2)
    with jax.named_scope("qg3"):
        for h in range(2):
            project_qg(h, end, far_rows)
    scoped("inside23", over, 2, seqs, inside)
    scoped("back0", hand_back, 0)
    scoped("back1", hand_back, 1)
    scoped("plane3", plane_total, end)
    scoped("back2", hand_back, 2)
    scoped("finish01", over, 0, 2, finish)
    scoped("back3", hand_back, end)
    scoped("finish23", over, 2, seqs, finish)
    scoped("emit0", emit, 0, end)
    scoped("emit3a", emit_half, end, side, 1)
    scoped("emit3b", emit_half, end, 1 - side, 0)
    scoped("closing", closing, end, rows)

    def sent(took, sem):
        pltpu.make_async_remote_copy(
            took, took, sem, h_recv, device_id={"tp": mirror}, device_id_type=MESH,
        ).wait_send()

    with jax.named_scope("drain"):
        sent(gath.at[:, 0:rows, :], x_send)
        sent(gath.at[:, 0:2 * rows, :], p_send)
        sent(w.at[0, :, :], w_send)
        sent(heads.at[0], w_send)
        sent(s1_in.at[:, 0:2 * NY - 1], s_send.at[0])
        sent(s2_in, s_send.at[1])
        sent(s3_out.at[:, 0:2 * NY - 1], s_send.at[2])
        sent(g_in.at[:, :, 0:6 * HEAD_DIM], g_send)


def hand_over(source, out, sem):
    copy = pltpu.make_async_copy(source, out, sem)
    copy.start()
    copy.wait()


def solution(mesh):
    tp, sp = mesh.shape["tp"], mesh.shape["sp"]

    def body(tok, gain, wq, wk, wv, wg, decay, ngain, wo, pgain):
        seqs, rows, width = tok.shape
        length = rows * 4
        nz = sp // NY
        part = HEAD_DIM // NY
        half = HEAD_DIM // 2
        inv = np.float32(rope_base) ** (-np.arange(half, dtype=np.float32) / half)
        inv = jnp.asarray(np.concatenate([inv, inv])[None, :], F32)
        dma = pltpu.SemaphoreType.DMA
        hbm = pl.BlockSpec(memory_space=pltpu.HBM)
        vmem = pltpu.VMEM
        wide = vmem((2, seqs, length, HEAD_DIM), BF16)
        mixed = pl.pallas_call(
            functools.partial(kernel, tp, sp),
            out_shape=jax.ShapeDtypeStruct(tok.shape, BF16),
            in_specs=[
                hbm, hbm, hbm, hbm, hbm, hbm,
                pl.BlockSpec(memory_space=pltpu.SMEM), hbm, hbm, hbm, hbm,
            ],
            out_specs=pl.BlockSpec(memory_space=pltpu.VMEM),
            scratch_shapes=[
                vmem((1, width), F32), vmem((1, width), F32), vmem((1, HEAD_DIM), F32),
                vmem((2, 8, HEAD_DIM), F32),
                vmem((seqs - 1, rows, width), BF16),
                vmem((length, width), BF16),
                vmem((seqs, length, width), BF16),
                vmem((2, width, 4 * HEAD_DIM), BF16),
                vmem(wo.shape, BF16),
                vmem((length, HEAD_DIM), F32), vmem((length, HEAD_DIM), F32),
                vmem((2, length, length), F32),
                vmem((2, length, HEAD_DIM), F32), vmem((2, length, HEAD_DIM), F32),
                wide, wide, wide, wide,
                vmem((2, seqs, length, HEAD_DIM), F32),
                vmem((2, seqs, length, HEAD_DIM), F32),
                vmem((2, seqs, HEAD_DIM, HEAD_DIM), BF16),
                vmem((seqs, 2 * NY, part, HEAD_DIM), BF16),
                vmem((seqs, part, HEAD_DIM), BF16),
                vmem((seqs, nz - 1, part, HEAD_DIM), BF16),
                vmem((seqs, 2 * NY, part, HEAD_DIM), BF16),
                vmem((2, seqs, HEAD_DIM, HEAD_DIM), BF16),
                vmem((seqs, length, 2 * HEAD_DIM), BF16),
                vmem((seqs, rows, HEAD_DIM * tp), BF16),
                vmem((seqs * rows, width), F32),
                dma(()), dma(()), dma((seqs, 4)), dma(()), dma((6,)), dma(()),
                dma((3,)), dma((seqs,)), dma((seqs,)), dma((seqs,)), dma(()), dma((2, seqs)),
                dma((8,)), dma(()), dma((seqs,)),
            ],
            compiler_params=pltpu.CompilerParams(
                collective_id=0, has_side_effects=True, vmem_limit_bytes=40 * 2**20
            ),
            name="retention",
        )(
            *(pltpu.with_memory_space_constraint(x, pltpu.HBM) for x in (tok, gain[None, :], wq, wk, wv, wg)), decay,
            *(pltpu.with_memory_space_constraint(x, pltpu.HBM) for x in (ngain[None, :], wo, pgain[None, :], inv))
        )
        return pl.pallas_call(
            hand_over,
            out_shape=jax.ShapeDtypeStruct(tok.shape, BF16),
            in_specs=[pl.BlockSpec(memory_space=pltpu.VMEM)],
            out_specs=hbm,
            scratch_shapes=[dma(())],
            compiler_params=pltpu.CompilerParams(vmem_limit_bytes=16 * 2**20),
            name="hand_over",
        )(mixed)

    placed = (
        P(None, ("sp", "tp"), None),
        P(),
        P(None, "tp"),
        P(None, "tp"),
        P(None, "tp"),
        P(None, "tp"),
        P("tp"),
        P("tp"),
        P(),
        P(),
    )
    return jax.shard_map(
        body, mesh=mesh, in_specs=placed, out_specs=P(None, ("sp", "tp"), None), check_vma=False
    )
```

```python
import functools

import jax
import jax.numpy as jnp
import numpy as np
from jax import lax
from jax.experimental import pallas as pl
from jax.experimental.pallas import tpu as pltpu
from jax.sharding import PartitionSpec as P

HEAD_DIM = 128
SUB = 128
NY = 4
rms_eps = 1e-06
group_eps = 1e-05
rope_base = 10000.0
MESH = pl.DeviceIdType.MESH
F32 = jnp.float32
BF16 = jnp.bfloat16


def kernel(
    tp, sp,
    tok, gain_h, wq_h, wk_h, wv_h, wg_h, decay, ngain_h, wo_h, pgain_h, inv_h,
    out,
    gain, pgain, inv, heads, tokv, raw, gath, w, wo, cosv, sinv, mask, fade, reach,
    qs, qr, ks, vs, sg, within, s1_out, s1_in, s2_out, s2_in, s3_out, excl,
    g_out, g_in, premix,
    x_send, p_send, t_recv, w_send, wx_recv, h_recv,
    s_send, s1_recv, s2_recv, s3_recv, g_send, g_recv,
    w_sem, o_sem, in_sem, present,
):
    seqs, rows, width = tok.shape
    pair = 2 * rows
    length = 2 * pair
    line = rows * tp
    nz = sp // NY
    part = HEAD_DIM // NY
    direct = width // 4
    piece = (width - direct) // NY
    s, t = lax.axis_index("sp"), lax.axis_index("tp")
    z, y = lax.div(s, NY), lax.rem(s, NY)
    chip, core = lax.div(t, 2), lax.rem(t, 2)
    group, side = lax.div(chip, 2), lax.rem(chip, 2)
    base = group * 4
    me = side * 2 + core
    twin = side * 2 + 1 - core
    across = (1 - side) * 2 + core
    across_twin = (1 - side) * 2 + 1 - core
    mirror = (3 - chip) * 2 + core
    slot = y * 2 + group

    def at_rows(who, n):
        return pl.ds(pl.multiple_of(who * n, n), n)

    loads_in = [
        pltpu.make_async_copy(
            tok.at[q], tokv.at[q - 1] if q else raw.at[at_rows(me, rows), :], in_sem.at[q]
        )
        for q in range(seqs)
    ]

    cuts = [slice(i * HEAD_DIM, (i + 1) * HEAD_DIM) for i in range(4)]
    loads_w = [
        pltpu.make_async_copy(a, w.at[0, :, cuts[i]], w_sem.at[i])
        for i, a in enumerate((wk_h, wv_h, wq_h, wg_h))
    ]
    loads = [
        pltpu.make_async_copy(a, b, w_sem.at[4 + i])
        for i, (a, b) in enumerate(
            ((ngain_h, heads.at[0, 1:2, :]), (gain_h, gain), (inv_h, inv), (pgain_h, pgain))
        )
    ]

    def head_of(u, flip):
        c = group * 2 + u // 2
        return ((3 - c) if flip else c) * 2 + u % 2

    loads_o = [
        pltpu.make_async_copy(
            wo_h.at[pl.ds(pl.multiple_of(head_of(i // 2, i % 2) * HEAD_DIM, HEAD_DIM), HEAD_DIM), :],
            wo.at[i * HEAD_DIM:(i + 1) * HEAD_DIM, :], o_sem,
        )
        for i in range(8)
    ]
    for load in loads_in[:1] + loads[:3] + loads_in[1:] + loads_w + loads[3:] + loads_o:
        load.start()

    barrier = pltpu.get_barrier_semaphore()

    def greet(dest):
        pl.semaphore_signal(barrier, inc=1, device_id=dest, device_id_type=MESH)

    for u in (twin, across, across_twin):
        greet({"tp": base + u})
    for j in range(1, NY):
        greet({"sp": z * NY + lax.rem(y + j, NY)})
    for j in range(NY):
        greet({"sp": z * NY + lax.rem(y + j, NY), "tp": mirror})
    for d in range(1, nz):
        @pl.when(z + d < nz)
        def _():
            greet({"sp": lax.rem(z + d, nz) * NY + y})

    def cross(i):
        span = pl.ds(pl.multiple_of(direct + y * piece, 128), piece)
        return pltpu.make_async_remote_copy(
            w.at[0, span, cuts[i]], w.at[1, span, cuts[i]], w_send, wx_recv.at[i],
            device_id={"tp": mirror}, device_id_type=MESH,
        )

    def straight(i):
        return pltpu.make_async_remote_copy(
            w.at[0, 0:direct, cuts[i]], w.at[1, 0:direct, cuts[i]],
            w_send, wx_recv.at[4 + i // 2],
            device_id={"tp": mirror}, device_id_type=MESH,
        )

    def along(i, j):
        peer = lax.rem(y + j, NY)
        span = pl.ds(pl.multiple_of(direct + y * piece, 128), piece)
        return pltpu.make_async_remote_copy(
            w.at[1, span, cuts[i]], w.at[1, span, cuts[i]], w_send, wx_recv.at[4 + i // 2],
            device_id={"sp": z * NY + peer}, device_id_type=MESH,
        )

    def pass_on(i):
        cross(i).wait_recv()
        for j in range(1, NY):
            along(i, j).start()

    def have(k):
        took = w.at[1, 0:width - piece, 256 * k:256 * (k + 1)]
        pltpu.make_async_remote_copy(
            took, took, w_send, wx_recv.at[4 + k], device_id={"tp": mirror}, device_id_type=MESH,
        ).wait_recv()

    def head_copy():
        return pltpu.make_async_remote_copy(
            heads.at[0], heads.at[1], w_send, h_recv, device_id={"tp": mirror}, device_id_type=MESH,
        )

    def block_copy(q, u, dest, sem):
        held = raw.at[at_rows(u, rows), :] if q is None else gath.at[q, at_rows(u, rows), :]
        return pltpu.make_async_remote_copy(
            held, held, sem, t_recv.at[0 if q is None else q, u],
            device_id={"tp": base + dest}, device_id_type=MESH,
        )

    def raw_own(dest, sem):
        return pltpu.make_async_remote_copy(
            tok.at[0], raw.at[at_rows(me, rows), :], sem, t_recv.at[0, me],
            device_id={"tp": base + dest}, device_id_type=MESH,
        )

    def arrived(q, u):
        block_copy(q, u, twin, x_send).wait_recv()

    def normalise(source, q, u):
        def norm(i, _):
            x = source(pl.multiple_of(i * 16, 16)).astype(F32)
            scale = lax.rsqrt(jnp.mean(x * x, axis=-1, keepdims=True) + rms_eps)
            to = pl.ds(pl.multiple_of(u * rows + i * 16, 16), 16)
            gath[q, to, :] = (x * scale * gain[...]).astype(BF16)
            return 0

        lax.fori_loop(0, rows // 16, norm, 0, unroll=2)

    def norm_own(q):
        loads_in[q].wait()
        normalise(lambda at: tokv[q - 1, pl.ds(at, 16), :], q, me)

    def norm_raw(u):
        normalise(lambda at: raw[pl.ds(pl.multiple_of(u * rows + at, 16), 16), :], 0, u)

    def send(q):
        block_copy(q, me, across, x_send).start()
        block_copy(q, me, twin, p_send).start()

    with jax.named_scope("barrier"):
        pl.semaphore_wait(barrier, 3 + NY - 1 + NY + z)
    raw_own(across, x_send).start()
    raw_own(twin, p_send).start()
    for d in range(1, nz):
        @pl.when(z >= d)
        def _():
            pl.semaphore_signal(
                present, inc=1, device_id={"sp": lax.rem(z + nz - d, nz) * NY + y},
                device_id_type=MESH,
            )
    with jax.named_scope("norm"):
        loads[0].wait()
        heads[0, 0:1, :] = jnp.full((1, HEAD_DIM), decay[0], F32)
        loads[1].wait()
        norm_own(1)
        head_copy().start()
        norm_own(2)
        send(1)
        for i in range(4):
            loads_w[i].wait()
            cross(i).start()
        for i in range(4):
            straight(i).start()
        norm_own(3)
        send(2)
        send(3)
        loads_in[0].wait()
        norm_raw(me)

    with jax.named_scope("tables"):
        loads[2].wait()
        place = s * line + group * length + lax.broadcasted_iota(jnp.int32, (length, HEAD_DIM), 0)
        angle = place.astype(F32) * inv[...]
        cosv[...] = jnp.cos(angle)
        lane = lax.broadcasted_iota(jnp.int32, (length, HEAD_DIM), 1)
        sine = jnp.sin(angle)
        sinv[...] = jnp.where(lane < HEAD_DIM // 2, -sine, sine)

    def tables(h):
        rate = heads[h, 0:1, :]
        spot = lax.broadcasted_iota(jnp.int32, (length, HEAD_DIM), 0)
        fade[h] = jnp.exp(rate * (length - 1 - spot).astype(F32))
        reach[h] = jnp.exp(rate * (1 + spot).astype(F32))
        for c in range(length // HEAD_DIM):
            gap = spot - c * HEAD_DIM - lax.broadcasted_iota(jnp.int32, (length, HEAD_DIM), 1)
            weight = jnp.exp(rate * jnp.maximum(gap, 0).astype(F32))
            mask[h, :, c * HEAD_DIM:(c + 1) * HEAD_DIM] = jnp.where(gap >= 0, weight, 0.0)

    with jax.named_scope("tables0"):
        tables(0)

    def rotate(x, span):
        x = x.astype(BF16).astype(F32)
        return x * cosv[span, :] + pltpu.roll(x, HEAD_DIM // 2, 1) * sinv[span, :]

    def project_kv(h, q, span):
        r = jnp.dot(gath[q, span, :], w[h, :, 0:256], preferred_element_type=F32)
        ks[h, q, span, :] = (rotate(r[:, cuts[0]], span) * HEAD_DIM ** (-0.5)).astype(BF16)
        vs[h, q, span, :] = r[:, cuts[1]].astype(BF16)

    def project_qg(h, q, span):
        r = jnp.dot(gath[q, span, :], w[h, :, 256:512], preferred_element_type=F32)
        query = rotate(r[:, cuts[0]], span).astype(BF16)
        qs[h, q, span, :] = query
        qr[h, q, span, :] = (query.astype(F32) * reach[h, span, :]).astype(BF16)
        gate = r[:, cuts[1]].astype(BF16).astype(F32)
        sg[h, q, span, :] = heads[h, 1:2, :] * (gate * jax.nn.sigmoid(gate))

    everything = slice(0, length)
    own_rows = at_rows(side, pair)
    far_rows = at_rows(1 - side, pair)

    def power(n):
        return jnp.exp(jnp.full((1, 1), decay[0] * n, F32))

    def s1_copy(q, h, j):
        peer = lax.rem(y + j, NY)
        dest = {"sp": z * NY + peer, "tp": mirror} if h else {"sp": z * NY + peer}
        return pltpu.make_async_remote_copy(
            s1_out.at[h, q, at_rows(peer, part), :], s1_in.at[q, slot],
            s_send.at[0], s1_recv.at[q], device_id=dest, device_id_type=MESH,
        )

    def make_state(q):
        for h in range(2):
            scaled = (ks[h, q].astype(F32) * fade[h]).astype(BF16)
            total = lax.dot_general(
                scaled, vs[h, q], (((0,), (0,)), ((), ())), preferred_element_type=F32
            )
            s1_out[h, q] = total.astype(BF16)
        for j in range(NY):
            s1_copy(q, 1, j).start()
            if j:
                s1_copy(q, 0, j).start()
        s1_in[q, slot] = s1_out[0, q, at_rows(y, part), :]

    def s2_copy(q, d):
        return pltpu.make_async_remote_copy(
            s2_out.at[q], s2_in.at[q, d - 1], s_send.at[1], s2_recv.at[q],
            device_id={"sp": lax.rem(z + d, nz) * NY + y}, device_id_type=MESH,
        )

    def plane_total(q):
        took = s1_in.at[q, 0:2 * NY - 1]
        pltpu.make_async_remote_copy(
            took, took, s_send.at[0], s1_recv.at[q], device_id={"tp": mirror}, device_id_type=MESH,
        ).wait_recv()
        step = power(length)
        total = s1_in[q, 0].astype(F32)
        for k in range(1, 2 * NY):
            total = total * step + s1_in[q, k].astype(F32)
        s2_out[q] = total.astype(BF16)
        for d in range(1, nz):
            @pl.when(z + d < nz)
            def _():
                s2_copy(q, d).start()

    def s3_copy(q, h, j):
        peer = lax.rem(y + j, NY)
        dest = {"sp": z * NY + peer, "tp": mirror} if h else {"sp": z * NY + peer}
        return pltpu.make_async_remote_copy(
            s3_out.at[q, peer * 2 + (1 - group if h else group)],
            excl.at[h, q, at_rows(y, part), :],
            s_send.at[2], s3_recv.at[q], device_id=dest, device_id_type=MESH,
        )

    def hand_back(q):
        for n in range(1, nz):
            @pl.when(z == n)
            def _():
                took = s2_in.at[q, 0:n]
                pltpu.make_async_remote_copy(
                    took, took, s_send.at[1], s2_recv.at[q],
                    device_id={"tp": mirror}, device_id_type=MESH,
                ).wait_recv()

        def add(d, total):
            return total + power(line * NY * d) * s2_in[q, d].astype(F32)

        before = lax.fori_loop(0, z, add, jnp.zeros((part, HEAD_DIM), F32))
        step = power(length)
        for k in range(2 * NY):
            s3_out[q, k] = before.astype(BF16)
            before = before * step + s1_in[q, k].astype(F32)
        for j in range(NY):
            s3_copy(q, 1, j).start()
            if j:
                s3_copy(q, 0, j).start()
        excl[0, q, at_rows(y, part), :] = s3_out[q, slot]

    def inside(q):
        for h in range(2):
            for i in range(length // SUB):
                here, upto = slice(i * SUB, (i + 1) * SUB), slice(0, (i + 1) * SUB)
                score = lax.dot_general(
                    qs[h, q, here, :], ks[h, q, upto, :],
                    (((1,), (1,)), ((), ())), preferred_element_type=F32,
                )
                weight = (score * mask[h, here, upto]).astype(BF16)
                within[h, q, here, :] = jnp.dot(
                    weight, vs[h, q, upto, :], preferred_element_type=F32
                )

    def gated_copy(q, dest, source, near_by=0):
        return pltpu.make_async_remote_copy(
            g_out.at[q, at_rows(dest, rows), :], g_in.at[q, :, at_rows(source, 2 * HEAD_DIM)],
            g_send, g_recv.at[near_by, q],
            device_id={"tp": base + dest}, device_id_type=MESH,
        )

    def finish(q):
        took = s1_in.at[q, 0:2 * NY - 1]
        pltpu.make_async_remote_copy(
            took, took, s_send.at[2], s3_recv.at[q], device_id={"tp": mirror}, device_id_type=MESH,
        ).wait_recv()
        for k in range(2):
            here = at_rows((1 - side) if k == 0 else side, pair)
            for h in range(2):
                kept = within[h, q, here, :] + jnp.dot(
                    qr[h, q, here, :], excl[h, q], preferred_element_type=F32
                )
                kept = kept - jnp.mean(kept, axis=-1, keepdims=True)
                spread = jnp.mean(kept * kept, axis=-1, keepdims=True)
                normal = kept * lax.rsqrt(spread + group_eps) * sg[h, q, here, :]
                g_out[q, here, cuts[h]] = normal.astype(BF16)
            if k == 0:
                gated_copy(q, across, me).start()
                gated_copy(q, across_twin, me).start()
            else:
                gated_copy(q, twin, me, 1).start()
                g_in[q, :, at_rows(me, 2 * HEAD_DIM)] = g_out[q, at_rows(me, rows), :]

    def gated_wait(q, near_by):
        took = g_in.at[q, :, 0:(2 if near_by else 4) * HEAD_DIM]
        pltpu.make_async_remote_copy(
            took, took, g_send, g_recv.at[near_by, q],
            device_id={"tp": mirror}, device_id_type=MESH,
        ).wait_recv()

    step = 512
    side_cols = 4 * HEAD_DIM

    def closing(lo, n):
        def norm(i, _):
            at = pl.multiple_of(i * 16, 16)
            x = premix[pl.ds(at, 16), :]
            scale = lax.rsqrt(jnp.mean(x * x, axis=-1, keepdims=True) + rms_eps)
            q = lo + lax.div(i, rows // 16)
            to = pl.multiple_of(lax.rem(i, rows // 16) * 16, 16)
            out[q, pl.ds(to, 16), :] = (x * scale * pgain[...]).astype(BF16)
            return 0

        lax.fori_loop(0, n // 16, norm, 0, unroll=2)

    def emit(lo, hi):
        n = (hi - lo) * rows
        with jax.named_scope("gated_wait"):
            for q in range(lo, hi):
                gated_wait(q, 0)
                gated_wait(q, 1)
        g = g_in[lo:hi].reshape(n, g_in.shape[2])
        for c in range(width // step):
            cut = slice(c * step, (c + 1) * step)
            premix[0:n, cut] = jnp.dot(g, wo[:, cut], preferred_element_type=F32)
        closing(lo, n)

    def emit_half(q, which, near_by):
        gated_wait(q, near_by)
        span = at_rows(which, side_cols)
        for c in range(width // step):
            cut = slice(c * step, (c + 1) * step)
            term = jnp.dot(g_in[q, :, span], wo[span, cut], preferred_element_type=F32)
            premix[0:rows, cut] = term if near_by else premix[0:rows, cut] + term

    def scoped(name, function, *args):
        with jax.named_scope(name):
            function(*args)

    def over(lo, hi, function):
        def run(q, _):
            function(q)
            return 0

        lax.fori_loop(lo, hi, run, 0)

    def near(q):
        arrived(q, twin)
        project_kv(0, q, own_rows)
        project_qg(0, q, own_rows)

    def near_raw():
        arrived(None, twin)
        norm_raw(twin)
        project_kv(0, 0, own_rows)
        project_qg(0, 0, own_rows)

    def take(q):
        with jax.named_scope("take"):
            arrived(q, across)
        block_copy(q, across, twin, p_send).start()

    def rest(q):
        with jax.named_scope("take2"):
            arrived(q, across_twin)
        project_kv(0, q, far_rows)
        project_qg(0, q, far_rows)

    def rest_raw():
        norm_raw(across)
        with jax.named_scope("take2"):
            arrived(None, across_twin)
        norm_raw(across_twin)
        project_kv(0, 0, far_rows)
        project_qg(0, 0, far_rows)

    end = seqs - 1
    scoped("near0", near_raw)
    scoped("pass0", pass_on, 0)
    scoped("near123", over, 1, seqs, near)
    scoped("pass1", pass_on, 1)
    with jax.named_scope("tables1"):
        head_copy().wait_recv()
        tables(1)
    loads[3].wait()
    pltpu.make_async_copy(wo_h, wo, o_sem).wait()
    scoped("pass2", pass_on, 2)
    take(None)
    scoped("pass3", pass_on, 3)
    scoped("rest0", rest_raw)
    take(1)
    scoped("rest1", rest, 1)
    with jax.named_scope("havekv"):
        have(0)

    def early(q):
        project_kv(1, q, everything)
        make_state(q)

    def lone(q):
        project_kv(1, q, own_rows)

    def later(q):
        project_qg(1, q, everything)

    scoped("early", over, 0, 2, early)
    take(2)
    scoped("lone", over, 2, seqs, lone)
    scoped("rest2", rest, 2)
    project_kv(1, 2, far_rows)
    scoped("state2", make_state, 2)
    with jax.named_scope("haveqg"):
        have(1)
    scoped("later01", over, 0, 2, later)
    with jax.named_scope("present"):
        @pl.when(z < nz - 1)
        def _():
            pl.semaphore_wait(present, nz - 1 - z)

    scoped("plane0", plane_total, 0)
    scoped("plane1", plane_total, 1)
    take(end)
    scoped("later2", later, 2)
    project_qg(1, end, own_rows)
    with jax.named_scope("take2e"):
        arrived(end, across_twin)
    with jax.named_scope("rest3"):
        for h in range(2):
            project_kv(h, end, far_rows)
        make_state(end)
    scoped("plane2", plane_total, 2)
    with jax.named_scope("qg3"):
        for h in range(2):
            project_qg(h, end, far_rows)
    scoped("inside01", over, 0, 2, inside)
    scoped("back0", hand_back, 0)
    scoped("back1", hand_back, 1)
    scoped("inside2", inside, 2)
    scoped("plane3", plane_total, end)
    scoped("inside3", inside, end)
    scoped("back2", hand_back, 2)
    scoped("finish01", over, 0, 2, finish)
    scoped("back3", hand_back, end)
    scoped("finish23", over, 2, seqs, finish)
    scoped("emit0", emit, 0, end)
    scoped("emit3a", emit_half, end, side, 1)
    scoped("emit3b", emit_half, end, 1 - side, 0)
    scoped("closing", closing, end, rows)

    def sent(took, sem):
        pltpu.make_async_remote_copy(
            took, took, sem, h_recv, device_id={"tp": mirror}, device_id_type=MESH,
        ).wait_send()

    with jax.named_scope("drain"):
        sent(gath.at[:, 0:rows, :], x_send)
        sent(gath.at[:, 0:2 * rows, :], p_send)
        sent(w.at[0, :, :], w_send)
        sent(heads.at[0], w_send)
        sent(s1_in.at[:, 0:2 * NY - 1], s_send.at[0])
        for n in range(nz - 1):
            @pl.when(z == n)
            def _():
                sent(s2_in.at[:, 0:nz - 1 - n], s_send.at[1])
        sent(s3_out.at[:, 0:2 * NY - 1], s_send.at[2])
        sent(g_in.at[:, :, 0:6 * HEAD_DIM], g_send)


def hand_over(source, out, sem):
    copy = pltpu.make_async_copy(source, out, sem)
    copy.start()
    copy.wait()


def solution(mesh):
    tp, sp = mesh.shape["tp"], mesh.shape["sp"]

    def body(tok, gain, wq, wk, wv, wg, decay, ngain, wo, pgain):
        seqs, rows, width = tok.shape
        length = rows * 4
        nz = sp // NY
        part = HEAD_DIM // NY
        half = HEAD_DIM // 2
        inv = np.float32(rope_base) ** (-np.arange(half, dtype=np.float32) / half)
        inv = jnp.asarray(np.concatenate([inv, inv])[None, :], F32)
        dma = pltpu.SemaphoreType.DMA
        hbm = pl.BlockSpec(memory_space=pltpu.HBM)
        vmem = pltpu.VMEM
        wide = vmem((2, seqs, length, HEAD_DIM), BF16)
        mixed = pl.pallas_call(
            functools.partial(kernel, tp, sp),
            out_shape=jax.ShapeDtypeStruct(tok.shape, BF16),
            in_specs=[
                hbm, hbm, hbm, hbm, hbm, hbm,
                pl.BlockSpec(memory_space=pltpu.SMEM), hbm, hbm, hbm, hbm,
            ],
            out_specs=pl.BlockSpec(memory_space=pltpu.VMEM),
            scratch_shapes=[
                vmem((1, width), F32), vmem((1, width), F32), vmem((1, HEAD_DIM), F32),
                vmem((2, 8, HEAD_DIM), F32),
                vmem((seqs - 1, rows, width), BF16),
                vmem((length, width), BF16),
                vmem((seqs, length, width), BF16),
                vmem((2, width, 4 * HEAD_DIM), BF16),
                vmem(wo.shape, BF16),
                vmem((length, HEAD_DIM), F32), vmem((length, HEAD_DIM), F32),
                vmem((2, length, length), F32),
                vmem((2, length, HEAD_DIM), F32), vmem((2, length, HEAD_DIM), F32),
                wide, wide, wide, wide,
                vmem((2, seqs, length, HEAD_DIM), F32),
                vmem((2, seqs, length, HEAD_DIM), F32),
                vmem((2, seqs, HEAD_DIM, HEAD_DIM), BF16),
                vmem((seqs, 2 * NY, part, HEAD_DIM), BF16),
                vmem((seqs, part, HEAD_DIM), BF16),
                vmem((seqs, nz - 1, part, HEAD_DIM), BF16),
                vmem((seqs, 2 * NY, part, HEAD_DIM), BF16),
                vmem((2, seqs, HEAD_DIM, HEAD_DIM), BF16),
                vmem((seqs, length, 2 * HEAD_DIM), BF16),
                vmem((seqs, rows, HEAD_DIM * tp), BF16),
                vmem((seqs * rows, width), F32),
                dma(()), dma(()), dma((seqs, 4)), dma(()), dma((6,)), dma(()),
                dma((3,)), dma((seqs,)), dma((seqs,)), dma((seqs,)), dma(()), dma((2, seqs)),
                dma((8,)), dma(()), dma((seqs,)), pltpu.SemaphoreType.REGULAR,
            ],
            compiler_params=pltpu.CompilerParams(
                collective_id=0, has_side_effects=True, vmem_limit_bytes=40 * 2**20
            ),
            name="retention",
        )(
            *(pltpu.with_memory_space_constraint(x, pltpu.HBM) for x in (tok, gain[None, :], wq, wk, wv, wg)), decay,
            *(pltpu.with_memory_space_constraint(x, pltpu.HBM) for x in (ngain[None, :], wo, pgain[None, :], inv))
        )
        return pl.pallas_call(
            hand_over,
            out_shape=jax.ShapeDtypeStruct(tok.shape, BF16),
            in_specs=[pl.BlockSpec(memory_space=pltpu.VMEM)],
            out_specs=hbm,
            scratch_shapes=[dma(())],
            compiler_params=pltpu.CompilerParams(vmem_limit_bytes=16 * 2**20),
            name="hand_over",
        )(mixed)

    placed = (
        P(None, ("sp", "tp"), None),
        P(),
        P(None, "tp"),
        P(None, "tp"),
        P(None, "tp"),
        P(None, "tp"),
        P("tp"),
        P("tp"),
        P(),
        P(),
    )
    return jax.shard_map(
        body, mesh=mesh, in_specs=placed, out_specs=P(None, ("sp", "tp"), None), check_vma=False
    )
```

```python
import functools

import jax
import jax.numpy as jnp
import numpy as np
from jax import lax
from jax.experimental import pallas as pl
from jax.experimental.pallas import tpu as pltpu
from jax.sharding import PartitionSpec as P

HEAD_DIM = 128
SUB = 128
NY = 4
rms_eps = 1e-06
group_eps = 1e-05
rope_base = 10000.0
MESH = pl.DeviceIdType.MESH
F32 = jnp.float32
BF16 = jnp.bfloat16


def kernel(
    tp, sp,
    tok, gain_h, wq_h, wk_h, wv_h, wg_h, decay, ngain_h, wo_h, pgain_h, inv_h,
    out,
    gain, pgain, inv, heads, tokv, raw, gath, w, wo, cosv, sinv, mask, fade, reach,
    qs, qr, ks, vs, sg, within, s1_out, s1_in, s2_out, s2_in, s3_out, excl,
    g_out, g_in, premix,
    x_send, p_send, t_recv, last_recv, w_send, wx_recv, h_recv,
    s_send, s1_recv, s2_recv, s3_recv, g_send, g_recv,
    w_sem, o_sem, in_sem, present,
):
    seqs, rows, width = tok.shape
    pair = 2 * rows
    length = 2 * pair
    line = rows * tp
    nz = sp // NY
    part = HEAD_DIM // NY
    direct = width // 4
    piece = (width - direct) // NY
    s, t = lax.axis_index("sp"), lax.axis_index("tp")
    z, y = lax.div(s, NY), lax.rem(s, NY)
    chip, core = lax.div(t, 2), lax.rem(t, 2)
    group, side = lax.div(chip, 2), lax.rem(chip, 2)
    base = group * 4
    me = side * 2 + core
    twin = side * 2 + 1 - core
    across = (1 - side) * 2 + core
    across_twin = (1 - side) * 2 + 1 - core
    mirror = (3 - chip) * 2 + core
    slot = y * 2 + group

    def at_rows(who, n):
        return pl.ds(pl.multiple_of(who * n, n), n)

    loads_in = [
        pltpu.make_async_copy(
            tok.at[q], tokv.at[q - 1] if q else raw.at[at_rows(me, rows), :], in_sem.at[q]
        )
        for q in range(seqs)
    ]

    cuts = [slice(i * HEAD_DIM, (i + 1) * HEAD_DIM) for i in range(4)]
    loads_w = [
        pltpu.make_async_copy(a, w.at[0, :, cuts[i]], w_sem.at[i])
        for i, a in enumerate((wk_h, wv_h, wq_h, wg_h))
    ]
    loads = [
        pltpu.make_async_copy(a, b, w_sem.at[4 + i])
        for i, (a, b) in enumerate(
            ((ngain_h, heads.at[0, 1:2, :]), (gain_h, gain), (inv_h, inv), (pgain_h, pgain))
        )
    ]

    def head_of(u, flip):
        c = group * 2 + u // 2
        return ((3 - c) if flip else c) * 2 + u % 2

    loads_o = [
        pltpu.make_async_copy(
            wo_h.at[pl.ds(pl.multiple_of(head_of(i // 2, i % 2) * HEAD_DIM, HEAD_DIM), HEAD_DIM), :],
            wo.at[i * HEAD_DIM:(i + 1) * HEAD_DIM, :], o_sem,
        )
        for i in range(8)
    ]
    for load in loads_in + loads:
        load.start()

    barrier = pltpu.get_barrier_semaphore()

    def greet(dest):
        pl.semaphore_signal(barrier, inc=1, device_id=dest, device_id_type=MESH)

    for u in (twin, across, across_twin):
        greet({"tp": base + u})
    for j in range(1, NY):
        greet({"sp": z * NY + lax.rem(y + j, NY)})
    for j in range(NY):
        greet({"sp": z * NY + lax.rem(y + j, NY), "tp": mirror})
    for d in range(1, nz):
        @pl.when(z + d < nz)
        def _():
            greet({"sp": lax.rem(z + d, nz) * NY + y})

    def cross(i):
        span = pl.ds(pl.multiple_of(direct + y * piece, 128), piece)
        return pltpu.make_async_remote_copy(
            w.at[0, span, cuts[i]], w.at[1, span, cuts[i]], w_send, wx_recv.at[i],
            device_id={"tp": mirror}, device_id_type=MESH,
        )

    def straight(i):
        return pltpu.make_async_remote_copy(
            w.at[0, 0:direct, cuts[i]], w.at[1, 0:direct, cuts[i]],
            w_send, wx_recv.at[4 + i // 2],
            device_id={"tp": mirror}, device_id_type=MESH,
        )

    def along(i, j):
        peer = lax.rem(y + j, NY)
        span = pl.ds(pl.multiple_of(direct + y * piece, 128), piece)
        return pltpu.make_async_remote_copy(
            w.at[1, span, cuts[i]], w.at[1, span, cuts[i]], w_send, wx_recv.at[4 + i // 2],
            device_id={"sp": z * NY + peer}, device_id_type=MESH,
        )

    def pass_on(i):
        cross(i).wait_recv()
        for j in range(1, NY):
            along(i, j).start()

    def have(k):
        took = w.at[1, 0:width - piece, 256 * k:256 * (k + 1)]
        pltpu.make_async_remote_copy(
            took, took, w_send, wx_recv.at[4 + k], device_id={"tp": mirror}, device_id_type=MESH,
        ).wait_recv()

    def head_copy():
        return pltpu.make_async_remote_copy(
            heads.at[0], heads.at[1], w_send, h_recv, device_id={"tp": mirror}, device_id_type=MESH,
        )

    def block_copy(q, u, dest, sem):
        held = raw.at[at_rows(u, rows), :] if q is None else gath.at[q, at_rows(u, rows), :]
        return pltpu.make_async_remote_copy(
            held, held, sem, t_recv.at[0 if q is None else q, u],
            device_id={"tp": base + dest}, device_id_type=MESH,
        )

    def arrived(q, u):
        block_copy(q, u, twin, x_send).wait_recv()

    def normalise(source, q, u):
        def norm(i, _):
            x = source(pl.multiple_of(i * 16, 16)).astype(F32)
            scale = lax.rsqrt(jnp.mean(x * x, axis=-1, keepdims=True) + rms_eps)
            to = pl.ds(pl.multiple_of(u * rows + i * 16, 16), 16)
            gath[q, to, :] = (x * scale * gain[...]).astype(BF16)
            return 0

        lax.fori_loop(0, rows // 16, norm, 0, unroll=2)

    def norm_own(q):
        loads_in[q].wait()
        normalise(lambda at: tokv[q - 1, pl.ds(at, 16), :], q, me)

    def norm_raw(u):
        normalise(lambda at: raw[pl.ds(pl.multiple_of(u * rows + at, 16), 16), :], 0, u)

    def send(q):
        block_copy(q, me, across, x_send).start()
        block_copy(q, me, twin, p_send).start()

    def last_copy(u, late, dest, sem, arrival):
        span = pl.ds(pl.multiple_of(u * rows + late * (rows - 16), 16), 16 if late else rows - 16)
        held = gath.at[seqs - 1, span, :]
        return pltpu.make_async_remote_copy(
            held, held, sem, arrival, device_id={"tp": base + dest}, device_id_type=MESH,
        )

    def take_last():
        for late in range(2):
            with jax.named_scope("takelast"):
                last_copy(across, late, twin, p_send, last_recv.at[late]).wait_recv()
            last_copy(across, late, twin, p_send, t_recv.at[seqs - 1, across]).start()

    with jax.named_scope("load0"):
        loads_in[0].wait()
    for load in loads_w:
        load.start()
    with jax.named_scope("barrier"):
        pl.semaphore_wait(barrier, 3 + NY - 1 + NY + z)
    block_copy(None, me, across, x_send).start()
    block_copy(None, me, twin, p_send).start()
    for d in range(1, nz):
        @pl.when(z >= d)
        def _():
            pl.semaphore_signal(
                present, inc=1, device_id={"sp": lax.rem(z + nz - d, nz) * NY + y},
                device_id_type=MESH,
            )
    with jax.named_scope("norm"):
        loads[0].wait()
        heads[0, 0:1, :] = jnp.full((1, HEAD_DIM), decay[0], F32)
        loads[1].wait()
        norm_own(1)
        head_copy().start()
        norm_own(2)
        send(1)
        for i in range(4):
            loads_w[i].wait()
            cross(i).start()
        for i in range(4):
            straight(i).start()
        for load in loads_o:
            load.start()
        norm_own(3)
        send(2)
        for late in range(2):
            last_copy(me, late, across, x_send, last_recv.at[late]).start()
        block_copy(seqs - 1, me, twin, p_send).start()
        norm_raw(me)

    with jax.named_scope("tables"):
        loads[2].wait()
        place = s * line + group * length + lax.broadcasted_iota(jnp.int32, (length, HEAD_DIM), 0)
        angle = place.astype(F32) * inv[...]
        cosv[...] = jnp.cos(angle)
        lane = lax.broadcasted_iota(jnp.int32, (length, HEAD_DIM), 1)
        sine = jnp.sin(angle)
        sinv[...] = jnp.where(lane < HEAD_DIM // 2, -sine, sine)

    def tables(h):
        rate = heads[h, 0:1, :]
        spot = lax.broadcasted_iota(jnp.int32, (length, HEAD_DIM), 0)
        fade[h] = jnp.exp(rate * (length - 1 - spot).astype(F32))
        reach[h] = jnp.exp(rate * (1 + spot).astype(F32))
        for c in range(length // HEAD_DIM):
            gap = spot - c * HEAD_DIM - lax.broadcasted_iota(jnp.int32, (length, HEAD_DIM), 1)
            weight = jnp.exp(rate * jnp.maximum(gap, 0).astype(F32))
            mask[h, :, c * HEAD_DIM:(c + 1) * HEAD_DIM] = jnp.where(gap >= 0, weight, 0.0)

    with jax.named_scope("tables0"):
        tables(0)

    def rotate(x, span):
        x = x.astype(BF16).astype(F32)
        return x * cosv[span, :] + pltpu.roll(x, HEAD_DIM // 2, 1) * sinv[span, :]

    def project_kv(h, q, span):
        r = jnp.dot(gath[q, span, :], w[h, :, 0:256], preferred_element_type=F32)
        ks[h, q, span, :] = (rotate(r[:, cuts[0]], span) * HEAD_DIM ** (-0.5)).astype(BF16)
        vs[h, q, span, :] = r[:, cuts[1]].astype(BF16)

    def project_qg(h, q, span):
        r = jnp.dot(gath[q, span, :], w[h, :, 256:512], preferred_element_type=F32)
        query = rotate(r[:, cuts[0]], span).astype(BF16)
        qs[h, q, span, :] = query
        qr[h, q, span, :] = (query.astype(F32) * reach[h, span, :]).astype(BF16)
        gate = r[:, cuts[1]].astype(BF16).astype(F32)
        sg[h, q, span, :] = heads[h, 1:2, :] * (gate * jax.nn.sigmoid(gate))

    everything = slice(0, length)
    own_rows = at_rows(side, pair)
    far_rows = at_rows(1 - side, pair)

    def power(n):
        return jnp.exp(jnp.full((1, 1), decay[0] * n, F32))

    def s1_copy(q, h, j):
        peer = lax.rem(y + j, NY)
        dest = {"sp": z * NY + peer, "tp": mirror} if h else {"sp": z * NY + peer}
        return pltpu.make_async_remote_copy(
            s1_out.at[h, q, at_rows(peer, part), :], s1_in.at[q, slot],
            s_send.at[0], s1_recv.at[q], device_id=dest, device_id_type=MESH,
        )

    def make_state(q):
        for h in range(2):
            scaled = (ks[h, q].astype(F32) * fade[h]).astype(BF16)
            total = lax.dot_general(
                scaled, vs[h, q], (((0,), (0,)), ((), ())), preferred_element_type=F32
            )
            s1_out[h, q] = total.astype(BF16)
        for j in range(NY):
            s1_copy(q, 1, j).start()
            if j:
                s1_copy(q, 0, j).start()
        s1_in[q, slot] = s1_out[0, q, at_rows(y, part), :]

    def s2_copy(q, d):
        return pltpu.make_async_remote_copy(
            s2_out.at[q], s2_in.at[q, d - 1], s_send.at[1], s2_recv.at[q],
            device_id={"sp": lax.rem(z + d, nz) * NY + y}, device_id_type=MESH,
        )

    def plane_total(q):
        took = s1_in.at[q, 0:2 * NY - 1]
        pltpu.make_async_remote_copy(
            took, took, s_send.at[0], s1_recv.at[q], device_id={"tp": mirror}, device_id_type=MESH,
        ).wait_recv()
        step = power(length)
        total = s1_in[q, 0].astype(F32)
        for k in range(1, 2 * NY):
            total = total * step + s1_in[q, k].astype(F32)
        s2_out[q] = total.astype(BF16)
        for d in range(1, nz):
            @pl.when(z + d < nz)
            def _():
                s2_copy(q, d).start()

    def s3_copy(q, h, j):
        peer = lax.rem(y + j, NY)
        dest = {"sp": z * NY + peer, "tp": mirror} if h else {"sp": z * NY + peer}
        return pltpu.make_async_remote_copy(
            s3_out.at[q, peer * 2 + (1 - group if h else group)],
            excl.at[h, q, at_rows(y, part), :],
            s_send.at[2], s3_recv.at[q], device_id=dest, device_id_type=MESH,
        )

    def hand_back(q):
        for n in range(1, nz):
            @pl.when(z == n)
            def _():
                took = s2_in.at[q, 0:n]
                pltpu.make_async_remote_copy(
                    took, took, s_send.at[1], s2_recv.at[q],
                    device_id={"tp": mirror}, device_id_type=MESH,
                ).wait_recv()

        def add(d, total):
            return total + power(line * NY * d) * s2_in[q, d].astype(F32)

        before = lax.fori_loop(0, z, add, jnp.zeros((part, HEAD_DIM), F32))
        step = power(length)
        for k in range(2 * NY):
            s3_out[q, k] = before.astype(BF16)
            before = before * step + s1_in[q, k].astype(F32)
        for j in range(NY):
            s3_copy(q, 1, j).start()
            if j:
                s3_copy(q, 0, j).start()
        excl[0, q, at_rows(y, part), :] = s3_out[q, slot]

    def inside(q):
        for h in range(2):
            for i in range(length // SUB):
                here, upto = slice(i * SUB, (i + 1) * SUB), slice(0, (i + 1) * SUB)
                score = lax.dot_general(
                    qs[h, q, here, :], ks[h, q, upto, :],
                    (((1,), (1,)), ((), ())), preferred_element_type=F32,
                )
                weight = (score * mask[h, here, upto]).astype(BF16)
                within[h, q, here, :] = jnp.dot(
                    weight, vs[h, q, upto, :], preferred_element_type=F32
                )

    def gated_copy(q, dest, source, near_by=0):
        return pltpu.make_async_remote_copy(
            g_out.at[q, at_rows(dest, rows), :], g_in.at[q, :, at_rows(source, 2 * HEAD_DIM)],
            g_send, g_recv.at[near_by, q],
            device_id={"tp": base + dest}, device_id_type=MESH,
        )

    def finish(q):
        took = s1_in.at[q, 0:2 * NY - 1]
        pltpu.make_async_remote_copy(
            took, took, s_send.at[2], s3_recv.at[q], device_id={"tp": mirror}, device_id_type=MESH,
        ).wait_recv()
        for k in range(2):
            here = at_rows((1 - side) if k == 0 else side, pair)
            for h in range(2):
                kept = within[h, q, here, :] + jnp.dot(
                    qr[h, q, here, :], excl[h, q], preferred_element_type=F32
                )
                kept = kept - jnp.mean(kept, axis=-1, keepdims=True)
                spread = jnp.mean(kept * kept, axis=-1, keepdims=True)
                normal = kept * lax.rsqrt(spread + group_eps) * sg[h, q, here, :]
                g_out[q, here, cuts[h]] = normal.astype(BF16)
            if k == 0:
                gated_copy(q, across, me).start()
                gated_copy(q, across_twin, me).start()
            else:
                gated_copy(q, twin, me, 1).start()
                g_in[q, :, at_rows(me, 2 * HEAD_DIM)] = g_out[q, at_rows(me, rows), :]

    def gated_wait(q, near_by):
        took = g_in.at[q, :, 0:(2 if near_by else 4) * HEAD_DIM]
        pltpu.make_async_remote_copy(
            took, took, g_send, g_recv.at[near_by, q],
            device_id={"tp": mirror}, device_id_type=MESH,
        ).wait_recv()

    step = 512
    side_cols = 4 * HEAD_DIM

    def closing(lo, n):
        def norm(i, _):
            at = pl.multiple_of(i * 16, 16)
            x = premix[pl.ds(at, 16), :]
            scale = lax.rsqrt(jnp.mean(x * x, axis=-1, keepdims=True) + rms_eps)
            q = lo + lax.div(i, rows // 16)
            to = pl.multiple_of(lax.rem(i, rows // 16) * 16, 16)
            out[q, pl.ds(to, 16), :] = (x * scale * pgain[...]).astype(BF16)
            return 0

        lax.fori_loop(0, n // 16, norm, 0, unroll=2)

    def emit(lo, hi):
        n = (hi - lo) * rows
        with jax.named_scope("gated_wait"):
            for q in range(lo, hi):
                gated_wait(q, 0)
                gated_wait(q, 1)
        g = g_in[lo:hi].reshape(n, g_in.shape[2])
        for c in range(width // step):
            cut = slice(c * step, (c + 1) * step)
            premix[0:n, cut] = jnp.dot(g, wo[:, cut], preferred_element_type=F32)
        closing(lo, n)

    def emit_half(lo, hi, which, near_by):
        for q in range(lo, hi):
            gated_wait(q, near_by)
        n = (hi - lo) * rows
        span = at_rows(which, side_cols)
        g = g_in[lo:hi, :, span].reshape(n, side_cols)
        for c in range(width // step):
            cut = slice(c * step, (c + 1) * step)
            term = jnp.dot(g, wo[span, cut], preferred_element_type=F32)
            premix[0:n, cut] = term if near_by else premix[0:n, cut] + term

    def scoped(name, function, *args):
        with jax.named_scope(name):
            function(*args)

    def over(lo, hi, function):
        def run(q, _):
            function(q)
            return 0

        lax.fori_loop(lo, hi, run, 0)

    def near(q):
        arrived(q, twin)
        project_kv(0, q, own_rows)
        project_qg(0, q, own_rows)

    def near_raw():
        arrived(None, twin)
        norm_raw(twin)
        project_kv(0, 0, own_rows)
        project_qg(0, 0, own_rows)

    def take(q):
        with jax.named_scope("take"):
            arrived(q, across)
        block_copy(q, across, twin, p_send).start()

    def rest(q):
        with jax.named_scope("take2"):
            arrived(q, across_twin)
        project_kv(0, q, far_rows)
        project_qg(0, q, far_rows)

    def rest_raw():
        norm_raw(across)
        with jax.named_scope("take2"):
            arrived(None, across_twin)
        norm_raw(across_twin)
        project_kv(0, 0, far_rows)
        project_qg(0, 0, far_rows)

    end = seqs - 1
    scoped("near0", near_raw)
    scoped("pass0", pass_on, 0)
    scoped("near123", over, 1, seqs, near)
    scoped("pass1", pass_on, 1)
    with jax.named_scope("tables1"):
        head_copy().wait_recv()
        tables(1)
    loads[3].wait()
    pltpu.make_async_copy(wo_h, wo, o_sem).wait()
    scoped("pass2", pass_on, 2)
    take(None)
    scoped("pass3", pass_on, 3)
    scoped("rest0", rest_raw)
    take(1)
    scoped("rest1", rest, 1)
    with jax.named_scope("havekv"):
        have(0)

    def early(q):
        project_kv(1, q, everything)
        make_state(q)

    def lone(q):
        project_kv(1, q, own_rows)

    def later(q):
        project_qg(1, q, everything)

    scoped("early", over, 0, 2, early)
    take(2)
    scoped("lone", over, 2, seqs, lone)
    scoped("rest2", rest, 2)
    project_kv(1, 2, far_rows)
    scoped("state2", make_state, 2)
    with jax.named_scope("haveqg"):
        have(1)
    take_last()
    scoped("later0", over, 0, 1, later)
    with jax.named_scope("present"):
        @pl.when(z < nz - 1)
        def _():
            pl.semaphore_wait(present, nz - 1 - z)

    scoped("plane0", plane_total, 0)
    project_qg(1, end, own_rows)
    scoped("plane1", plane_total, 1)
    with jax.named_scope("take2e"):
        arrived(end, across_twin)
    with jax.named_scope("rest3"):
        for h in range(2):
            project_kv(h, end, far_rows)
        make_state(end)
    scoped("plane2", plane_total, 2)
    with jax.named_scope("qg3"):
        for h in range(2):
            project_qg(h, end, far_rows)
    scoped("later12", over, 1, seqs - 1, later)
    scoped("back0", hand_back, 0)
    scoped("back1", hand_back, 1)
    scoped("inside01", over, 0, 2, inside)
    scoped("plane3", plane_total, end)
    scoped("back2", hand_back, 2)
    scoped("inside23", over, 2, seqs, inside)
    scoped("back3", hand_back, end)
    scoped("finish01", over, 0, 2, finish)
    scoped("finish23", over, 2, seqs, finish)
    scoped("emit0", emit, 0, 2)
    scoped("emit2", emit, 2, end)
    scoped("emit3a", emit_half, end, seqs, side, 1)
    scoped("emit3b", emit_half, end, seqs, 1 - side, 0)
    scoped("closing", closing, end, rows)

    def sent(took, sem):
        pltpu.make_async_remote_copy(
            took, took, sem, h_recv, device_id={"tp": mirror}, device_id_type=MESH,
        ).wait_send()

    with jax.named_scope("drain"):
        sent(gath.at[:, 0:rows, :], x_send)
        sent(gath.at[:, 0:2 * rows, :], p_send)
        sent(w.at[0, :, :], w_send)
        sent(heads.at[0], w_send)
        sent(s1_in.at[:, 0:2 * NY - 1], s_send.at[0])
        for n in range(nz - 1):
            @pl.when(z == n)
            def _():
                sent(s2_in.at[:, 0:nz - 1 - n], s_send.at[1])
        sent(s3_out.at[:, 0:2 * NY - 1], s_send.at[2])
        sent(g_in.at[:, :, 0:6 * HEAD_DIM], g_send)


def hand_over(source, out, sem):
    copy = pltpu.make_async_copy(source, out, sem)
    copy.start()
    copy.wait()


def solution(mesh):
    tp, sp = mesh.shape["tp"], mesh.shape["sp"]

    def body(tok, gain, wq, wk, wv, wg, decay, ngain, wo, pgain):
        seqs, rows, width = tok.shape
        length = rows * 4
        nz = sp // NY
        part = HEAD_DIM // NY
        half = HEAD_DIM // 2
        inv = np.float32(rope_base) ** (-np.arange(half, dtype=np.float32) / half)
        inv = jnp.asarray(np.concatenate([inv, inv])[None, :], F32)
        dma = pltpu.SemaphoreType.DMA
        hbm = pl.BlockSpec(memory_space=pltpu.HBM)
        vmem = pltpu.VMEM
        wide = vmem((2, seqs, length, HEAD_DIM), BF16)
        mixed = pl.pallas_call(
            functools.partial(kernel, tp, sp),
            out_shape=jax.ShapeDtypeStruct(tok.shape, BF16),
            in_specs=[
                hbm, hbm, hbm, hbm, hbm, hbm,
                pl.BlockSpec(memory_space=pltpu.SMEM), hbm, hbm, hbm, hbm,
            ],
            out_specs=pl.BlockSpec(memory_space=pltpu.VMEM),
            scratch_shapes=[
                vmem((1, width), F32), vmem((1, width), F32), vmem((1, HEAD_DIM), F32),
                vmem((2, 8, HEAD_DIM), F32),
                vmem((seqs - 1, rows, width), BF16),
                vmem((length, width), BF16),
                vmem((seqs, length, width), BF16),
                vmem((2, width, 4 * HEAD_DIM), BF16),
                vmem(wo.shape, BF16),
                vmem((length, HEAD_DIM), F32), vmem((length, HEAD_DIM), F32),
                vmem((2, length, length), F32),
                vmem((2, length, HEAD_DIM), F32), vmem((2, length, HEAD_DIM), F32),
                wide, wide, wide, wide,
                vmem((2, seqs, length, HEAD_DIM), F32),
                vmem((2, seqs, length, HEAD_DIM), F32),
                vmem((2, seqs, HEAD_DIM, HEAD_DIM), BF16),
                vmem((seqs, 2 * NY, part, HEAD_DIM), BF16),
                vmem((seqs, part, HEAD_DIM), BF16),
                vmem((seqs, nz - 1, part, HEAD_DIM), BF16),
                vmem((seqs, 2 * NY, part, HEAD_DIM), BF16),
                vmem((2, seqs, HEAD_DIM, HEAD_DIM), BF16),
                vmem((seqs, length, 2 * HEAD_DIM), BF16),
                vmem((seqs, rows, HEAD_DIM * tp), BF16),
                vmem((seqs * rows, width), F32),
                dma(()), dma(()), dma((seqs, 4)), dma((2,)), dma(()), dma((6,)), dma(()),
                dma((3,)), dma((seqs,)), dma((seqs,)), dma((seqs,)), dma(()), dma((2, seqs)),
                dma((8,)), dma(()), dma((seqs,)), pltpu.SemaphoreType.REGULAR,
            ],
            compiler_params=pltpu.CompilerParams(
                collective_id=0, has_side_effects=True, vmem_limit_bytes=40 * 2**20
            ),
            name="retention",
        )(
            *(pltpu.with_memory_space_constraint(x, pltpu.HBM) for x in (tok, gain[None, :], wq, wk, wv, wg)), decay,
            *(pltpu.with_memory_space_constraint(x, pltpu.HBM) for x in (ngain[None, :], wo, pgain[None, :], inv))
        )
        return pl.pallas_call(
            hand_over,
            out_shape=jax.ShapeDtypeStruct(tok.shape, BF16),
            in_specs=[pl.BlockSpec(memory_space=pltpu.VMEM)],
            out_specs=hbm,
            scratch_shapes=[dma(())],
            compiler_params=pltpu.CompilerParams(vmem_limit_bytes=16 * 2**20),
            name="hand_over",
        )(mixed)

    placed = (
        P(None, ("sp", "tp"), None),
        P(),
        P(None, "tp"),
        P(None, "tp"),
        P(None, "tp"),
        P(None, "tp"),
        P("tp"),
        P("tp"),
        P(),
        P(),
    )
    return jax.shard_map(
        body, mesh=mesh, in_specs=placed, out_specs=P(None, ("sp", "tp"), None), check_vma=False
    )
```

```python
import functools

import jax
import jax.numpy as jnp
import numpy as np
from jax import lax
from jax.experimental import pallas as pl
from jax.experimental.pallas import tpu as pltpu
from jax.sharding import PartitionSpec as P

HEAD_DIM = 128
SUB = 128
NY = 4
rms_eps = 1e-06
group_eps = 1e-05
rope_base = 10000.0
MESH = pl.DeviceIdType.MESH
F32 = jnp.float32
BF16 = jnp.bfloat16


def kernel(
    tp, sp,
    tok, gain_h, wq_h, wk_h, wv_h, wg_h, decay, ngain_h, wo_h, pgain_h, inv_h,
    out, premix, pgain,
    gain, inv, heads, tokv, raw, gath, w, wo, cosv, sinv, mask, fade, reach,
    qs, qr, ks, vs, sg, within, s1_out, s1_in, s2_out, s2_in, s3_out, excl,
    g_out, g_in,
    x_send, p_send, t_recv, last_recv, w_send, wx_recv, h_recv,
    s_send, s1_recv, s2_recv, s3_recv, g_send, g_recv,
    w_sem, o_sem, in_sem, present,
):
    seqs, rows, width = tok.shape
    pair = 2 * rows
    length = 2 * pair
    line = rows * tp
    nz = sp // NY
    part = HEAD_DIM // NY
    direct = width // 4
    piece = (width - direct) // NY
    s, t = lax.axis_index("sp"), lax.axis_index("tp")
    z, y = lax.div(s, NY), lax.rem(s, NY)
    chip, core = lax.div(t, 2), lax.rem(t, 2)
    group, side = lax.div(chip, 2), lax.rem(chip, 2)
    base = group * 4
    me = side * 2 + core
    twin = side * 2 + 1 - core
    across = (1 - side) * 2 + core
    across_twin = (1 - side) * 2 + 1 - core
    mirror = (3 - chip) * 2 + core
    slot = y * 2 + group

    def at_rows(who, n):
        return pl.ds(pl.multiple_of(who * n, n), n)

    loads_in = [
        pltpu.make_async_copy(
            tok.at[q], tokv.at[q - 1] if q else raw.at[at_rows(me, rows), :], in_sem.at[q]
        )
        for q in range(seqs)
    ]

    cuts = [slice(i * HEAD_DIM, (i + 1) * HEAD_DIM) for i in range(4)]
    loads_w = [
        pltpu.make_async_copy(a, w.at[0, :, cuts[i]], w_sem.at[i])
        for i, a in enumerate((wk_h, wv_h, wq_h, wg_h))
    ]
    loads = [
        pltpu.make_async_copy(a, b, w_sem.at[4 + i])
        for i, (a, b) in enumerate(
            ((ngain_h, heads.at[0, 1:2, :]), (gain_h, gain), (inv_h, inv), (pgain_h, pgain))
        )
    ]

    def head_of(u, flip):
        c = group * 2 + u // 2
        return ((3 - c) if flip else c) * 2 + u % 2

    loads_o = [
        pltpu.make_async_copy(
            wo_h.at[pl.ds(pl.multiple_of(head_of(i // 2, i % 2) * HEAD_DIM, HEAD_DIM), HEAD_DIM), :],
            wo.at[i * HEAD_DIM:(i + 1) * HEAD_DIM, :], o_sem,
        )
        for i in range(8)
    ]
    for load in loads_in + loads:
        load.start()

    barrier = pltpu.get_barrier_semaphore()

    def greet(dest):
        pl.semaphore_signal(barrier, inc=1, device_id=dest, device_id_type=MESH)

    for u in (twin, across, across_twin):
        greet({"tp": base + u})
    for j in range(1, NY):
        greet({"sp": z * NY + lax.rem(y + j, NY)})
    for j in range(NY):
        greet({"sp": z * NY + lax.rem(y + j, NY), "tp": mirror})
    for d in range(1, nz):
        @pl.when(z + d < nz)
        def _():
            greet({"sp": lax.rem(z + d, nz) * NY + y})

    def cross(i):
        span = pl.ds(pl.multiple_of(direct + y * piece, 128), piece)
        return pltpu.make_async_remote_copy(
            w.at[0, span, cuts[i]], w.at[1, span, cuts[i]], w_send, wx_recv.at[i],
            device_id={"tp": mirror}, device_id_type=MESH,
        )

    def straight(i):
        return pltpu.make_async_remote_copy(
            w.at[0, 0:direct, cuts[i]], w.at[1, 0:direct, cuts[i]],
            w_send, wx_recv.at[4 + i // 2],
            device_id={"tp": mirror}, device_id_type=MESH,
        )

    def along(i, j):
        peer = lax.rem(y + j, NY)
        span = pl.ds(pl.multiple_of(direct + y * piece, 128), piece)
        return pltpu.make_async_remote_copy(
            w.at[1, span, cuts[i]], w.at[1, span, cuts[i]], w_send, wx_recv.at[4 + i // 2],
            device_id={"sp": z * NY + peer}, device_id_type=MESH,
        )

    def pass_on(i):
        cross(i).wait_recv()
        for j in range(1, NY):
            along(i, j).start()

    def have(k):
        took = w.at[1, 0:width - piece, 256 * k:256 * (k + 1)]
        pltpu.make_async_remote_copy(
            took, took, w_send, wx_recv.at[4 + k], device_id={"tp": mirror}, device_id_type=MESH,
        ).wait_recv()

    def head_copy():
        return pltpu.make_async_remote_copy(
            heads.at[0], heads.at[1], w_send, h_recv, device_id={"tp": mirror}, device_id_type=MESH,
        )

    def block_copy(q, u, dest, sem):
        held = raw.at[at_rows(u, rows), :] if q is None else gath.at[q, at_rows(u, rows), :]
        return pltpu.make_async_remote_copy(
            held, held, sem, t_recv.at[0 if q is None else q, u],
            device_id={"tp": base + dest}, device_id_type=MESH,
        )

    def arrived(q, u):
        block_copy(q, u, twin, x_send).wait_recv()

    def normalise(source, q, u):
        def norm(i, _):
            x = source(pl.multiple_of(i * 16, 16)).astype(F32)
            scale = lax.rsqrt(jnp.mean(x * x, axis=-1, keepdims=True) + rms_eps)
            to = pl.ds(pl.multiple_of(u * rows + i * 16, 16), 16)
            gath[q, to, :] = (x * scale * gain[...]).astype(BF16)
            return 0

        lax.fori_loop(0, rows // 16, norm, 0, unroll=2)

    def norm_own(q):
        loads_in[q].wait()
        normalise(lambda at: tokv[q - 1, pl.ds(at, 16), :], q, me)

    def norm_raw(u):
        normalise(lambda at: raw[pl.ds(pl.multiple_of(u * rows + at, 16), 16), :], 0, u)

    def send(q):
        block_copy(q, me, across, x_send).start()
        block_copy(q, me, twin, p_send).start()

    def last_copy(u, late, dest, sem, arrival):
        span = pl.ds(pl.multiple_of(u * rows + late * (rows - 16), 16), 16 if late else rows - 16)
        held = gath.at[seqs - 1, span, :]
        return pltpu.make_async_remote_copy(
            held, held, sem, arrival, device_id={"tp": base + dest}, device_id_type=MESH,
        )

    def take_last():
        for late in range(2):
            with jax.named_scope("takelast"):
                last_copy(across, late, twin, p_send, last_recv.at[late]).wait_recv()
            last_copy(across, late, twin, p_send, t_recv.at[seqs - 1, across]).start()

    with jax.named_scope("load0"):
        loads_in[0].wait()
    for load in loads_w:
        load.start()
    with jax.named_scope("barrier"):
        pl.semaphore_wait(barrier, 3 + NY - 1 + NY + z)
    block_copy(None, me, across, x_send).start()
    block_copy(None, me, twin, p_send).start()
    for d in range(1, nz):
        @pl.when(z >= d)
        def _():
            pl.semaphore_signal(
                present, inc=1, device_id={"sp": lax.rem(z + nz - d, nz) * NY + y},
                device_id_type=MESH,
            )
    with jax.named_scope("norm"):
        loads[0].wait()
        heads[0, 0:1, :] = jnp.full((1, HEAD_DIM), decay[0], F32)
        loads[1].wait()
        norm_own(1)
        head_copy().start()
        norm_own(2)
        send(1)
        for i in range(4):
            loads_w[i].wait()
            cross(i).start()
        for i in range(4):
            straight(i).start()
        for load in loads_o:
            load.start()
        norm_own(3)
        norm_raw(me)
        send(2)
        for late in range(2):
            last_copy(me, late, across, x_send, last_recv.at[late]).start()
        block_copy(seqs - 1, me, twin, p_send).start()

    with jax.named_scope("tables"):
        loads[2].wait()
        place = s * line + group * length + lax.broadcasted_iota(jnp.int32, (length, HEAD_DIM), 0)
        angle = place.astype(F32) * inv[...]
        cosv[...] = jnp.cos(angle)
        lane = lax.broadcasted_iota(jnp.int32, (length, HEAD_DIM), 1)
        sine = jnp.sin(angle)
        sinv[...] = jnp.where(lane < HEAD_DIM // 2, -sine, sine)

    def tables(h):
        rate = heads[h, 0:1, :]
        spot = lax.broadcasted_iota(jnp.int32, (length, HEAD_DIM), 0)
        fade[h] = jnp.exp(rate * (length - 1 - spot).astype(F32))
        reach[h] = jnp.exp(rate * (1 + spot).astype(F32))
        for c in range(length // HEAD_DIM):
            gap = spot - c * HEAD_DIM - lax.broadcasted_iota(jnp.int32, (length, HEAD_DIM), 1)
            weight = jnp.exp(rate * jnp.maximum(gap, 0).astype(F32))
            mask[h, :, c * HEAD_DIM:(c + 1) * HEAD_DIM] = jnp.where(gap >= 0, weight, 0.0)

    with jax.named_scope("tables0"):
        tables(0)

    def rotate(x, span):
        x = x.astype(BF16).astype(F32)
        return x * cosv[span, :] + pltpu.roll(x, HEAD_DIM // 2, 1) * sinv[span, :]

    def project_kv(h, q, span):
        r = jnp.dot(gath[q, span, :], w[h, :, 0:256], preferred_element_type=F32)
        ks[h, q, span, :] = (rotate(r[:, cuts[0]], span) * HEAD_DIM ** (-0.5)).astype(BF16)
        vs[h, q, span, :] = r[:, cuts[1]].astype(BF16)

    def project_qg(h, q, span):
        r = jnp.dot(gath[q, span, :], w[h, :, 256:512], preferred_element_type=F32)
        query = rotate(r[:, cuts[0]], span).astype(BF16)
        qs[h, q, span, :] = query
        qr[h, q, span, :] = (query.astype(F32) * reach[h, span, :]).astype(BF16)
        gate = r[:, cuts[1]].astype(BF16).astype(F32)
        sg[h, q, span, :] = heads[h, 1:2, :] * (gate * jax.nn.sigmoid(gate))

    everything = slice(0, length)
    own_rows = at_rows(side, pair)
    far_rows = at_rows(1 - side, pair)

    def power(n):
        return jnp.exp(jnp.full((1, 1), decay[0] * n, F32))

    def s1_copy(q, h, j):
        peer = lax.rem(y + j, NY)
        dest = {"sp": z * NY + peer, "tp": mirror} if h else {"sp": z * NY + peer}
        return pltpu.make_async_remote_copy(
            s1_out.at[h, q, at_rows(peer, part), :], s1_in.at[q, slot],
            s_send.at[0], s1_recv.at[q], device_id=dest, device_id_type=MESH,
        )

    def make_state(q):
        for h in range(2):
            scaled = (ks[h, q].astype(F32) * fade[h]).astype(BF16)
            total = lax.dot_general(
                scaled, vs[h, q], (((0,), (0,)), ((), ())), preferred_element_type=F32
            )
            s1_out[h, q] = total.astype(BF16)
        for j in range(NY):
            s1_copy(q, 1, j).start()
            if j:
                s1_copy(q, 0, j).start()
        s1_in[q, slot] = s1_out[0, q, at_rows(y, part), :]

    def s2_copy(q, d):
        return pltpu.make_async_remote_copy(
            s2_out.at[q], s2_in.at[q, d - 1], s_send.at[1], s2_recv.at[q],
            device_id={"sp": lax.rem(z + d, nz) * NY + y}, device_id_type=MESH,
        )

    def plane_total(q):
        took = s1_in.at[q, 0:2 * NY - 1]
        pltpu.make_async_remote_copy(
            took, took, s_send.at[0], s1_recv.at[q], device_id={"tp": mirror}, device_id_type=MESH,
        ).wait_recv()
        step = power(length)
        total = s1_in[q, 0].astype(F32)
        for k in range(1, 2 * NY):
            total = total * step + s1_in[q, k].astype(F32)
        s2_out[q] = total.astype(BF16)
        for d in range(1, nz):
            @pl.when(z + d < nz)
            def _():
                s2_copy(q, d).start()

    def s3_copy(q, h, j):
        peer = lax.rem(y + j, NY)
        dest = {"sp": z * NY + peer, "tp": mirror} if h else {"sp": z * NY + peer}
        return pltpu.make_async_remote_copy(
            s3_out.at[q, peer * 2 + (1 - group if h else group)],
            excl.at[h, q, at_rows(y, part), :],
            s_send.at[2], s3_recv.at[q], device_id=dest, device_id_type=MESH,
        )

    def hand_back(q):
        for n in range(1, nz):
            @pl.when(z == n)
            def _():
                took = s2_in.at[q, 0:n]
                pltpu.make_async_remote_copy(
                    took, took, s_send.at[1], s2_recv.at[q],
                    device_id={"tp": mirror}, device_id_type=MESH,
                ).wait_recv()

        def add(d, total):
            return total + power(line * NY * d) * s2_in[q, d].astype(F32)

        before = lax.fori_loop(0, z, add, jnp.zeros((part, HEAD_DIM), F32))
        step = power(length)
        for k in range(2 * NY):
            s3_out[q, k] = before.astype(BF16)
            before = before * step + s1_in[q, k].astype(F32)
        for j in range(NY):
            s3_copy(q, 1, j).start()
            if j:
                s3_copy(q, 0, j).start()
        excl[0, q, at_rows(y, part), :] = s3_out[q, slot]

    def inside(q):
        for h in range(2):
            for i in range(length // SUB):
                here, upto = slice(i * SUB, (i + 1) * SUB), slice(0, (i + 1) * SUB)
                score = lax.dot_general(
                    qs[h, q, here, :], ks[h, q, upto, :],
                    (((1,), (1,)), ((), ())), preferred_element_type=F32,
                )
                weight = (score * mask[h, here, upto]).astype(BF16)
                within[h, q, here, :] = jnp.dot(
                    weight, vs[h, q, upto, :], preferred_element_type=F32
                )

    def gated_copy(q, dest, source, near_by=0):
        return pltpu.make_async_remote_copy(
            g_out.at[q, at_rows(dest, rows), :], g_in.at[q, :, at_rows(source, 2 * HEAD_DIM)],
            g_send, g_recv.at[near_by, q],
            device_id={"tp": base + dest}, device_id_type=MESH,
        )

    def finish(q):
        took = s1_in.at[q, 0:2 * NY - 1]
        pltpu.make_async_remote_copy(
            took, took, s_send.at[2], s3_recv.at[q], device_id={"tp": mirror}, device_id_type=MESH,
        ).wait_recv()
        for k in range(2):
            here = at_rows((1 - side) if k == 0 else side, pair)
            for h in range(2):
                kept = within[h, q, here, :] + jnp.dot(
                    qr[h, q, here, :], excl[h, q], preferred_element_type=F32
                )
                kept = kept - jnp.mean(kept, axis=-1, keepdims=True)
                spread = jnp.mean(kept * kept, axis=-1, keepdims=True)
                normal = kept * lax.rsqrt(spread + group_eps) * sg[h, q, here, :]
                g_out[q, here, cuts[h]] = normal.astype(BF16)
            if k == 0:
                gated_copy(q, across, me).start()
                gated_copy(q, across_twin, me).start()
            else:
                gated_copy(q, twin, me, 1).start()
                g_in[q, :, at_rows(me, 2 * HEAD_DIM)] = g_out[q, at_rows(me, rows), :]

    def gated_wait(q, near_by):
        took = g_in.at[q, :, 0:(2 if near_by else 4) * HEAD_DIM]
        pltpu.make_async_remote_copy(
            took, took, g_send, g_recv.at[near_by, q],
            device_id={"tp": mirror}, device_id_type=MESH,
        ).wait_recv()

    step = 512
    side_cols = 4 * HEAD_DIM

    def closing(lo, n):
        def norm(i, _):
            at = pl.multiple_of(i * 16, 16)
            x = premix[pl.ds(at, 16), :]
            scale = lax.rsqrt(jnp.mean(x * x, axis=-1, keepdims=True) + rms_eps)
            q = lo + lax.div(i, rows // 16)
            to = pl.multiple_of(lax.rem(i, rows // 16) * 16, 16)
            out[q, pl.ds(to, 16), :] = (x * scale * pgain[...]).astype(BF16)
            return 0

        lax.fori_loop(0, n // 16, norm, 0, unroll=2)

    def emit(lo, hi):
        n = (hi - lo) * rows
        with jax.named_scope("gated_wait"):
            for q in range(lo, hi):
                gated_wait(q, 0)
                gated_wait(q, 1)
        g = g_in[lo:hi].reshape(n, g_in.shape[2])
        for c in range(width // step):
            cut = slice(c * step, (c + 1) * step)
            premix[0:n, cut] = jnp.dot(g, wo[:, cut], preferred_element_type=F32)
        closing(lo, n)

    def emit_half(lo, hi, which, near_by):
        for q in range(lo, hi):
            gated_wait(q, near_by)
        n = (hi - lo) * rows
        span = at_rows(which, side_cols)
        g = g_in[lo:hi, :, span].reshape(n, side_cols)
        for c in range(width // step):
            cut = slice(c * step, (c + 1) * step)
            term = jnp.dot(g, wo[span, cut], preferred_element_type=F32)
            premix[0:n, cut] = term if near_by else premix[0:n, cut] + term

    def scoped(name, function, *args):
        with jax.named_scope(name):
            function(*args)

    def over(lo, hi, function):
        def run(q, _):
            function(q)
            return 0

        lax.fori_loop(lo, hi, run, 0)

    def near(q):
        arrived(q, twin)
        project_kv(0, q, own_rows)
        project_qg(0, q, own_rows)

    def near_raw():
        arrived(None, twin)
        norm_raw(twin)
        project_kv(0, 0, own_rows)
        project_qg(0, 0, own_rows)

    def take(q):
        with jax.named_scope("take"):
            arrived(q, across)
        block_copy(q, across, twin, p_send).start()

    def rest(q):
        with jax.named_scope("take2"):
            arrived(q, across_twin)
        project_kv(0, q, far_rows)
        project_qg(0, q, far_rows)

    def rest_raw():
        norm_raw(across)
        with jax.named_scope("take2"):
            arrived(None, across_twin)
        norm_raw(across_twin)
        project_kv(0, 0, far_rows)
        project_qg(0, 0, far_rows)

    end = seqs - 1
    scoped("near0", near_raw)
    scoped("pass0", pass_on, 0)
    scoped("near123", over, 1, seqs, near)
    scoped("pass1", pass_on, 1)
    with jax.named_scope("tables1"):
        head_copy().wait_recv()
        tables(1)
    loads[3].wait()
    pltpu.make_async_copy(wo_h, wo, o_sem).wait()
    scoped("pass2", pass_on, 2)
    take(None)
    scoped("pass3", pass_on, 3)
    scoped("rest0", rest_raw)
    take(1)
    scoped("rest1", rest, 1)
    with jax.named_scope("havekv"):
        have(0)

    def early(q):
        project_kv(1, q, everything)
        make_state(q)

    def lone(q):
        project_kv(1, q, own_rows)

    def later(q):
        project_qg(1, q, everything)

    scoped("early", over, 0, 2, early)
    take(2)
    scoped("lone", over, 2, seqs, lone)
    scoped("rest2", rest, 2)
    project_kv(1, 2, far_rows)
    scoped("state2", make_state, 2)
    with jax.named_scope("haveqg"):
        have(1)
    take_last()
    scoped("later0", over, 0, 1, later)
    with jax.named_scope("present"):
        @pl.when(z < nz - 1)
        def _():
            pl.semaphore_wait(present, nz - 1 - z)

    scoped("plane0", plane_total, 0)
    project_qg(1, end, own_rows)
    scoped("plane1", plane_total, 1)
    with jax.named_scope("take2e"):
        arrived(end, across_twin)
    with jax.named_scope("rest3"):
        for h in range(2):
            project_kv(h, end, far_rows)
        make_state(end)
    scoped("plane2", plane_total, 2)
    with jax.named_scope("qg3"):
        for h in range(2):
            project_qg(h, end, far_rows)
    scoped("later12", over, 1, seqs - 1, later)
    scoped("back0", hand_back, 0)
    scoped("back1", hand_back, 1)
    scoped("inside01", over, 0, 2, inside)
    scoped("plane3", plane_total, end)
    scoped("back2", hand_back, 2)
    scoped("inside23", over, 2, seqs, inside)
    scoped("back3", hand_back, end)
    scoped("finish01", over, 0, 2, finish)
    scoped("finish23", over, 2, seqs, finish)
    scoped("emit0", emit, 0, end)
    scoped("emit3a", emit_half, end, seqs, side, 1)
    scoped("emit3b", emit_half, end, seqs, 1 - side, 0)

    def sent(took, sem):
        pltpu.make_async_remote_copy(
            took, took, sem, h_recv, device_id={"tp": mirror}, device_id_type=MESH,
        ).wait_send()

    with jax.named_scope("drain"):
        sent(gath.at[:, 0:rows, :], x_send)
        sent(gath.at[:, 0:2 * rows, :], p_send)
        sent(w.at[0, :, :], w_send)
        sent(heads.at[0], w_send)
        sent(s1_in.at[:, 0:2 * NY - 1], s_send.at[0])
        for n in range(nz - 1):
            @pl.when(z == n)
            def _():
                sent(s2_in.at[:, 0:nz - 1 - n], s_send.at[1])
        sent(s3_out.at[:, 0:2 * NY - 1], s_send.at[2])
        sent(g_in.at[:, :, 0:6 * HEAD_DIM], g_send)


def hand_over(source, premix, pgain, out, held, sem):
    seqs, rows, _ = source.shape
    done = pltpu.make_async_copy(source.at[0:seqs - 1], out.at[0:seqs - 1], sem.at[0])
    done.start()

    def norm(i, _):
        at = pl.multiple_of(i * 16, 16)
        x = premix[pl.ds(at, 16), :]
        scale = lax.rsqrt(jnp.mean(x * x, axis=-1, keepdims=True) + rms_eps)
        held[pl.ds(at, 16), :] = (x * scale * pgain[...]).astype(BF16)
        return 0

    lax.fori_loop(0, rows // 16, norm, 0, unroll=2)
    last = pltpu.make_async_copy(held, out.at[seqs - 1], sem.at[1])
    last.start()
    done.wait()
    last.wait()


def solution(mesh):
    tp, sp = mesh.shape["tp"], mesh.shape["sp"]

    def body(tok, gain, wq, wk, wv, wg, decay, ngain, wo, pgain):
        seqs, rows, width = tok.shape
        length = rows * 4
        nz = sp // NY
        part = HEAD_DIM // NY
        half = HEAD_DIM // 2
        inv = np.float32(rope_base) ** (-np.arange(half, dtype=np.float32) / half)
        inv = jnp.asarray(np.concatenate([inv, inv])[None, :], F32)
        dma = pltpu.SemaphoreType.DMA
        hbm = pl.BlockSpec(memory_space=pltpu.HBM)
        vmem = pltpu.VMEM
        wide = vmem((2, seqs, length, HEAD_DIM), BF16)
        mixed, premix, post = pl.pallas_call(
            functools.partial(kernel, tp, sp),
            out_shape=(
                jax.ShapeDtypeStruct(tok.shape, BF16),
                jax.ShapeDtypeStruct((seqs * rows, width), F32),
                jax.ShapeDtypeStruct((1, width), F32),
            ),
            in_specs=[
                hbm, hbm, hbm, hbm, hbm, hbm,
                pl.BlockSpec(memory_space=pltpu.SMEM), hbm, hbm, hbm, hbm,
            ],
            out_specs=(pl.BlockSpec(memory_space=pltpu.VMEM),) * 3,
            scratch_shapes=[
                vmem((1, width), F32), vmem((1, HEAD_DIM), F32),
                vmem((2, 8, HEAD_DIM), F32),
                vmem((seqs - 1, rows, width), BF16),
                vmem((length, width), BF16),
                vmem((seqs, length, width), BF16),
                vmem((2, width, 4 * HEAD_DIM), BF16),
                vmem(wo.shape, BF16),
                vmem((length, HEAD_DIM), F32), vmem((length, HEAD_DIM), F32),
                vmem((2, length, length), F32),
                vmem((2, length, HEAD_DIM), F32), vmem((2, length, HEAD_DIM), F32),
                wide, wide, wide, wide,
                vmem((2, seqs, length, HEAD_DIM), F32),
                vmem((2, seqs, length, HEAD_DIM), F32),
                vmem((2, seqs, HEAD_DIM, HEAD_DIM), BF16),
                vmem((seqs, 2 * NY, part, HEAD_DIM), BF16),
                vmem((seqs, part, HEAD_DIM), BF16),
                vmem((seqs, nz - 1, part, HEAD_DIM), BF16),
                vmem((seqs, 2 * NY, part, HEAD_DIM), BF16),
                vmem((2, seqs, HEAD_DIM, HEAD_DIM), BF16),
                vmem((seqs, length, 2 * HEAD_DIM), BF16),
                vmem((seqs, rows, HEAD_DIM * tp), BF16),
                dma(()), dma(()), dma((seqs, 4)), dma((2,)), dma(()), dma((6,)), dma(()),
                dma((3,)), dma((seqs,)), dma((seqs,)), dma((seqs,)), dma(()), dma((2, seqs)),
                dma((8,)), dma(()), dma((seqs,)), pltpu.SemaphoreType.REGULAR,
            ],
            compiler_params=pltpu.CompilerParams(
                collective_id=0, has_side_effects=True, vmem_limit_bytes=40 * 2**20
            ),
            name="retention",
        )(
            *(pltpu.with_memory_space_constraint(x, pltpu.HBM) for x in (tok, gain[None, :], wq, wk, wv, wg)), decay,
            *(pltpu.with_memory_space_constraint(x, pltpu.HBM) for x in (ngain[None, :], wo, pgain[None, :], inv))
        )
        return pl.pallas_call(
            hand_over,
            out_shape=jax.ShapeDtypeStruct(tok.shape, BF16),
            in_specs=[pl.BlockSpec(memory_space=pltpu.VMEM)] * 3,
            out_specs=hbm,
            scratch_shapes=[vmem((rows, width), BF16), dma((2,))],
            compiler_params=pltpu.CompilerParams(vmem_limit_bytes=16 * 2**20),
            name="hand_over",
        )(mixed, premix, post)

    placed = (
        P(None, ("sp", "tp"), None),
        P(),
        P(None, "tp"),
        P(None, "tp"),
        P(None, "tp"),
        P(None, "tp"),
        P("tp"),
        P("tp"),
        P(),
        P(),
    )
    return jax.shard_map(
        body, mesh=mesh, in_specs=placed, out_specs=P(None, ("sp", "tp"), None), check_vma=False
    )
```

```python
import functools

import jax
import jax.numpy as jnp
import numpy as np
from jax import lax
from jax.experimental import pallas as pl
from jax.experimental.pallas import tpu as pltpu
from jax.sharding import PartitionSpec as P

HEAD_DIM = 128
SUB = 128
NY = 4
rms_eps = 1e-06
group_eps = 1e-05
rope_base = 10000.0
MESH = pl.DeviceIdType.MESH
F32 = jnp.float32
BF16 = jnp.bfloat16


def kernel(
    tp, sp,
    tok, gain_h, wq_h, wk_h, wv_h, wg_h, decay, ngain_h, wo_h, pgain_h, inv_h,
    out, premix, pgain,
    gain, inv, heads, tokv, raw, gath, w, wo, cosv, sinv, mask, fade, reach,
    qs, qr, ks, vs, sg, within, s1_out, s1_in, s2_out, s2_in, s3_out, excl,
    g_out, g_in,
    x_send, p_send, t_recv, last_recv, w_send, wx_recv, h_recv,
    s_send, s1_recv, s2_recv, s3_recv, g_send, g_recv,
    w_sem, o_sem, in_sem, present,
):
    seqs, rows, width = tok.shape
    pair = 2 * rows
    length = 2 * pair
    line = rows * tp
    nz = sp // NY
    part = HEAD_DIM // NY
    direct = width // 4
    piece = (width - direct) // NY
    s, t = lax.axis_index("sp"), lax.axis_index("tp")
    z, y = lax.div(s, NY), lax.rem(s, NY)
    chip, core = lax.div(t, 2), lax.rem(t, 2)
    group, side = lax.div(chip, 2), lax.rem(chip, 2)
    base = group * 4
    me = side * 2 + core
    twin = side * 2 + 1 - core
    across = (1 - side) * 2 + core
    across_twin = (1 - side) * 2 + 1 - core
    mirror = (3 - chip) * 2 + core
    slot = y * 2 + group

    def at_rows(who, n):
        return pl.ds(pl.multiple_of(who * n, n), n)

    loads_in = [
        pltpu.make_async_copy(
            tok.at[q], tokv.at[q - 1] if q else raw.at[at_rows(me, rows), :], in_sem.at[q]
        )
        for q in range(seqs)
    ]

    cuts = [slice(i * HEAD_DIM, (i + 1) * HEAD_DIM) for i in range(4)]
    loads_w = [
        pltpu.make_async_copy(a, w.at[0, :, cuts[i]], w_sem.at[0])
        for i, a in enumerate((wk_h, wv_h, wq_h, wg_h))
    ]
    loads = [
        pltpu.make_async_copy(a, b, w_sem.at[1 + i])
        for i, (a, b) in enumerate(
            ((ngain_h, heads.at[0, 1:2, :]), (gain_h, gain), (inv_h, inv), (pgain_h, pgain))
        )
    ]

    def head_of(u, flip):
        c = group * 2 + u // 2
        return ((3 - c) if flip else c) * 2 + u % 2

    loads_o = [
        pltpu.make_async_copy(
            wo_h.at[pl.ds(pl.multiple_of(head_of(i // 2, i % 2) * HEAD_DIM, HEAD_DIM), HEAD_DIM), :],
            wo.at[i * HEAD_DIM:(i + 1) * HEAD_DIM, :], o_sem,
        )
        for i in range(8)
    ]
    for load in loads_in + loads:
        load.start()

    barrier = pltpu.get_barrier_semaphore()

    def greet(dest):
        pl.semaphore_signal(barrier, inc=1, device_id=dest, device_id_type=MESH)

    for u in (twin, across, across_twin):
        greet({"tp": base + u})
    for j in range(1, NY):
        greet({"sp": z * NY + lax.rem(y + j, NY)})
    for j in range(NY):
        greet({"sp": z * NY + lax.rem(y + j, NY), "tp": mirror})
    for d in range(1, nz):
        @pl.when(z + d < nz)
        def _():
            greet({"sp": lax.rem(z + d, nz) * NY + y})

    def cross(i):
        span = pl.ds(pl.multiple_of(direct + y * piece, 128), piece)
        return pltpu.make_async_remote_copy(
            w.at[0, span, cuts[i]], w.at[1, span, cuts[i]], w_send, wx_recv.at[i],
            device_id={"tp": mirror}, device_id_type=MESH,
        )

    def straight(i):
        return pltpu.make_async_remote_copy(
            w.at[0, 0:direct, cuts[i]], w.at[1, 0:direct, cuts[i]],
            w_send, wx_recv.at[4 + i // 2],
            device_id={"tp": mirror}, device_id_type=MESH,
        )

    def along(i, j):
        peer = lax.rem(y + j, NY)
        span = pl.ds(pl.multiple_of(direct + y * piece, 128), piece)
        return pltpu.make_async_remote_copy(
            w.at[1, span, cuts[i]], w.at[1, span, cuts[i]], w_send, wx_recv.at[4 + i // 2],
            device_id={"sp": z * NY + peer}, device_id_type=MESH,
        )

    def pass_on(i):
        cross(i).wait_recv()
        for j in range(1, NY):
            along(i, j).start()

    def have(k):
        took = w.at[1, 0:width - piece, 256 * k:256 * (k + 1)]
        pltpu.make_async_remote_copy(
            took, took, w_send, wx_recv.at[4 + k], device_id={"tp": mirror}, device_id_type=MESH,
        ).wait_recv()

    def head_copy():
        return pltpu.make_async_remote_copy(
            heads.at[0], heads.at[1], w_send, h_recv, device_id={"tp": mirror}, device_id_type=MESH,
        )

    def block_copy(q, u, dest, sem, kind):
        held = raw.at[at_rows(u, rows), :] if q is None else gath.at[q, at_rows(u, rows), :]
        return pltpu.make_async_remote_copy(
            held, held, sem, t_recv.at[(0 if q is None else q) * 3 + kind],
            device_id={"tp": base + dest}, device_id_type=MESH,
        )

    def arrived(q, u, kind):
        block_copy(q, u, twin, x_send, kind).wait_recv()

    def normalise(source, q, u):
        def norm(i, _):
            x = source(pl.multiple_of(i * 16, 16)).astype(F32)
            scale = lax.rsqrt(jnp.mean(x * x, axis=-1, keepdims=True) + rms_eps)
            to = pl.ds(pl.multiple_of(u * rows + i * 16, 16), 16)
            gath[q, to, :] = (x * scale * gain[...]).astype(BF16)
            return 0

        lax.fori_loop(0, rows // 16, norm, 0, unroll=2)

    def norm_own(q):
        loads_in[q].wait()
        normalise(lambda at: tokv[q - 1, pl.ds(at, 16), :], q, me)

    def norm_raw(u):
        normalise(lambda at: raw[pl.ds(pl.multiple_of(u * rows + at, 16), 16), :], 0, u)

    def send(q):
        block_copy(q, me, across, x_send, 1).start()
        block_copy(q, me, twin, p_send, 0).start()

    def last_copy(u, late, dest, sem, arrival):
        span = pl.ds(pl.multiple_of(u * rows + late * (rows - 16), 16), 16 if late else rows - 16)
        held = gath.at[seqs - 1, span, :]
        return pltpu.make_async_remote_copy(
            held, held, sem, arrival, device_id={"tp": base + dest}, device_id_type=MESH,
        )

    def take_last():
        for late in range(2):
            with jax.named_scope("takelast"):
                last_copy(across, late, twin, p_send, last_recv.at[late]).wait_recv()
            last_copy(across, late, twin, p_send, t_recv.at[3 * seqs - 1]).start()

    with jax.named_scope("load0"):
        loads_in[0].wait()
    for load in loads_w:
        load.start()
    with jax.named_scope("barrier"):
        pl.semaphore_wait(barrier, 3 + NY - 1 + NY + z)
    block_copy(None, me, across, x_send, 1).start()
    block_copy(None, me, twin, p_send, 0).start()
    for d in range(1, nz):
        @pl.when(z >= d)
        def _():
            pl.semaphore_signal(
                present, inc=1, device_id={"sp": lax.rem(z + nz - d, nz) * NY + y},
                device_id_type=MESH,
            )
    with jax.named_scope("norm"):
        loads[0].wait()
        heads[0, 0:1, :] = jnp.full((1, HEAD_DIM), decay[0], F32)
        loads[1].wait()
        norm_own(1)
        head_copy().start()
        norm_own(2)
        send(1)
        pltpu.make_async_remote_copy(
            w.at[0], w.at[0], w_sem.at[0], h_recv, device_id={"tp": mirror}, device_id_type=MESH,
        ).wait_send()
        for i in range(4):
            cross(i).start()
        for i in range(4):
            straight(i).start()
        for load in loads_o:
            load.start()
        norm_own(3)
        norm_raw(me)
        send(2)
        for late in range(2):
            last_copy(me, late, across, x_send, last_recv.at[late]).start()
        block_copy(seqs - 1, me, twin, p_send, 0).start()

    with jax.named_scope("tables"):
        loads[2].wait()
        place = s * line + group * length + lax.broadcasted_iota(jnp.int32, (length, HEAD_DIM), 0)
        angle = place.astype(F32) * inv[...]
        cosv[...] = jnp.cos(angle)
        lane = lax.broadcasted_iota(jnp.int32, (length, HEAD_DIM), 1)
        sine = jnp.sin(angle)
        sinv[...] = jnp.where(lane < HEAD_DIM // 2, -sine, sine)

    def tables(h):
        rate = heads[h, 0:1, :]
        spot = lax.broadcasted_iota(jnp.int32, (length, HEAD_DIM), 0)
        fade[h] = jnp.exp(rate * (length - 1 - spot).astype(F32))
        reach[h] = jnp.exp(rate * (1 + spot).astype(F32))
        for c in range(length // HEAD_DIM):
            gap = spot - c * HEAD_DIM - lax.broadcasted_iota(jnp.int32, (length, HEAD_DIM), 1)
            weight = jnp.exp(rate * jnp.maximum(gap, 0).astype(F32))
            mask[h, :, c * HEAD_DIM:(c + 1) * HEAD_DIM] = jnp.where(gap >= 0, weight, 0.0)

    with jax.named_scope("tables0"):
        tables(0)

    def rotate(x, span):
        x = x.astype(BF16).astype(F32)
        return x * cosv[span, :] + pltpu.roll(x, HEAD_DIM // 2, 1) * sinv[span, :]

    def project_kv(h, q, span):
        r = jnp.dot(gath[q, span, :], w[h, :, 0:256], preferred_element_type=F32)
        ks[h, q, span, :] = (rotate(r[:, cuts[0]], span) * HEAD_DIM ** (-0.5)).astype(BF16)
        vs[h, q, span, :] = r[:, cuts[1]].astype(BF16)

    def project_qg(h, q, span):
        r = jnp.dot(gath[q, span, :], w[h, :, 256:512], preferred_element_type=F32)
        query = rotate(r[:, cuts[0]], span).astype(BF16)
        qs[h, q, span, :] = query
        qr[h, q, span, :] = (query.astype(F32) * reach[h, span, :]).astype(BF16)
        gate = r[:, cuts[1]].astype(BF16).astype(F32)
        sg[h, q, span, :] = heads[h, 1:2, :] * (gate * jax.nn.sigmoid(gate))

    everything = slice(0, length)
    own_rows = at_rows(side, pair)
    far_rows = at_rows(1 - side, pair)

    def power(n):
        return jnp.exp(jnp.full((1, 1), decay[0] * n, F32))

    def s1_copy(q, h, j):
        peer = lax.rem(y + j, NY)
        dest = {"sp": z * NY + peer, "tp": mirror} if h else {"sp": z * NY + peer}
        return pltpu.make_async_remote_copy(
            s1_out.at[h, q, at_rows(peer, part), :], s1_in.at[q, slot],
            s_send.at[0], s1_recv.at[q], device_id=dest, device_id_type=MESH,
        )

    def make_state(q):
        for h in range(2):
            scaled = (ks[h, q].astype(F32) * fade[h]).astype(BF16)
            total = lax.dot_general(
                scaled, vs[h, q], (((0,), (0,)), ((), ())), preferred_element_type=F32
            )
            s1_out[h, q] = total.astype(BF16)
        for j in range(NY):
            s1_copy(q, 1, j).start()
            if j:
                s1_copy(q, 0, j).start()
        s1_in[q, slot] = s1_out[0, q, at_rows(y, part), :]

    def s2_copy(q, d):
        return pltpu.make_async_remote_copy(
            s2_out.at[q], s2_in.at[q, d - 1], s_send.at[1], s2_recv.at[q],
            device_id={"sp": lax.rem(z + d, nz) * NY + y}, device_id_type=MESH,
        )

    def plane_total(q):
        took = s1_in.at[q, 0:2 * NY - 1]
        pltpu.make_async_remote_copy(
            took, took, s_send.at[0], s1_recv.at[q], device_id={"tp": mirror}, device_id_type=MESH,
        ).wait_recv()
        step = power(length)
        total = s1_in[q, 0].astype(F32)
        for k in range(1, 2 * NY):
            total = total * step + s1_in[q, k].astype(F32)
        s2_out[q] = total.astype(BF16)
        for d in range(1, nz):
            @pl.when(z + d < nz)
            def _():
                s2_copy(q, d).start()

    def s3_copy(q, h, j):
        peer = lax.rem(y + j, NY)
        dest = {"sp": z * NY + peer, "tp": mirror} if h else {"sp": z * NY + peer}
        return pltpu.make_async_remote_copy(
            s3_out.at[q, peer * 2 + (1 - group if h else group)],
            excl.at[h, q, at_rows(y, part), :],
            s_send.at[2], s3_recv.at[q], device_id=dest, device_id_type=MESH,
        )

    def hand_back(q):
        for n in range(1, nz):
            @pl.when(z == n)
            def _():
                took = s2_in.at[q, 0:n]
                pltpu.make_async_remote_copy(
                    took, took, s_send.at[1], s2_recv.at[q],
                    device_id={"tp": mirror}, device_id_type=MESH,
                ).wait_recv()

        def add(d, total):
            return total + power(line * NY * d) * s2_in[q, d].astype(F32)

        before = lax.fori_loop(0, z, add, jnp.zeros((part, HEAD_DIM), F32))
        step = power(length)
        for k in range(2 * NY):
            s3_out[q, k] = before.astype(BF16)
            before = before * step + s1_in[q, k].astype(F32)
        for j in range(NY):
            s3_copy(q, 1, j).start()
            if j:
                s3_copy(q, 0, j).start()
        excl[0, q, at_rows(y, part), :] = s3_out[q, slot]

    def inside(q):
        for h in range(2):
            for i in range(length // SUB):
                here, upto = slice(i * SUB, (i + 1) * SUB), slice(0, (i + 1) * SUB)
                score = lax.dot_general(
                    qs[h, q, here, :], ks[h, q, upto, :],
                    (((1,), (1,)), ((), ())), preferred_element_type=F32,
                )
                weight = (score * mask[h, here, upto]).astype(BF16)
                within[h, q, here, :] = jnp.dot(
                    weight, vs[h, q, upto, :], preferred_element_type=F32
                )

    def gated_copy(q, dest, source, near_by=0):
        return pltpu.make_async_remote_copy(
            g_out.at[q, at_rows(dest, rows), :], g_in.at[q, :, at_rows(source, 2 * HEAD_DIM)],
            g_send, g_recv.at[q + near_by * lax.div(q, seqs - 1)],
            device_id={"tp": base + dest}, device_id_type=MESH,
        )

    def finish(q):
        took = s1_in.at[q, 0:2 * NY - 1]
        pltpu.make_async_remote_copy(
            took, took, s_send.at[2], s3_recv.at[q], device_id={"tp": mirror}, device_id_type=MESH,
        ).wait_recv()
        for k in range(2):
            here = at_rows((1 - side) if k == 0 else side, pair)
            for h in range(2):
                kept = within[h, q, here, :] + jnp.dot(
                    qr[h, q, here, :], excl[h, q], preferred_element_type=F32
                )
                kept = kept - jnp.mean(kept, axis=-1, keepdims=True)
                spread = jnp.mean(kept * kept, axis=-1, keepdims=True)
                normal = kept * lax.rsqrt(spread + group_eps) * sg[h, q, here, :]
                g_out[q, here, cuts[h]] = normal.astype(BF16)
            if k == 0:
                gated_copy(q, across, me).start()
                gated_copy(q, across_twin, me).start()
            else:
                gated_copy(q, twin, me, 1).start()
                g_in[q, :, at_rows(me, 2 * HEAD_DIM)] = g_out[q, at_rows(me, rows), :]

    def gated_wait(q, near_by):
        took = g_in.at[q, :, 0:(2 if near_by else 4 if q == seqs - 1 else 6) * HEAD_DIM]
        pltpu.make_async_remote_copy(
            took, took, g_send, g_recv.at[q + near_by],
            device_id={"tp": mirror}, device_id_type=MESH,
        ).wait_recv()

    step = 512
    side_cols = 4 * HEAD_DIM

    def closing(lo, n):
        def norm(i, _):
            at = pl.multiple_of(i * 16, 16)
            x = premix[pl.ds(at, 16), :]
            scale = lax.rsqrt(jnp.mean(x * x, axis=-1, keepdims=True) + rms_eps)
            q = lo + lax.div(i, rows // 16)
            to = pl.multiple_of(lax.rem(i, rows // 16) * 16, 16)
            out[q, pl.ds(to, 16), :] = (x * scale * pgain[...]).astype(BF16)
            return 0

        lax.fori_loop(0, n // 16, norm, 0, unroll=2)

    def emit(lo, hi):
        n = (hi - lo) * rows
        with jax.named_scope("gated_wait"):
            for q in range(lo, hi):
                gated_wait(q, 0)
        g = g_in[lo:hi].reshape(n, g_in.shape[2])
        for c in range(width // step):
            cut = slice(c * step, (c + 1) * step)
            premix[0:n, cut] = jnp.dot(g, wo[:, cut], preferred_element_type=F32)
        closing(lo, n)

    def emit_half(lo, hi, which, near_by):
        for q in range(lo, hi):
            gated_wait(q, near_by)
        n = (hi - lo) * rows
        span = at_rows(which, side_cols)
        g = g_in[lo:hi, :, span].reshape(n, side_cols)
        for c in range(width // step):
            cut = slice(c * step, (c + 1) * step)
            term = jnp.dot(g, wo[span, cut], preferred_element_type=F32)
            premix[0:n, cut] = term if near_by else premix[0:n, cut] + term

    def scoped(name, function, *args):
        with jax.named_scope(name):
            function(*args)

    def over(lo, hi, function):
        def run(q, _):
            function(q)
            return 0

        lax.fori_loop(lo, hi, run, 0)

    def near(q):
        arrived(q, twin, 0)
        project_kv(0, q, own_rows)
        project_qg(0, q, own_rows)

    def near_raw():
        arrived(None, twin, 0)
        norm_raw(twin)
        project_kv(0, 0, own_rows)
        project_qg(0, 0, own_rows)

    def take(q):
        with jax.named_scope("take"):
            arrived(q, across, 1)
        block_copy(q, across, twin, p_send, 2).start()

    def rest(q):
        with jax.named_scope("take2"):
            arrived(q, across_twin, 2)
        project_kv(0, q, far_rows)
        project_qg(0, q, far_rows)

    def rest_raw():
        norm_raw(across)
        with jax.named_scope("take2"):
            arrived(None, across_twin, 2)
        norm_raw(across_twin)
        project_kv(0, 0, far_rows)
        project_qg(0, 0, far_rows)

    end = seqs - 1
    scoped("near0", near_raw)
    scoped("pass0", pass_on, 0)
    scoped("near123", over, 1, seqs, near)
    scoped("pass1", pass_on, 1)
    with jax.named_scope("tables1"):
        head_copy().wait_recv()
        tables(1)
    loads[3].wait()
    pltpu.make_async_copy(wo_h, wo, o_sem).wait()
    scoped("pass2", pass_on, 2)
    take(None)
    scoped("pass3", pass_on, 3)
    scoped("rest0", rest_raw)
    take(1)
    scoped("rest1", rest, 1)
    with jax.named_scope("havekv"):
        have(0)

    def early(q):
        project_kv(1, q, everything)
        make_state(q)

    def lone(q):
        project_kv(1, q, own_rows)

    def later(q):
        project_qg(1, q, everything)

    scoped("early", over, 0, 2, early)
    take(2)
    scoped("lone", over, 2, seqs, lone)
    scoped("rest2", rest, 2)
    project_kv(1, 2, far_rows)
    scoped("state2", make_state, 2)
    with jax.named_scope("haveqg"):
        have(1)
    take_last()
    scoped("later0", over, 0, 1, later)
    with jax.named_scope("present"):
        @pl.when(z < nz - 1)
        def _():
            pl.semaphore_wait(present, nz - 1 - z)

    scoped("plane0", plane_total, 0)
    project_qg(1, end, own_rows)
    scoped("plane1", plane_total, 1)
    with jax.named_scope("take2e"):
        arrived(end, across_twin, 2)
    with jax.named_scope("rest3"):
        for h in range(2):
            project_kv(h, end, far_rows)
        make_state(end)
    scoped("plane2", plane_total, 2)
    with jax.named_scope("qg3"):
        for h in range(2):
            project_qg(h, end, far_rows)
    scoped("later12", over, 1, seqs - 1, later)
    scoped("back0", hand_back, 0)
    scoped("back1", hand_back, 1)
    scoped("inside01", over, 0, 2, inside)
    scoped("plane3", plane_total, end)
    scoped("back2", hand_back, 2)
    scoped("inside23", over, 2, seqs, inside)
    scoped("back3", hand_back, end)
    scoped("finish01", over, 0, 2, finish)
    scoped("finish23", over, 2, seqs, finish)
    scoped("emit0", emit, 0, end)
    scoped("emit3a", emit_half, end, seqs, side, 1)
    scoped("emit3b", emit_half, end, seqs, 1 - side, 0)

    def sent(took, sem):
        pltpu.make_async_remote_copy(
            took, took, sem, h_recv, device_id={"tp": mirror}, device_id_type=MESH,
        ).wait_send()

    with jax.named_scope("drain"):
        sent(gath.at[:, 0:rows, :], x_send)
        sent(gath.at[:, 0:2 * rows, :], p_send)
        sent(w.at[0, :, :], w_send)
        sent(heads.at[0], w_send)
        sent(s1_in.at[:, 0:2 * NY - 1], s_send.at[0])
        for n in range(nz - 1):
            @pl.when(z == n)
            def _():
                sent(s2_in.at[:, 0:nz - 1 - n], s_send.at[1])
        sent(s3_out.at[:, 0:2 * NY - 1], s_send.at[2])
        sent(g_in.at[:, :, 0:6 * HEAD_DIM], g_send)


def hand_over(source, premix, pgain, out, held, sem):
    seqs, rows, _ = source.shape
    done = pltpu.make_async_copy(source.at[0:seqs - 1], out.at[0:seqs - 1], sem.at[0])
    done.start()

    def norm(i, _):
        at = pl.multiple_of(i * 16, 16)
        x = premix[pl.ds(at, 16), :]
        scale = lax.rsqrt(jnp.mean(x * x, axis=-1, keepdims=True) + rms_eps)
        held[pl.ds(at, 16), :] = (x * scale * pgain[...]).astype(BF16)
        return 0

    lax.fori_loop(0, rows // 16, norm, 0, unroll=2)
    last = pltpu.make_async_copy(held, out.at[seqs - 1], sem.at[1])
    last.start()
    done.wait()
    last.wait()


def solution(mesh):
    tp, sp = mesh.shape["tp"], mesh.shape["sp"]

    def body(tok, gain, wq, wk, wv, wg, decay, ngain, wo, pgain):
        seqs, rows, width = tok.shape
        length = rows * 4
        nz = sp // NY
        part = HEAD_DIM // NY
        half = HEAD_DIM // 2
        inv = np.float32(rope_base) ** (-np.arange(half, dtype=np.float32) / half)
        inv = jnp.asarray(np.concatenate([inv, inv])[None, :], F32)
        dma = pltpu.SemaphoreType.DMA
        hbm = pl.BlockSpec(memory_space=pltpu.HBM)
        vmem = pltpu.VMEM
        wide = vmem((2, seqs, length, HEAD_DIM), BF16)
        mixed, premix, post = pl.pallas_call(
            functools.partial(kernel, tp, sp),
            out_shape=(
                jax.ShapeDtypeStruct(tok.shape, BF16),
                jax.ShapeDtypeStruct((seqs * rows, width), F32),
                jax.ShapeDtypeStruct((1, width), F32),
            ),
            in_specs=[
                hbm, hbm, hbm, hbm, hbm, hbm,
                pl.BlockSpec(memory_space=pltpu.SMEM), hbm, hbm, hbm, hbm,
            ],
            out_specs=(pl.BlockSpec(memory_space=pltpu.VMEM),) * 3,
            scratch_shapes=[
                vmem((1, width), F32), vmem((1, HEAD_DIM), F32),
                vmem((2, 8, HEAD_DIM), F32),
                vmem((seqs - 1, rows, width), BF16),
                vmem((length, width), BF16),
                vmem((seqs, length, width), BF16),
                vmem((2, width, 4 * HEAD_DIM), BF16),
                vmem(wo.shape, BF16),
                vmem((length, HEAD_DIM), F32), vmem((length, HEAD_DIM), F32),
                vmem((2, length, length), F32),
                vmem((2, length, HEAD_DIM), F32), vmem((2, length, HEAD_DIM), F32),
                wide, wide, wide, wide,
                vmem((2, seqs, length, HEAD_DIM), F32),
                vmem((2, seqs, length, HEAD_DIM), F32),
                vmem((2, seqs, HEAD_DIM, HEAD_DIM), BF16),
                vmem((seqs, 2 * NY, part, HEAD_DIM), BF16),
                vmem((seqs, part, HEAD_DIM), BF16),
                vmem((seqs, nz - 1, part, HEAD_DIM), BF16),
                vmem((seqs, 2 * NY, part, HEAD_DIM), BF16),
                vmem((2, seqs, HEAD_DIM, HEAD_DIM), BF16),
                vmem((seqs, length, 2 * HEAD_DIM), BF16),
                vmem((seqs, rows, HEAD_DIM * tp), BF16),
                dma(()), dma(()), dma((3 * seqs,)), dma((2,)), dma(()), dma((6,)), dma(()),
                dma((3,)), dma((seqs,)), dma((seqs,)), dma((seqs,)), dma(()), dma((seqs + 1,)),
                dma((5,)), dma(()), dma((seqs,)), pltpu.SemaphoreType.REGULAR,
            ],
            compiler_params=pltpu.CompilerParams(
                collective_id=0, has_side_effects=True, vmem_limit_bytes=40 * 2**20
            ),
            name="retention",
        )(
            *(pltpu.with_memory_space_constraint(x, pltpu.HBM) for x in (tok, gain[None, :], wq, wk, wv, wg)), decay,
            *(pltpu.with_memory_space_constraint(x, pltpu.HBM) for x in (ngain[None, :], wo, pgain[None, :], inv))
        )
        return pl.pallas_call(
            hand_over,
            out_shape=jax.ShapeDtypeStruct(tok.shape, BF16),
            in_specs=[pl.BlockSpec(memory_space=pltpu.VMEM)] * 3,
            out_specs=hbm,
            scratch_shapes=[vmem((rows, width), BF16), dma((2,))],
            compiler_params=pltpu.CompilerParams(vmem_limit_bytes=16 * 2**20),
            name="hand_over",
        )(mixed, premix, post)

    placed = (
        P(None, ("sp", "tp"), None),
        P(),
        P(None, "tp"),
        P(None, "tp"),
        P(None, "tp"),
        P(None, "tp"),
        P("tp"),
        P("tp"),
        P(),
        P(),
    )
    return jax.shard_map(
        body, mesh=mesh, in_specs=placed, out_specs=P(None, ("sp", "tp"), None), check_vma=False
    )
```

```python
import functools

import jax
import jax.numpy as jnp
import numpy as np
from jax import lax
from jax.experimental import pallas as pl
from jax.experimental.pallas import tpu as pltpu
from jax.sharding import PartitionSpec as P

HEAD_DIM = 128
SUB = 128
NY = 4
rms_eps = 1e-06
group_eps = 1e-05
rope_base = 10000.0
MESH = pl.DeviceIdType.MESH
F32 = jnp.float32
BF16 = jnp.bfloat16


def kernel(
    tp, sp,
    tok, gain_h, wq_h, wk_h, wv_h, wg_h, decay, ngain_h, wo_h, pgain_h, inv_h,
    out, premix, pgain,
    gain, inv, heads, tokv, raw, gath, w, wo, cosv, sinv, mask, fade, reach,
    qs, qr, ks, vs, sg, within, s1_out, s1_in, s2_out, s2_in, s3_out, excl,
    g_out, g_in,
    x_send, p_send, t_recv, last_recv, w_send, wx_recv, h_recv,
    s_send, s1_recv, s2_recv, s3_recv, g_send, g_recv,
    w_sem, o_sem, in_sem, present,
):
    seqs, rows, width = tok.shape
    pair = 2 * rows
    length = 2 * pair
    line = rows * tp
    nz = sp // NY
    part = HEAD_DIM // NY
    direct = width // 4
    piece = (width - direct) // NY
    s, t = lax.axis_index("sp"), lax.axis_index("tp")
    z, y = lax.div(s, NY), lax.rem(s, NY)
    chip, core = lax.div(t, 2), lax.rem(t, 2)
    group, side = lax.div(chip, 2), lax.rem(chip, 2)
    base = group * 4
    me = side * 2 + core
    twin = side * 2 + 1 - core
    across = (1 - side) * 2 + core
    across_twin = (1 - side) * 2 + 1 - core
    mirror = (3 - chip) * 2 + core
    slot = y * 2 + group

    def at_rows(who, n):
        return pl.ds(pl.multiple_of(who * n, n), n)

    loads_in = [
        pltpu.make_async_copy(
            tok.at[q], tokv.at[q - 1] if q else raw.at[at_rows(me, rows), :], in_sem.at[q]
        )
        for q in range(seqs)
    ]

    cuts = [slice(i * HEAD_DIM, (i + 1) * HEAD_DIM) for i in range(4)]
    loads_w = [
        pltpu.make_async_copy(a, w.at[0, :, cuts[i]], w_sem.at[0])
        for i, a in enumerate((wk_h, wv_h, wq_h, wg_h))
    ]
    loads = [
        pltpu.make_async_copy(a, b, w_sem.at[1 + i])
        for i, (a, b) in enumerate(
            ((ngain_h, heads.at[0, 1:2, :]), (gain_h, gain), (inv_h, inv), (pgain_h, pgain))
        )
    ]

    def head_of(u, flip):
        c = group * 2 + u // 2
        return ((3 - c) if flip else c) * 2 + u % 2

    loads_o = [
        pltpu.make_async_copy(
            wo_h.at[pl.ds(pl.multiple_of(head_of(i // 2, i % 2) * HEAD_DIM, HEAD_DIM), HEAD_DIM), :],
            wo.at[i * HEAD_DIM:(i + 1) * HEAD_DIM, :], o_sem,
        )
        for i in range(8)
    ]
    for load in loads_in + loads:
        load.start()

    barrier = pltpu.get_barrier_semaphore()

    def greet(dest):
        pl.semaphore_signal(barrier, inc=1, device_id=dest, device_id_type=MESH)

    for u in (twin, across, across_twin):
        greet({"tp": base + u})
    for j in range(1, NY):
        greet({"sp": z * NY + lax.rem(y + j, NY)})
    for j in range(NY):
        greet({"sp": z * NY + lax.rem(y + j, NY), "tp": mirror})
    for d in range(1, nz):
        @pl.when(z + d < nz)
        def _():
            greet({"sp": lax.rem(z + d, nz) * NY + y})

    def cross(i):
        span = pl.ds(pl.multiple_of(direct + y * piece, 128), piece)
        return pltpu.make_async_remote_copy(
            w.at[0, span, cuts[i]], w.at[1, span, cuts[i]], w_send, wx_recv.at[i],
            device_id={"tp": mirror}, device_id_type=MESH,
        )

    def straight(i):
        return pltpu.make_async_remote_copy(
            w.at[0, 0:direct, cuts[i]], w.at[1, 0:direct, cuts[i]],
            w_send, wx_recv.at[4 + i // 2],
            device_id={"tp": mirror}, device_id_type=MESH,
        )

    def along(i, j):
        peer = lax.rem(y + j, NY)
        span = pl.ds(pl.multiple_of(direct + y * piece, 128), piece)
        return pltpu.make_async_remote_copy(
            w.at[1, span, cuts[i]], w.at[1, span, cuts[i]], w_send, wx_recv.at[4 + i // 2],
            device_id={"sp": z * NY + peer}, device_id_type=MESH,
        )

    def pass_on(i):
        cross(i).wait_recv()
        for j in range(1, NY):
            along(i, j).start()

    def have(k):
        took = w.at[1, 0:width - piece, 256 * k:256 * (k + 1)]
        pltpu.make_async_remote_copy(
            took, took, w_send, wx_recv.at[4 + k], device_id={"tp": mirror}, device_id_type=MESH,
        ).wait_recv()

    def head_copy():
        return pltpu.make_async_remote_copy(
            heads.at[0], heads.at[1], w_send, h_recv, device_id={"tp": mirror}, device_id_type=MESH,
        )

    def block_copy(q, u, dest, sem, kind):
        held = raw.at[at_rows(u, rows), :] if q is None else gath.at[q, at_rows(u, rows), :]
        return pltpu.make_async_remote_copy(
            held, held, sem, t_recv.at[(0 if q is None else q) * 3 + kind],
            device_id={"tp": base + dest}, device_id_type=MESH,
        )

    def arrived(q, u, kind):
        block_copy(q, u, twin, x_send, kind).wait_recv()

    def normalise(source, q, u):
        def norm(i, _):
            x = source(pl.multiple_of(i * 16, 16)).astype(F32)
            scale = lax.rsqrt(jnp.mean(x * x, axis=-1, keepdims=True) + rms_eps)
            to = pl.ds(pl.multiple_of(u * rows + i * 16, 16), 16)
            gath[q, to, :] = (x * scale * gain[...]).astype(BF16)
            return 0

        lax.fori_loop(0, rows // 16, norm, 0, unroll=2)

    def norm_own(q):
        loads_in[q].wait()
        normalise(lambda at: tokv[q - 1, pl.ds(at, 16), :], q, me)

    def norm_raw(u):
        normalise(lambda at: raw[pl.ds(pl.multiple_of(u * rows + at, 16), 16), :], 0, u)

    def send(q):
        block_copy(q, me, across, x_send, 1).start()
        block_copy(q, me, twin, p_send, 0).start()

    def last_copy(u, late, dest, sem, arrival):
        span = pl.ds(pl.multiple_of(u * rows + late * (rows - 16), 16), 16 if late else rows - 16)
        held = gath.at[seqs - 1, span, :]
        return pltpu.make_async_remote_copy(
            held, held, sem, arrival, device_id={"tp": base + dest}, device_id_type=MESH,
        )

    def take_last():
        for late in range(2):
            with jax.named_scope("takelast"):
                last_copy(across, late, twin, p_send, last_recv.at[late]).wait_recv()
            last_copy(across, late, twin, p_send, t_recv.at[3 * seqs - 1]).start()

    with jax.named_scope("load0"):
        loads_in[0].wait()
    for load in loads_w:
        load.start()
    with jax.named_scope("barrier"):
        pl.semaphore_wait(barrier, 3 + NY - 1 + NY + z)
    block_copy(None, me, across, x_send, 1).start()
    block_copy(None, me, twin, p_send, 0).start()
    for d in range(1, nz):
        @pl.when(z >= d)
        def _():
            pl.semaphore_signal(
                present, inc=1, device_id={"sp": lax.rem(z + nz - d, nz) * NY + y},
                device_id_type=MESH,
            )
    with jax.named_scope("norm"):
        loads[0].wait()
        heads[0, 0:1, :] = jnp.full((1, HEAD_DIM), decay[0], F32)
        loads[1].wait()
        norm_own(1)
        head_copy().start()
        norm_own(2)
        send(1)
        pltpu.make_async_remote_copy(
            w.at[0], w.at[0], w_sem.at[0], h_recv, device_id={"tp": mirror}, device_id_type=MESH,
        ).wait_send()
        for i in range(4):
            cross(i).start()
        for i in range(4):
            straight(i).start()
        for load in loads_o:
            load.start()
        norm_own(3)
        norm_raw(me)
        send(2)
        for late in range(2):
            last_copy(me, late, across, x_send, last_recv.at[late]).start()
        block_copy(seqs - 1, me, twin, p_send, 0).start()

    with jax.named_scope("tables"):
        loads[2].wait()
        place = s * line + group * length + lax.broadcasted_iota(jnp.int32, (length, HEAD_DIM), 0)
        angle = place.astype(F32) * inv[...]
        cosv[...] = jnp.cos(angle)
        lane = lax.broadcasted_iota(jnp.int32, (length, HEAD_DIM), 1)
        sine = jnp.sin(angle)
        sinv[...] = jnp.where(lane < HEAD_DIM // 2, -sine, sine)

    def tables(h):
        rate = heads[h, 0:1, :]
        spot = lax.broadcasted_iota(jnp.int32, (length, HEAD_DIM), 0)
        fade[h] = jnp.exp(rate * (length - 1 - spot).astype(F32))
        reach[h] = jnp.exp(rate * (1 + spot).astype(F32))
        for c in range(length // HEAD_DIM):
            gap = spot - c * HEAD_DIM - lax.broadcasted_iota(jnp.int32, (length, HEAD_DIM), 1)
            weight = jnp.exp(rate * jnp.maximum(gap, 0).astype(F32))
            mask[h, :, c * HEAD_DIM:(c + 1) * HEAD_DIM] = jnp.where(gap >= 0, weight, 0.0)

    with jax.named_scope("tables0"):
        tables(0)

    def rotate(x, span):
        x = x.astype(BF16).astype(F32)
        return x * cosv[span, :] + pltpu.roll(x, HEAD_DIM // 2, 1) * sinv[span, :]

    def project_kv(h, q, span):
        r = jnp.dot(gath[q, span, :], w[h, :, 0:256], preferred_element_type=F32)
        ks[h, q, span, :] = (rotate(r[:, cuts[0]], span) * HEAD_DIM ** (-0.5)).astype(BF16)
        vs[h, q, span, :] = r[:, cuts[1]].astype(BF16)

    def project_qg(h, q, span):
        r = jnp.dot(gath[q, span, :], w[h, :, 256:512], preferred_element_type=F32)
        query = rotate(r[:, cuts[0]], span).astype(BF16)
        qs[h, q, span, :] = query
        qr[h, q, span, :] = (query.astype(F32) * reach[h, span, :]).astype(BF16)
        gate = r[:, cuts[1]].astype(BF16).astype(F32)
        sg[h, q, span, :] = heads[h, 1:2, :] * (gate * jax.nn.sigmoid(gate))

    everything = slice(0, length)
    own_rows = at_rows(side, pair)
    far_rows = at_rows(1 - side, pair)

    def power(n):
        return jnp.exp(jnp.full((1, 1), decay[0] * n, F32))

    def s1_copy(q, h, j):
        peer = lax.rem(y + j, NY)
        dest = {"sp": z * NY + peer, "tp": mirror} if h else {"sp": z * NY + peer}
        return pltpu.make_async_remote_copy(
            s1_out.at[h, q, at_rows(peer, part), :], s1_in.at[q, slot],
            s_send.at[0], s1_recv.at[q], device_id=dest, device_id_type=MESH,
        )

    def make_state(q):
        for h in range(2):
            scaled = (ks[h, q].astype(F32) * fade[h]).astype(BF16)
            total = lax.dot_general(
                scaled, vs[h, q], (((0,), (0,)), ((), ())), preferred_element_type=F32
            )
            s1_out[h, q] = total.astype(BF16)
        for j in range(NY):
            s1_copy(q, 1, j).start()
            if j:
                s1_copy(q, 0, j).start()
        s1_in[q, slot] = s1_out[0, q, at_rows(y, part), :]

    def s2_copy(q, d):
        return pltpu.make_async_remote_copy(
            s2_out.at[q], s2_in.at[q, d - 1], s_send.at[1], s2_recv.at[q],
            device_id={"sp": lax.rem(z + d, nz) * NY + y}, device_id_type=MESH,
        )

    def plane_total(q):
        took = s1_in.at[q, 0:2 * NY - 1]
        pltpu.make_async_remote_copy(
            took, took, s_send.at[0], s1_recv.at[q], device_id={"tp": mirror}, device_id_type=MESH,
        ).wait_recv()
        step = power(length)
        total = s1_in[q, 0].astype(F32)
        for k in range(1, 2 * NY):
            total = total * step + s1_in[q, k].astype(F32)
        s2_out[q] = total.astype(BF16)
        for d in range(1, nz):
            @pl.when(z + d < nz)
            def _():
                s2_copy(q, d).start()

    def s3_copy(q, h, j):
        peer = lax.rem(y + j, NY)
        dest = {"sp": z * NY + peer, "tp": mirror} if h else {"sp": z * NY + peer}
        return pltpu.make_async_remote_copy(
            s3_out.at[q, peer * 2 + (1 - group if h else group)],
            excl.at[h, q, at_rows(y, part), :],
            s_send.at[2], s3_recv.at[q], device_id=dest, device_id_type=MESH,
        )

    def hand_back(q):
        for n in range(1, nz):
            @pl.when(z == n)
            def _():
                took = s2_in.at[q, 0:n]
                pltpu.make_async_remote_copy(
                    took, took, s_send.at[1], s2_recv.at[q],
                    device_id={"tp": mirror}, device_id_type=MESH,
                ).wait_recv()

        def add(d, total):
            return total + power(line * NY * d) * s2_in[q, d].astype(F32)

        before = lax.fori_loop(0, z, add, jnp.zeros((part, HEAD_DIM), F32))
        step = power(length)
        for k in range(2 * NY):
            s3_out[q, k] = before.astype(BF16)
            before = before * step + s1_in[q, k].astype(F32)
        for j in range(NY):
            s3_copy(q, 1, j).start()
            if j:
                s3_copy(q, 0, j).start()
        excl[0, q, at_rows(y, part), :] = s3_out[q, slot]

    def inside(q):
        for h in range(2):
            for i in range(length // SUB):
                here, upto = slice(i * SUB, (i + 1) * SUB), slice(0, (i + 1) * SUB)
                score = lax.dot_general(
                    qs[h, q, here, :], ks[h, q, upto, :],
                    (((1,), (1,)), ((), ())), preferred_element_type=F32,
                )
                weight = (score * mask[h, here, upto]).astype(BF16)
                within[h, q, here, :] = jnp.dot(
                    weight, vs[h, q, upto, :], preferred_element_type=F32
                )

    def gated_copy(q, dest, source, near_by=0):
        return pltpu.make_async_remote_copy(
            g_out.at[q, at_rows(dest, rows), :], g_in.at[q, :, at_rows(source, 2 * HEAD_DIM)],
            g_send, g_recv.at[q + near_by * lax.div(q, seqs - 1)],
            device_id={"tp": base + dest}, device_id_type=MESH,
        )

    def finish(q):
        took = s1_in.at[q, 0:2 * NY - 1]
        pltpu.make_async_remote_copy(
            took, took, s_send.at[2], s3_recv.at[q], device_id={"tp": mirror}, device_id_type=MESH,
        ).wait_recv()
        for k in range(2):
            here = at_rows((1 - side) if k == 0 else side, pair)
            for h in range(2):
                kept = within[h, q, here, :] + jnp.dot(
                    qr[h, q, here, :], excl[h, q], preferred_element_type=F32
                )
                kept = kept - jnp.mean(kept, axis=-1, keepdims=True)
                spread = jnp.mean(kept * kept, axis=-1, keepdims=True)
                normal = kept * lax.rsqrt(spread + group_eps) * sg[h, q, here, :]
                g_out[q, here, cuts[h]] = normal.astype(BF16)
            if k == 0:
                gated_copy(q, across, me).start()
                gated_copy(q, across_twin, me).start()
            else:
                gated_copy(q, twin, me, 1).start()
                g_in[q, :, at_rows(me, 2 * HEAD_DIM)] = g_out[q, at_rows(me, rows), :]

    def gated_wait(q, near_by):
        took = g_in.at[q, :, 0:(2 if near_by else 4 if q == seqs - 1 else 6) * HEAD_DIM]
        pltpu.make_async_remote_copy(
            took, took, g_send, g_recv.at[q + near_by],
            device_id={"tp": mirror}, device_id_type=MESH,
        ).wait_recv()

    step = 512
    side_cols = 4 * HEAD_DIM

    def closing(lo, n):
        def norm(i, _):
            at = pl.multiple_of(i * 16, 16)
            x = premix[pl.ds(at, 16), :]
            scale = lax.rsqrt(jnp.mean(x * x, axis=-1, keepdims=True) + rms_eps)
            q = lo + lax.div(i, rows // 16)
            to = pl.multiple_of(lax.rem(i, rows // 16) * 16, 16)
            out[q, pl.ds(to, 16), :] = (x * scale * pgain[...]).astype(BF16)
            return 0

        lax.fori_loop(0, n // 16, norm, 0, unroll=2)

    def emit(lo, hi):
        n = (hi - lo) * rows
        with jax.named_scope("gated_wait"):
            for q in range(lo, hi):
                gated_wait(q, 0)
        g = g_in[lo:hi].reshape(n, g_in.shape[2])
        for c in range(width // step):
            cut = slice(c * step, (c + 1) * step)
            premix[0:n, cut] = jnp.dot(g, wo[:, cut], preferred_element_type=F32)
        closing(lo, n)

    def emit_half(lo, hi, which, near_by):
        for q in range(lo, hi):
            gated_wait(q, near_by)
        n = (hi - lo) * rows
        span = at_rows(which, side_cols)
        g = g_in[lo:hi, :, span].reshape(n, side_cols)
        for c in range(width // step):
            cut = slice(c * step, (c + 1) * step)
            term = jnp.dot(g, wo[span, cut], preferred_element_type=F32)
            premix[0:n, cut] = term if near_by else premix[0:n, cut] + term

    def scoped(name, function, *args):
        with jax.named_scope(name):
            function(*args)

    def over(lo, hi, function):
        def run(q, _):
            function(q)
            return 0

        lax.fori_loop(lo, hi, run, 0)

    def near(q):
        arrived(q, twin, 0)
        project_kv(0, q, own_rows)
        project_qg(0, q, own_rows)

    def near_raw():
        arrived(None, twin, 0)
        norm_raw(twin)
        project_kv(0, 0, own_rows)
        project_qg(0, 0, own_rows)

    def take(q):
        with jax.named_scope("take"):
            arrived(q, across, 1)
        block_copy(q, across, twin, p_send, 2).start()

    def rest(q):
        with jax.named_scope("take2"):
            arrived(q, across_twin, 2)
        project_kv(0, q, far_rows)
        project_qg(0, q, far_rows)

    def rest_raw():
        norm_raw(across)
        with jax.named_scope("take2"):
            arrived(None, across_twin, 2)
        norm_raw(across_twin)
        project_kv(0, 0, far_rows)
        project_qg(0, 0, far_rows)

    end = seqs - 1
    scoped("near0", near_raw)
    scoped("pass0", pass_on, 0)
    scoped("near123", over, 1, seqs, near)
    scoped("pass1", pass_on, 1)
    with jax.named_scope("tables1"):
        head_copy().wait_recv()
        tables(1)
    loads[3].wait()
    pltpu.make_async_copy(wo_h, wo, o_sem).wait()
    scoped("pass2", pass_on, 2)
    take(None)
    scoped("pass3", pass_on, 3)
    scoped("rest0", rest_raw)
    take(1)
    scoped("rest1", rest, 1)
    with jax.named_scope("havekv"):
        have(0)

    def early(q):
        project_kv(1, q, everything)
        make_state(q)

    def lone(q):
        project_kv(1, q, own_rows)

    def later(q):
        project_qg(1, q, everything)

    scoped("early", over, 0, 2, early)
    take(2)
    scoped("lone", over, 2, seqs, lone)
    scoped("rest2", rest, 2)
    project_kv(1, 2, far_rows)
    scoped("state2", make_state, 2)
    with jax.named_scope("haveqg"):
        have(1)
    take_last()
    scoped("later0", over, 0, 1, later)
    with jax.named_scope("present"):
        @pl.when(z < nz - 1)
        def _():
            pl.semaphore_wait(present, nz - 1 - z)

    scoped("plane0", plane_total, 0)
    project_qg(1, end, own_rows)
    scoped("plane1", plane_total, 1)
    with jax.named_scope("take2e"):
        arrived(end, across_twin, 2)
    with jax.named_scope("rest3"):
        for h in range(2):
            project_kv(h, end, far_rows)
        make_state(end)
    scoped("plane2", plane_total, 2)
    with jax.named_scope("qg3"):
        for h in range(2):
            project_qg(h, end, far_rows)
    scoped("later12", over, 1, seqs - 1, later)
    scoped("back0", hand_back, 0)
    scoped("back1", hand_back, 1)
    scoped("inside01", over, 0, 2, inside)
    scoped("plane3", plane_total, end)
    scoped("back2", hand_back, 2)
    scoped("inside23", over, 2, seqs, inside)
    scoped("back3", hand_back, end)
    scoped("finish01", over, 0, 2, finish)
    scoped("finish23", over, 2, seqs, finish)
    scoped("emit0", emit, 0, 2)
    scoped("emit2", emit, 2, end)
    scoped("emit3a", emit_half, end, seqs, side, 1)
    scoped("emit3b", emit_half, end, seqs, 1 - side, 0)

    def sent(took, sem):
        pltpu.make_async_remote_copy(
            took, took, sem, h_recv, device_id={"tp": mirror}, device_id_type=MESH,
        ).wait_send()

    with jax.named_scope("drain"):
        sent(gath.at[:, 0:rows, :], x_send)
        sent(gath.at[:, 0:2 * rows, :], p_send)
        sent(w.at[0, :, :], w_send)
        sent(heads.at[0], w_send)
        sent(s1_in.at[:, 0:2 * NY - 1], s_send.at[0])
        for n in range(nz - 1):
            @pl.when(z == n)
            def _():
                sent(s2_in.at[:, 0:nz - 1 - n], s_send.at[1])
        sent(s3_out.at[:, 0:2 * NY - 1], s_send.at[2])
        sent(g_in.at[:, :, 0:6 * HEAD_DIM], g_send)


def hand_over(source, premix, pgain, out, held, sem):
    seqs, rows, _ = source.shape
    done = pltpu.make_async_copy(source.at[0:seqs - 1], out.at[0:seqs - 1], sem.at[0])
    done.start()

    def norm(i, _):
        at = pl.multiple_of(i * 16, 16)
        x = premix[pl.ds(at, 16), :]
        scale = lax.rsqrt(jnp.mean(x * x, axis=-1, keepdims=True) + rms_eps)
        held[pl.ds(at, 16), :] = (x * scale * pgain[...]).astype(BF16)
        return 0

    lax.fori_loop(0, rows // 16, norm, 0, unroll=2)
    last = pltpu.make_async_copy(held, out.at[seqs - 1], sem.at[1])
    last.start()
    done.wait()
    last.wait()


def solution(mesh):
    tp, sp = mesh.shape["tp"], mesh.shape["sp"]

    def body(tok, gain, wq, wk, wv, wg, decay, ngain, wo, pgain):
        seqs, rows, width = tok.shape
        length = rows * 4
        nz = sp // NY
        part = HEAD_DIM // NY
        half = HEAD_DIM // 2
        inv = np.float32(rope_base) ** (-np.arange(half, dtype=np.float32) / half)
        inv = jnp.asarray(np.concatenate([inv, inv])[None, :], F32)
        dma = pltpu.SemaphoreType.DMA
        hbm = pl.BlockSpec(memory_space=pltpu.HBM)
        vmem = pltpu.VMEM
        wide = vmem((2, seqs, length, HEAD_DIM), BF16)
        mixed, premix, post = pl.pallas_call(
            functools.partial(kernel, tp, sp),
            out_shape=(
                jax.ShapeDtypeStruct(tok.shape, BF16),
                jax.ShapeDtypeStruct((seqs * rows, width), F32),
                jax.ShapeDtypeStruct((1, width), F32),
            ),
            in_specs=[
                hbm, hbm, hbm, hbm, hbm, hbm,
                pl.BlockSpec(memory_space=pltpu.SMEM), hbm, hbm, hbm, hbm,
            ],
            out_specs=(pl.BlockSpec(memory_space=pltpu.VMEM),) * 3,
            scratch_shapes=[
                vmem((1, width), F32), vmem((1, HEAD_DIM), F32),
                vmem((2, 8, HEAD_DIM), F32),
                vmem((seqs - 1, rows, width), BF16),
                vmem((length, width), BF16),
                vmem((seqs, length, width), BF16),
                vmem((2, width, 4 * HEAD_DIM), BF16),
                vmem(wo.shape, BF16),
                vmem((length, HEAD_DIM), F32), vmem((length, HEAD_DIM), F32),
                vmem((2, length, length), F32),
                vmem((2, length, HEAD_DIM), F32), vmem((2, length, HEAD_DIM), F32),
                wide, wide, wide, wide,
                vmem((2, seqs, length, HEAD_DIM), F32),
                vmem((2, seqs, length, HEAD_DIM), F32),
                vmem((2, seqs, HEAD_DIM, HEAD_DIM), BF16),
                vmem((seqs, 2 * NY, part, HEAD_DIM), BF16),
                vmem((seqs, part, HEAD_DIM), BF16),
                vmem((seqs, nz - 1, part, HEAD_DIM), BF16),
                vmem((seqs, 2 * NY, part, HEAD_DIM), BF16),
                vmem((2, seqs, HEAD_DIM, HEAD_DIM), BF16),
                vmem((seqs, length, 2 * HEAD_DIM), BF16),
                vmem((seqs, rows, HEAD_DIM * tp), BF16),
                dma(()), dma(()), dma((3 * seqs,)), dma((2,)), dma(()), dma((6,)), dma(()),
                dma((3,)), dma((seqs,)), dma((seqs,)), dma((seqs,)), dma(()), dma((seqs + 1,)),
                dma((5,)), dma(()), dma((seqs,)), pltpu.SemaphoreType.REGULAR,
            ],
            compiler_params=pltpu.CompilerParams(
                collective_id=0, has_side_effects=True, vmem_limit_bytes=40 * 2**20
            ),
            name="retention",
        )(
            *(pltpu.with_memory_space_constraint(x, pltpu.HBM) for x in (tok, gain[None, :], wq, wk, wv, wg)), decay,
            *(pltpu.with_memory_space_constraint(x, pltpu.HBM) for x in (ngain[None, :], wo, pgain[None, :], inv))
        )
        return pl.pallas_call(
            hand_over,
            out_shape=jax.ShapeDtypeStruct(tok.shape, BF16),
            in_specs=[pl.BlockSpec(memory_space=pltpu.VMEM)] * 3,
            out_specs=hbm,
            scratch_shapes=[vmem((rows, width), BF16), dma((2,))],
            compiler_params=pltpu.CompilerParams(vmem_limit_bytes=16 * 2**20),
            name="hand_over",
        )(mixed, premix, post)

    placed = (
        P(None, ("sp", "tp"), None),
        P(),
        P(None, "tp"),
        P(None, "tp"),
        P(None, "tp"),
        P(None, "tp"),
        P("tp"),
        P("tp"),
        P(),
        P(),
    )
    return jax.shard_map(
        body, mesh=mesh, in_specs=placed, out_specs=P(None, ("sp", "tp"), None), check_vma=False
    )
```
